256 devices in a mesh: sp: 32 (over z, y), tp: 8 (over x, core).
Axes of the slice: x: 4, y: 4, z: 8, core: 2. Of those that a mesh axis runs over, the one named last changes fastest.
Arguments:
- inputs: bfloat16 [16384, 4096], P('sp', 'tp'), may hold values from -24 to 24
- length: int32 [1], replicated, may hold values from 8193 to 16384
- win_query: bfloat16 [4096, 1536], P(None, 'tp'), may hold values from -8 to 8
- win_key: bfloat16 [4096, 512], P(None, 'tp'), may hold values from -8 to 8
- win_value: bfloat16 [4096, 512], P(None, 'tp'), may hold values from -1.5 to 1.5
- sink_logit: float32 [24], P('tp'), may hold values from 4 to 8
- diff_query: bfloat16 [4096, 1024], P(None, 'tp'), may hold values from -8 to 8
- diff_key: bfloat16 [4096, 1024], P(None, 'tp'), may hold values from -8 to 8
- diff_value: bfloat16 [4096, 1024], P(None, 'tp'), may hold values from -0.09375 to 0.09375
- mix_lambda: float32 [16], P('tp'), may hold values from 0.3 to 0.8
- head_gain: float32 [64], replicated, may hold values from 0.1 to 1.9
- win_out: bfloat16 [1536, 4096], P('tp'), may hold values from -0.125 to 0.125
- diff_out: bfloat16 [1024, 4096], P('tp'), may hold values from -0.125 to 0.125
Outputs:
- merged_out: bfloat16 [16384, 4096], P(('sp', 'tp'))
The draws below stay inside these ranges and needn't reach their ends.
All inputs are finite; a program needn't handle non-finite values.
Results may differ from the reference program's by a relative error of at most 0.015.
Values may be sent and summed in bfloat16 or wider, within the bound.
A program may use at most 128 MiB of HBM per device.

```python
import jax
import jax.numpy as jnp
from jax import lax

D = 4096
HEAD = 64
DQK = 32
WKV = 8
GROUP = 3
WQH = 24
DH = 16
WINDOW = 128
TOKENS = 16384
N_TP = 8


def clipped(key, shape):
    return jnp.clip(jax.random.normal(key, shape, jnp.float32), -6.0, 6.0)


def window_pair(key):
    key_weight = clipped(jax.random.fold_in(key, 101), (D, WKV * HEAD)) * D ** (-0.5)
    noise_part = clipped(jax.random.fold_in(key, 102), (D, WKV * GROUP * HEAD)) * D ** (-0.5)
    query_weight = noise_part
    return (query_weight, key_weight)


def diff_pair(key):
    key_weight = clipped(jax.random.fold_in(key, 201), (D, DH * 2 * DQK)) * D ** (-0.5)
    noise_part = clipped(jax.random.fold_in(key, 202), (D, DH * 2 * DQK)) * (3.0 / D) ** 0.5
    query_weight = noise_part
    return (query_weight, key_weight)


def draw_inputs(key, part):
    base_rows = clipped(jax.random.fold_in(key, 301), (TOKENS, D))
    return base_rows.astype(jnp.bfloat16)


def draw_win_query(key, part):
    return window_pair(key)[0].astype(jnp.bfloat16)


def draw_win_key(key, part):
    return window_pair(key)[1].astype(jnp.bfloat16)


def draw_diff_query(key, part):
    return diff_pair(key)[0].astype(jnp.bfloat16)


def draw_diff_key(key, part):
    return diff_pair(key)[1].astype(jnp.bfloat16)


def block_scale(key, dims, cuts, low, top_value):
    gain, own = 1.0, jax.random.fold_in(key, 6)
    for dim, shards_of in cuts:
        steps = jnp.exp(jax.random.uniform(jax.random.fold_in(own, dim), (shards_of,), jnp.float32, low / len(cuts), top_value / len(cuts)))
        gain = gain * jnp.repeat(steps, dims[dim] // shards_of).reshape([-1 if axis == dim else 1 for axis in range(len(dims))])
    return gain


def gaussian(stream_key, shape, deviation, most, pieces=(), dtype=jnp.bfloat16):
    array = jax.random.normal(stream_key, shape, jnp.float32) * deviation
    if len(pieces) > 0:
        array = block_scale(stream_key, shape, pieces, -0.22, 0.18) * array
    return jnp.clip(array, min=-most, max=most).astype(dtype)


def setup_inputs(seed: int = 0) -> dict:
    splits = jax.random.split(jax.random.key(seed), 14)
    return {
        "inputs": draw_inputs(jax.random.fold_in(splits[13], 71), 0),
        "length": jax.random.randint(splits[1], (1,), TOKENS // 2 + 1, TOKENS + 1).astype(jnp.int32),
        "win_query": draw_win_query(jax.random.fold_in(splits[13], 71), 0),
        "win_key": draw_win_key(jax.random.fold_in(splits[13], 71), 0),
        "win_value": gaussian(splits[4], (D, WKV * HEAD), (max(D // 256, 1)) ** -0.5, 1.5, ((1, 8),)),
        "sink_logit": jnp.clip(4.0 + 4.0 * jax.random.uniform(splits[5], (WQH,), jnp.float32) ** block_scale(splits[5], (WQH,), ((0, 8),), -0.2, 0.2), 4.0, 8.0),
        "diff_query": draw_diff_query(jax.random.fold_in(splits[13], 71), 0),
        "diff_key": draw_diff_key(jax.random.fold_in(splits[13], 71), 0),
        "diff_value": gaussian(splits[8], (D, DH * HEAD), D ** -0.5, 0.09375, ((1, 8),)),
        "mix_lambda": jnp.clip(0.3 + 0.5 * jax.random.uniform(splits[9], (DH,), jnp.float32) ** block_scale(splits[9], (DH,), ((0, 8),), -0.2, 0.2), 0.3, 0.8),
        "head_gain": jnp.clip(1.0 + 0.18 * jax.random.normal(splits[10], (HEAD,), jnp.float32), 0.1, 1.9),
        "win_out": gaussian(splits[11], (WQH * HEAD, D), ((WQH + DH) * HEAD) ** -0.5, 0.125, ((0, 8),)),
        "diff_out": gaussian(splits[12], (DH * HEAD, D), ((WQH + DH) * HEAD) ** -0.5, 0.125, ((0, 8),)),
    }


epsilon = 1e-06
masked_score = -1e+30

def window_attention(win_q, win_k, win_v, sink_logit, live_count):
    queries = win_q.reshape(TOKENS, WKV, GROUP, HEAD)
    padded_k = jnp.pad(win_k.reshape(TOKENS, WKV, HEAD), ((WINDOW, WINDOW), (0, 0), (0, 0)))
    padded_v = jnp.pad(win_v.reshape(TOKENS, WKV, HEAD), ((WINDOW, WINDOW), (0, 0), (0, 0)))
    sink_table = sink_logit.reshape(WKV, GROUP)
    block_rows = 512
    block_count = TOKENS // block_rows

    def one_block(block_index):
        first_row = (block_index * block_rows).astype(jnp.int32)
        query_slab = lax.dynamic_slice_in_dim(queries, first_row, block_rows, 0).astype(jnp.float32)
        key_slab = lax.dynamic_slice_in_dim(padded_k, first_row, block_rows + 2 * WINDOW, 0).astype(jnp.float32)
        value_slab = lax.dynamic_slice_in_dim(padded_v, first_row, block_rows + 2 * WINDOW, 0).astype(jnp.float32)
        query_pos = first_row + jnp.arange(block_rows).astype(jnp.int32)
        key_pos = first_row - WINDOW + jnp.arange(block_rows + 2 * WINDOW).astype(jnp.int32)
        allowed = (jnp.abs(query_pos[:, None] - key_pos[None, :]) <= WINDOW) & (key_pos[None, :] >= 0) & (key_pos[None, :] < live_count)
        scores = jnp.einsum('qhgd,khd->hgqk', query_slab, key_slab) * HEAD ** (-0.5)
        scores = jnp.where(allowed[None, None], scores, masked_score)
        row_max = jnp.maximum(lax.optimization_barrier(jnp.max(scores, axis=-1)), sink_table[:, :, None])
        exponent = jnp.where(allowed[None, None], jnp.exp(scores - row_max[..., None]), 0.0)
        denominator = lax.optimization_barrier(jnp.sum(exponent, axis=-1)) + jnp.exp(sink_table[:, :, None] - row_max)
        weights_low = lax.optimization_barrier(exponent.astype(jnp.bfloat16)).astype(jnp.float32)
        result = jnp.einsum('hgqk,khd->qhgd', weights_low, value_slab) / jnp.transpose(denominator, (2, 0, 1))[..., None]
        result = jnp.where((query_pos < live_count)[:, None, None, None], result, 0.0)
        return result.reshape(block_rows, WQH * HEAD).astype(jnp.bfloat16)
    return lax.map(one_block, jnp.arange(block_count)).reshape(TOKENS, WQH * HEAD)

def diff_attention(diff_q, diff_k, diff_v, mix_lambda, head_gain, live_count):
    queries = diff_q.reshape(TOKENS, DH, 2, DQK)
    key_all = diff_k.reshape(TOKENS, DH, 2, DQK)
    value_all = diff_v.reshape(TOKENS, DH, HEAD)
    key_live = jnp.arange(TOKENS).astype(jnp.int32) < live_count
    block_rows = 512
    block_count = TOKENS // block_rows

    def one_head(head_index):
        query_head = lax.dynamic_index_in_dim(queries, head_index, 1, keepdims=False).astype(jnp.float32)
        key_head = lax.dynamic_index_in_dim(key_all, head_index, 1, keepdims=False).astype(jnp.float32)
        value_head = lax.dynamic_index_in_dim(value_all, head_index, 1, keepdims=False).astype(jnp.float32)
        mix_weight = lax.dynamic_index_in_dim(mix_lambda, head_index, 0, keepdims=False)

        def one_block(block_index):
            first_row = (block_index * block_rows).astype(jnp.int32)
            query_slab = lax.dynamic_slice_in_dim(query_head, first_row, block_rows, 0)
            scores = jnp.einsum('qmd,kmd->mqk', query_slab, key_head) * DQK ** (-0.5)
            scores = jnp.where(key_live[None, None], scores, masked_score)
            row_max = lax.optimization_barrier(jnp.max(scores, axis=-1, keepdims=True))
            exponent = jnp.where(key_live[None, None], jnp.exp(scores - row_max), 0.0)
            total_sum = lax.optimization_barrier(jnp.sum(exponent, axis=-1))
            weights_low = lax.optimization_barrier(exponent.astype(jnp.bfloat16)).astype(jnp.float32)
            map_rows = jnp.einsum('mqk,kd->mqd', weights_low, value_head) / total_sum[..., None]
            mixed_rows = map_rows[0] - mix_weight * map_rows[1]
            normed = mixed_rows * lax.rsqrt(lax.optimization_barrier(jnp.mean(mixed_rows * mixed_rows, axis=-1, keepdims=True)) + epsilon) * head_gain
            query_pos = first_row + jnp.arange(block_rows).astype(jnp.int32)
            return jnp.where((query_pos < live_count)[:, None], normed, 0.0)
        return lax.map(one_block, jnp.arange(block_count)).reshape(TOKENS, HEAD)
    result = lax.map(one_head, jnp.arange(DH))
    return jnp.transpose(result, (1, 0, 2)).reshape(TOKENS, DH * HEAD).astype(jnp.bfloat16)

def reference(inputs, length, win_query, win_key, win_value, sink_logit, diff_query, diff_key, diff_value, mix_lambda, head_gain, win_out, diff_out):
    live_count = length[0]

    def project(weight):
        return jnp.dot(inputs, weight, preferred_element_type=jnp.float32).astype(jnp.bfloat16)
    win_rows = window_attention(project(win_query), project(win_key), project(win_value), sink_logit, live_count)
    diff_rows = diff_attention(project(diff_query), project(diff_key), project(diff_value), mix_lambda, head_gain, live_count)
    win_cols = WQH // N_TP * HEAD
    diff_cols = DH // N_TP * HEAD
    merged = jnp.zeros((TOKENS, D), jnp.float32)
    for group_index in range(N_TP):
        partial_value = jnp.dot(win_rows[:, group_index * win_cols:(group_index + 1) * win_cols], win_out[group_index * win_cols:(group_index + 1) * win_cols], preferred_element_type=jnp.float32)
        partial_value = partial_value + jnp.dot(diff_rows[:, group_index * diff_cols:(group_index + 1) * diff_cols], diff_out[group_index * diff_cols:(group_index + 1) * diff_cols], preferred_element_type=jnp.float32)
        partial_value = lax.optimization_barrier(partial_value.astype(jnp.bfloat16)).astype(jnp.float32)
        merged = merged + partial_value
    return merged.astype(jnp.bfloat16)
```

```python
import functools

import jax
import jax.numpy as jnp
from jax import lax
from jax.experimental import pallas as pl
from jax.experimental.pallas import tpu as pltpu
from jax.sharding import PartitionSpec as P

HEAD = 64
DQK = 32
GROUP = 3
WINDOW = 128
NX, NY, NZ = 4, 4, 8
ROWS = 512
BLOCKS = NY * NZ
Q_SCALE = 1.4426950408889634 * DQK ** (-0.5)
MESH = pl.DeviceIdType.MESH

epsilon = 1e-06
masked_score = -1e30
VMEM_SPEC = pl.BlockSpec(memory_space=pltpu.VMEM)
SMEM_SPEC = pl.BlockSpec(memory_space=pltpu.SMEM)
ANY_SPEC = pl.BlockSpec(memory_space=pl.ANY)


def place():
    sp, tp = lax.axis_index("sp"), lax.axis_index("tp")
    return sp // NY, sp % NY, tp // 2, tp % 2


def greet(devices, conditions=None):
    barrier = pltpu.get_barrier_semaphore()
    for i, device in enumerate(devices):
        def signal(device=device):
            pl.semaphore_signal(barrier, inc=1, device_id=device, device_id_type=MESH)
        if conditions is None or conditions[i] is None:
            signal()
        else:
            pl.when(conditions[i])(signal)


WQ, WK, WV, DQ, DK, DV, ACC_COLS = 0, 256, 384, 512, 640, 768, 896


def project_kernel(
    x_ref, wq_hbm, wk_hbm, wv_hbm, dq_hbm, dk_hbm, dv_hbm,
    winq_ref, winkv_ref, msg_ref,
    xg, wq, wk, wv, dq, dk, dv, acc, w_sem, recv_sem, send_r, send_l, send_s,
):
    z, y, x, c = place()
    sp = z * NY + y
    tp = x * 2 + c
    right = (sp, ((x + 1) % NX) * 2 + c)
    left = (sp, ((x + NX - 1) % NX) * 2 + c)
    sibling = (sp, x * 2 + 1 - c)
    half = ROWS // 2
    loads = [
        pltpu.make_async_copy(src, dst, w_sem.at[i])
        for i, (src, dst) in enumerate(
            ((wq_hbm, wq), (wk_hbm, wk), (wv_hbm, wv), (dq_hbm, dq), (dk_hbm, dk), (dv_hbm, dv))
        )
    ]
    for load in loads:
        load.start()
    greet((right, left, sibling))
    pl.semaphore_wait(pltpu.get_barrier_semaphore(), 3)

    started = []

    def send(own, t, part, device, sem):
        rows = pl.ds(part * half, half)
        copy = pltpu.make_async_remote_copy(
            src_ref=x_ref.at[rows] if own else xg.at[t, rows],
            dst_ref=xg.at[t, rows],
            send_sem=sem,
            recv_sem=recv_sem.at[t, part],
            device_id=device,
            device_id_type=MESH,
        )
        copy.start()
        started.append(copy)

    def arrive(t, part):
        rows = pl.ds(part * half, half)
        pltpu.make_async_remote_copy(
            src_ref=xg.at[t, rows], dst_ref=xg.at[t, rows],
            send_sem=send_r.at[0], recv_sem=recv_sem.at[t, part],
            device_id=sibling, device_id_type=MESH,
        ).wait_recv()

    send(True, tp, 0, right, send_r.at[0])
    send(True, tp, 1, left, send_l.at[0])
    send(True, tp, 0, sibling, send_s.at[0])
    send(True, tp, 1, right, send_r.at[1])
    send(True, tp, 0, left, send_l.at[1])
    send(True, tp, 1, sibling, send_s.at[1])

    acc[...] = jnp.zeros_like(acc)

    def multiply(block, t):
        ks = pl.ds(pl.multiple_of(t * ROWS, ROWS), ROWS)
        for weight, at, width in ((wq, WQ, 192), (wk, WK, 64), (wv, WV, 64), (dv, DV, 128)):
            acc[:, at:at + width] += jnp.dot(block, weight[ks, :], preferred_element_type=jnp.float32)
        both = jnp.concatenate([dq[ks, :], dk[ks, :]], axis=1)
        acc[:, DQ:DQ + 256] += jnp.dot(block, both, preferred_element_type=jnp.float32)

    for load in loads:
        load.wait()
    multiply(x_ref[...], tp)

    t_left = ((x + NX - 1) % NX) * 2 + c
    t_right = ((x + 1) % NX) * 2 + c
    t_far = ((x + 2) % NX) * 2 + c

    def other(t):
        return t + 1 - 2 * c

    arrive(t_left, 0)
    send(False, t_left, 0, right, send_r.at[2])
    send(False, t_left, 0, sibling, send_s.at[2])
    arrive(t_right, 1)
    send(False, t_right, 1, left, send_l.at[2])
    send(False, t_right, 1, sibling, send_s.at[3])
    arrive(other(tp), 0)
    arrive(other(tp), 1)
    multiply(xg[other(tp)], other(tp))
    arrive(t_left, 1)
    send(False, t_left, 1, sibling, send_s.at[4])
    arrive(t_right, 0)
    send(False, t_right, 0, sibling, send_s.at[5])
    multiply(xg[t_left], t_left)
    multiply(xg[t_right], t_right)
    for t in (t_left, t_right):
        arrive(other(t), 0)
        arrive(other(t), 1)
        multiply(xg[other(t)], other(t))
    arrive(t_far, 0)
    send(False, t_far, 0, sibling, send_s.at[6])
    arrive(t_far, 1)
    send(False, t_far, 1, sibling, send_s.at[7])
    multiply(xg[t_far], t_far)
    arrive(other(t_far), 0)
    arrive(other(t_far), 1)
    multiply(xg[other(t_far)], other(t_far))

    winq_ref[...] = acc[:, WQ:WQ + 192].astype(jnp.bfloat16)
    lane = lax.broadcasted_iota(jnp.int32, (half, 128), 1)
    low = lane < 64
    for part in range(2):
        rows = pl.ds(part * half, half)
        winkv_ref[rows, :] = jnp.where(
            low, acc[rows, WK:WK + 128], pltpu.roll(acc[rows, WV:WV + 128], 64, 1)
        ).astype(jnp.bfloat16)
    first, second = acc[0:half, DK:DK + 128], acc[half:ROWS, DK:DK + 128]
    msg_ref[0, 0:256, :] = jnp.where(low, first, pltpu.roll(second, 64, 1)).astype(jnp.bfloat16)
    msg_ref[1, 0:256, :] = jnp.where(low, pltpu.roll(first, 64, 1), second).astype(jnp.bfloat16)
    for j in range(4):
        rows = pl.ds(j * 128, 128)
        v_t = acc[rows, DV:DV + 128].T.astype(jnp.bfloat16)
        q_t = (acc[rows, DQ:DQ + 128].T * Q_SCALE).astype(jnp.bfloat16)
        for head in range(2):
            msg_ref[head, 256 + j * 64:256 + (j + 1) * 64, :] = v_t[head * 64:(head + 1) * 64]
            msg_ref[head, 512 + j * 64:512 + (j + 1) * 64, :] = q_t[head * 64:(head + 1) * 64]
    for copy in started:
        copy.wait_send()


def project(inputs, weights):
    bf = jnp.bfloat16
    depth = weights[0].shape[0]
    return pl.pallas_call(
        project_kernel,
        out_shape=(
            jax.ShapeDtypeStruct((ROWS, 192), bf),
            jax.ShapeDtypeStruct((ROWS, 128), bf),
            jax.ShapeDtypeStruct((2, 768, 128), bf),
        ),
        in_specs=[VMEM_SPEC] + [ANY_SPEC] * 6,
        out_specs=(VMEM_SPEC,) * 3,
        scratch_shapes=[
            pltpu.VMEM((2 * NX, ROWS, ROWS), bf),
            pltpu.VMEM((depth, 192), bf),
            pltpu.VMEM((depth, 64), bf),
            pltpu.VMEM((depth, 64), bf),
            pltpu.VMEM((depth, 128), bf),
            pltpu.VMEM((depth, 128), bf),
            pltpu.VMEM((depth, 128), bf),
            pltpu.VMEM((ROWS, ACC_COLS), jnp.float32),
            pltpu.SemaphoreType.DMA((6,)),
            pltpu.SemaphoreType.DMA((2 * NX, 2)),
            pltpu.SemaphoreType.DMA((3,)),
            pltpu.SemaphoreType.DMA((3,)),
            pltpu.SemaphoreType.DMA((8,)),
        ],
        compiler_params=pltpu.CompilerParams(
            collective_id=0, has_side_effects=True, vmem_limit_bytes=48 * 1024 * 1024
        ),
        name="project",
    )(inputs, *weights)


def exchange_kernel(
    msg_ref, lam_ref, winkv_ref,
    kv_ref, q_ref, lamo_ref, halo_ref,
    recv_kv, recv_q, recv_lam, recv_halo, send_a, send_ring, send_sib, send_halo, local_sem,
):
    z, y, x, c = place()
    sp = z * NY + y
    tp = x * 2 + c
    up = (((z + 1) % NZ) * NY + y, tp)
    down = (((z + NZ - 1) % NZ) * NY + y, tp)
    sibling = (sp, x * 2 + 1 - c)
    after = ((sp + 1) % BLOCKS, tp)
    before = ((sp + BLOCKS - 1) % BLOCKS, tp)
    partners = [(z * NY + 2 * c + i, x * 2 + y // 2) for i in range(2)]
    away = [(2 * c + i) != y for i in range(2)]
    greet((up, down, sibling, after, before) + tuple(partners), (None,) * 5 + tuple(away))
    pl.semaphore_wait(pltpu.get_barrier_semaphore(), 5 + sum(a.astype(jnp.int32) for a in away))

    def remote(src, dst, send_sem, recv_sem, device):
        return pltpu.make_async_remote_copy(
            src_ref=src, dst_ref=dst, send_sem=send_sem, recv_sem=recv_sem,
            device_id=device, device_id_type=MESH,
        )

    mine = z * NY + y
    slot = y % 2
    head_copies = []
    for i in range(2):
        head_copies.append([
            remote(msg_ref.at[i, pl.ds(0, 512)], kv_ref.at[mine], send_a.at[i, 0], recv_kv.at[mine], partners[i]),
            remote(msg_ref.at[i, pl.ds(512, 256)], q_ref.at[slot], send_a.at[i, 1], recv_q.at[slot], partners[i]),
            remote(lam_ref.at[i], lamo_ref.at[slot], send_a.at[i, 2], recv_lam.at[slot], partners[i]),
        ])
        def go(i=i):
            for copy in head_copies[i]:
                copy.start()
        pl.when(away[i])(go)
        def stay(i=i):
            copies = [
                pltpu.make_async_copy(msg_ref.at[i, pl.ds(0, 512)], kv_ref.at[mine], local_sem.at[0]),
                pltpu.make_async_copy(msg_ref.at[i, pl.ds(512, 256)], q_ref.at[slot], local_sem.at[1]),
                pltpu.make_async_copy(lam_ref.at[i], lamo_ref.at[slot], local_sem.at[2]),
            ]
            for copy in copies:
                copy.start()
            for copy in copies:
                copy.wait()
        pl.when(jnp.logical_not(away[i]))(stay)
    edges = [
        remote(winkv_ref.at[pl.ds(ROWS - WINDOW, WINDOW)], halo_ref.at[0], send_halo.at[0], recv_halo.at[0], after),
        remote(winkv_ref.at[pl.ds(0, WINDOW)], halo_ref.at[1], send_halo.at[1], recv_halo.at[1], before),
    ]
    for copy in edges:
        copy.start()

    started = []

    def block(zz, s, core):
        return ((zz + NZ) % NZ) * NY + 2 * core + s

    def forward(b, device, sem):
        copy = remote(kv_ref.at[b], kv_ref.at[b], sem, recv_kv.at[b], device)
        copy.start()
        started.append(copy)

    def arrive(b):
        remote(kv_ref.at[b], kv_ref.at[b], send_sib.at[0], recv_kv.at[b], sibling).wait_recv()

    for s in range(2):
        b = block(z, s, c)
        pl.when(away[s])(lambda: arrive(b))
        forward(b, up, send_ring.at[0, s, 0])
        forward(b, down, send_ring.at[1, s, 0])
        forward(b, sibling, send_sib.at[s])
    count = 2
    for d in range(1, 5):
        for s in range(2):
            for way, (reach, device, sign) in enumerate(((4 - s, up, -1), (3 + s, down, 1))):
                if d > reach:
                    continue
                b = block(z + sign * d, s, c)
                arrive(b)
                if d < reach:
                    forward(b, device, send_ring.at[way, s, d])
                forward(b, sibling, send_sib.at[count])
                count += 1
    for i in range(2):
        pl.when(away[i])(lambda i=i: [
            remote(msg_ref.at[0, pl.ds(512, 256)], q_ref.at[i], send_a.at[0, 1], recv_q.at[i], sibling).wait_recv(),
            remote(lam_ref.at[0], lamo_ref.at[i], send_a.at[0, 2], recv_lam.at[i], sibling).wait_recv(),
        ] and None)
    for copy in edges:
        copy.wait_recv()
    for zz in range(NZ):
        for s in range(2):
            arrive(block(zz, s, 1 - c))
    for copy in started + edges:
        copy.wait_send()
    for i in range(2):
        pl.when(away[i])(lambda i=i: [copy.wait_send() for copy in head_copies[i]] and None)


def exchange(msg, lam, winkv):
    bf = jnp.bfloat16
    return pl.pallas_call(
        exchange_kernel,
        out_shape=(
            jax.ShapeDtypeStruct((BLOCKS, ROWS, 128), bf),
            jax.ShapeDtypeStruct((2, 256, 128), bf),
            jax.ShapeDtypeStruct((2, 8, 128), jnp.float32),
            jax.ShapeDtypeStruct((2, WINDOW, 128), bf),
        ),
        in_specs=[VMEM_SPEC] * 3,
        out_specs=(VMEM_SPEC,) * 4,
        scratch_shapes=[
            pltpu.SemaphoreType.DMA((BLOCKS,)),
            pltpu.SemaphoreType.DMA((2,)),
            pltpu.SemaphoreType.DMA((2,)),
            pltpu.SemaphoreType.DMA((2,)),
            pltpu.SemaphoreType.DMA((2, 3)),
            pltpu.SemaphoreType.DMA((2, 2, 4)),
            pltpu.SemaphoreType.DMA((16,)),
            pltpu.SemaphoreType.DMA((2,)),
            pltpu.SemaphoreType.DMA((3,)),
        ],
        compiler_params=pltpu.CompilerParams(
            collective_id=1, has_side_effects=True, vmem_limit_bytes=32 * 1024 * 1024
        ),
        name="exchange",
    )(msg, lam, winkv)


NQ = 2 * ROWS
TILE = 1024
UNITS = [(n, h) for n in range(2 * NQ // TILE) for h in range(2)]


def attend_kernel(info_ref, kv_ref, q_ref, lam_ref, gain_ref, o_ref, qz, va, acc, s_buf, m_buf):
    live = info_ref[0]
    first = info_ref[1]
    count = jnp.where(first < live, (live + ROWS - 1) // ROWS, 0)
    qz[...] = jnp.zeros_like(qz)
    for t in range(NQ // 128):
        q = q_ref[t // 4, (t % 4) * 64:(t % 4 + 1) * 64, :]
        for h in range(2):
            for m in range(2):
                qz[h, h * 64 + m * 32:h * 64 + (m + 1) * 32, m * NQ + t * 128:m * NQ + (t + 1) * 128] = (
                    q[m * 32:(m + 1) * 32]
                )
    acc[...] = jnp.zeros_like(acc)
    va[...] = jnp.zeros_like(va)

    def values(b):
        lane = lax.broadcasted_iota(jnp.int32, (64, 128), 1)
        row = lax.broadcasted_iota(jnp.int32, (16, 128), 0)
        for j in range(4):
            ok = (b * ROWS + j * 128 + lane) < live
            v = kv_ref[b, 256 + j * 64:256 + (j + 1) * 64, :].astype(jnp.float32)
            va[0:64, j * 128:(j + 1) * 128] = jnp.where(ok, v, 0.0).astype(jnp.bfloat16)
            va[64:80, j * 128:(j + 1) * 128] = jnp.where(ok[:16] & (row == 0), 1.0, 0.0).astype(jnp.bfloat16)

    def scores(b, n, h):
        return jnp.dot(
            kv_ref[b, 0:256, :], qz[h, :, n * TILE:(n + 1) * TILE], preferred_element_type=jnp.float32
        )

    def gather(n, h, weight):
        acc[:, n * TILE:(n + 1) * TILE] += jnp.dot(
            va[:, h * 256:(h + 1) * 256], weight, preferred_element_type=jnp.float32
        )

    s_buf[0] = scores(0, *UNITS[0])

    def step(b, carry):
        values(b)
        for i, (n, h) in enumerate(UNITS):
            s = s_buf[i % 2]
            if i + 1 < len(UNITS):
                s_buf[1 - i % 2] = scores(b, *UNITS[i + 1])
            else:
                s_buf[1 - i % 2] = scores(jnp.minimum(b + 1, BLOCKS - 1), *UNITS[0])
            gather(n, h, jnp.exp2(s).astype(jnp.bfloat16))
        return carry

    lax.fori_loop(0, count, step, 0)

    sums = acc[64:65, :]
    fine = (sums > 2.0 ** -80) & (sums < 2.0 ** 100)
    fine_all = jnp.min(jnp.where(fine, 1.0, 0.0)) > 0.5

    @pl.when((count > 0) & jnp.logical_not(fine_all))
    def _():
        m_buf[...] = jnp.full_like(m_buf, masked_score)
        acc[...] = jnp.zeros_like(acc)

        def masked(b, n, h):
            key = b * ROWS + h * 256 + lax.broadcasted_iota(jnp.int32, (256, TILE), 0)
            return jnp.where(key < live, scores(b, n, h), masked_score)

        def maxima(b, carry):
            for n, h in UNITS:
                cols = slice(n * TILE, (n + 1) * TILE)
                m_buf[0:1, cols] = jnp.maximum(
                    m_buf[0:1, cols], jnp.max(masked(b, n, h), axis=0, keepdims=True)
                )
            return carry

        def again(b, carry):
            values(b)
            for n, h in UNITS:
                s = masked(b, n, h) - m_buf[0:1, n * TILE:(n + 1) * TILE]
                gather(n, h, jnp.exp2(s).astype(jnp.bfloat16))
            return carry

        lax.fori_loop(0, count, maxima, 0)
        lax.fori_loop(0, count, again, 0)

    gain = gain_ref[...]
    lam = lam_ref[0, 0:1, :]
    for t in range(NQ // 128):
        maps = []
        for m in range(2):
            cols = slice(m * NQ + t * 128, m * NQ + (t + 1) * 128)
            total = acc[64:65, cols]
            maps.append(acc[0:64, cols] / jnp.where(total > 0.0, total, 1.0))
        mixed = maps[0] - lam * maps[1]
        normed = mixed * lax.rsqrt(jnp.mean(mixed * mixed, axis=0, keepdims=True) + epsilon) * gain
        ok = (first + t * 128 + lax.broadcasted_iota(jnp.int32, (64, 128), 1)) < live
        o_ref[t // 4, (t % 4) * 64:(t % 4 + 1) * 64, :] = jnp.where(ok, normed, 0.0).astype(jnp.bfloat16)


def attend(info, kv, q, lam, gain):
    return pl.pallas_call(
        attend_kernel,
        out_shape=jax.ShapeDtypeStruct((2, 256, 128), jnp.bfloat16),
        in_specs=[SMEM_SPEC] + [VMEM_SPEC] * 4,
        out_specs=VMEM_SPEC,
        scratch_shapes=[
            pltpu.VMEM((2, 128, 2 * NQ), jnp.bfloat16),
            pltpu.VMEM((80, ROWS), jnp.bfloat16),
            pltpu.VMEM((80, 2 * NQ), jnp.float32),
            pltpu.VMEM((2, 256, TILE), jnp.float32),
            pltpu.VMEM((8, 2 * NQ), jnp.float32),
        ],
        compiler_params=pltpu.CompilerParams(vmem_limit_bytes=48 * 1024 * 1024),
        name="attend",
    )(info, kv, q, lam, gain)


def back_kernel(o_ref, rows_ref, recv_sem, send_sem, local_sem):
    z, y, x, c = place()
    partners = [(z * NY + 2 * c + i, x * 2 + y // 2) for i in range(2)]
    away = [(2 * c + i) != y for i in range(2)]
    greet(partners, away)
    pl.semaphore_wait(pltpu.get_barrier_semaphore(), sum(a.astype(jnp.int32) for a in away))
    slot = y % 2
    copies = [
        pltpu.make_async_remote_copy(
            src_ref=o_ref.at[i], dst_ref=rows_ref.at[slot], send_sem=send_sem.at[i], recv_sem=recv_sem.at[slot],
            device_id=partners[i], device_id_type=MESH,
        )
        for i in range(2)
    ]
    for i in range(2):
        pl.when(away[i])(lambda i=i: copies[i].start())
        def stay(i=i):
            copy = pltpu.make_async_copy(o_ref.at[i], rows_ref.at[slot], local_sem)
            copy.start()
            copy.wait()
        pl.when(jnp.logical_not(away[i]))(stay)
    for i in range(2):
        def wait(i=i):
            pltpu.make_async_remote_copy(
                src_ref=o_ref.at[i], dst_ref=rows_ref.at[i], send_sem=send_sem.at[i], recv_sem=recv_sem.at[i],
                device_id=partners[i], device_id_type=MESH,
            ).wait_recv()
            copies[i].wait_send()
        pl.when(away[i])(wait)


def back(o):
    return pl.pallas_call(
        back_kernel,
        out_shape=jax.ShapeDtypeStruct((2, 256, 128), jnp.bfloat16),
        in_specs=[VMEM_SPEC],
        out_specs=VMEM_SPEC,
        scratch_shapes=[
            pltpu.SemaphoreType.DMA((2,)),
            pltpu.SemaphoreType.DMA((2,)),
            pltpu.SemaphoreType.DMA,
        ],
        compiler_params=pltpu.CompilerParams(collective_id=2, has_side_effects=True),
        name="back",
    )(o)


def window_part(win_q, padded, sink_logit, live_count, offset):
    row_count = win_q.shape[0]
    keys_win = padded[:, :HEAD]
    values_win = padded[:, HEAD:]
    queries = win_q.reshape(row_count, GROUP, HEAD)
    query_pos = offset + jnp.arange(row_count, dtype=jnp.int32)
    key_pos = offset - WINDOW + jnp.arange(row_count + 2 * WINDOW, dtype=jnp.int32)
    allowed = (
        (jnp.abs(query_pos[:, None] - key_pos[None, :]) <= WINDOW)
        & (key_pos[None, :] >= 0)
        & (key_pos[None, :] < live_count)
    )
    scores = jnp.einsum("qgd,kd->gqk", queries, keys_win, preferred_element_type=jnp.float32) * HEAD ** (-0.5)
    scores = jnp.where(allowed[None], scores, masked_score)
    row_max = jnp.maximum(jnp.max(scores, axis=-1), sink_logit[:, None])
    exponent = jnp.where(allowed[None], jnp.exp(scores - row_max[..., None]), 0.0)
    denominator = jnp.sum(exponent, axis=-1) + jnp.exp(sink_logit[:, None] - row_max)
    result = jnp.einsum(
        "gqk,kd->qgd", exponent.astype(jnp.bfloat16), values_win, preferred_element_type=jnp.float32
    )
    result = result / jnp.transpose(denominator, (1, 0))[..., None]
    result = jnp.where((query_pos < live_count)[:, None, None], result, 0.0)
    return result.reshape(row_count, GROUP * HEAD).astype(jnp.bfloat16)


def body(
    inputs, length, win_query, win_key, win_value, sink_logit,
    diff_query, diff_key, diff_value, mix_lambda, head_gain, win_out, diff_out,
):
    live_count = length[0]
    sp = lax.axis_index("sp")
    offset = sp * ROWS
    first = ((sp // NY) * NY + 2 * (lax.axis_index("tp") % 2)) * ROWS
    win_q, win_kv, msg = project(inputs, (win_query, win_key, win_value, diff_query, diff_key, diff_value))
    lam = jnp.broadcast_to(mix_lambda[:, None, None], (2, 8, 128))
    kv, q, lam, halo = exchange(msg, lam, win_kv)
    padded = jnp.concatenate([halo[0], win_kv, halo[1]], axis=0)
    win_rows = window_part(win_q, padded, sink_logit, live_count, offset)
    info = jnp.stack([live_count, first]).astype(jnp.int32)
    gain = jnp.broadcast_to(head_gain[:, None], (HEAD, 128))
    rows_t = back(attend(info, kv, q, lam, gain))
    diff_rows = rows_t.reshape(2, 4, 64, 128).transpose(1, 3, 0, 2).reshape(ROWS, 128)
    partial_value = jnp.dot(win_rows, win_out, preferred_element_type=jnp.float32)
    partial_value = partial_value + jnp.dot(diff_rows, diff_out, preferred_element_type=jnp.float32)
    return lax.psum_scatter(partial_value.astype(jnp.bfloat16), "tp", scatter_dimension=0, tiled=True)


def solution(mesh):
    placed = (
        P("sp", "tp"), P(), P(None, "tp"), P(None, "tp"), P(None, "tp"), P("tp"), P(None, "tp"),
        P(None, "tp"), P(None, "tp"), P("tp"), P(), P("tp", None), P("tp", None),
    )
    return jax.shard_map(
        body, mesh=mesh, in_specs=placed, out_specs=P(("sp", "tp"), None), check_vma=False
    )
```

```python
import functools

import jax
import jax.numpy as jnp
from jax import lax
from jax.experimental import pallas as pl
from jax.experimental.pallas import tpu as pltpu
from jax.sharding import PartitionSpec as P

HEAD = 64
DQK = 32
GROUP = 3
WINDOW = 128
NX, NY, NZ = 4, 4, 8
ROWS = 512
BLOCKS = NY * NZ
Q_SCALE = 1.4426950408889634 * DQK ** (-0.5)
MESH = pl.DeviceIdType.MESH

epsilon = 1e-06
masked_score = -1e30
VMEM_SPEC = pl.BlockSpec(memory_space=pltpu.VMEM)
SMEM_SPEC = pl.BlockSpec(memory_space=pltpu.SMEM)
ANY_SPEC = pl.BlockSpec(memory_space=pl.ANY)


def place():
    sp, tp = lax.axis_index("sp"), lax.axis_index("tp")
    return sp // NY, sp % NY, tp // 2, tp % 2


def greet(devices, conditions=None):
    barrier = pltpu.get_barrier_semaphore()
    for i, device in enumerate(devices):
        def signal(device=device):
            pl.semaphore_signal(barrier, inc=1, device_id=device, device_id_type=MESH)
        if conditions is None or conditions[i] is None:
            signal()
        else:
            pl.when(conditions[i])(signal)


WQ, DQ, DK, DV, ACC_COLS = 0, 384, 512, 640, 768


def project_kernel(
    x_ref, wq_hbm, wk_hbm, wv_hbm, dq_hbm, dk_hbm, dv_hbm,
    winq_ref, winvk_ref, msg_ref,
    xg, wt, dq, dk, dv, acc, w_sem, recv_sem, send_r, send_l, send_s,
):
    z, y, x, c = place()
    sp = z * NY + y
    tp = x * 2 + c
    right = (sp, ((x + 1) % NX) * 2 + c)
    left = (sp, ((x + NX - 1) % NX) * 2 + c)
    sibling = (sp, x * 2 + 1 - c)
    half = ROWS // 2
    loads = [
        pltpu.make_async_copy(src, dst, w_sem.at[i])
        for i, (src, dst) in enumerate(
            (
                (wq_hbm, wt.at[pl.ds(0, 192)]),
                (wk_hbm, wt.at[pl.ds(192, 64)]),
                (wv_hbm, wt.at[pl.ds(256, 64)]),
                (dq_hbm, dq),
                (dk_hbm, dk),
                (dv_hbm, dv),
            )
        )
    ]
    for load in loads:
        load.start()
    greet((right, left, sibling))
    pl.semaphore_wait(pltpu.get_barrier_semaphore(), 3)

    started = []

    def send(own, t, part, device, sem):
        rows = pl.ds(part * half, half)
        copy = pltpu.make_async_remote_copy(
            src_ref=x_ref.at[rows] if own else xg.at[t, rows],
            dst_ref=xg.at[t, rows],
            send_sem=sem,
            recv_sem=recv_sem.at[t, part],
            device_id=device,
            device_id_type=MESH,
        )
        copy.start()
        started.append(copy)

    def arrive(t, part):
        rows = pl.ds(part * half, half)
        pltpu.make_async_remote_copy(
            src_ref=xg.at[t, rows], dst_ref=xg.at[t, rows],
            send_sem=send_r.at[0], recv_sem=recv_sem.at[t, part],
            device_id=sibling, device_id_type=MESH,
        ).wait_recv()

    send(True, tp, 0, right, send_r.at[0])
    send(True, tp, 1, left, send_l.at[0])
    send(True, tp, 0, sibling, send_s.at[0])
    send(True, tp, 1, right, send_r.at[1])
    send(True, tp, 0, left, send_l.at[1])
    send(True, tp, 1, sibling, send_s.at[1])

    acc[...] = jnp.zeros_like(acc)

    def multiply(block, t):
        ks = pl.ds(pl.multiple_of(t * ROWS, ROWS), ROWS)
        acc[:, WQ:WQ + 320] += lax.dot_general(
            block, wt[:, ks], (((1,), (1,)), ((), ())), preferred_element_type=jnp.float32
        )
        both = jnp.concatenate([dq[ks, :], dk[ks, :]], axis=1)
        acc[:, DQ:DQ + 256] += jnp.dot(block, both, preferred_element_type=jnp.float32)
        acc[:, DV:DV + 128] += jnp.dot(block, dv[ks, :], preferred_element_type=jnp.float32)

    for load in loads:
        load.wait()
    multiply(x_ref[...], tp)

    t_left = ((x + NX - 1) % NX) * 2 + c
    t_right = ((x + 1) % NX) * 2 + c
    t_far = ((x + 2) % NX) * 2 + c

    def other(t):
        return t + 1 - 2 * c

    arrive(t_left, 0)
    send(False, t_left, 0, right, send_r.at[2])
    send(False, t_left, 0, sibling, send_s.at[2])
    arrive(t_right, 1)
    send(False, t_right, 1, left, send_l.at[2])
    send(False, t_right, 1, sibling, send_s.at[3])
    arrive(other(tp), 0)
    arrive(other(tp), 1)
    multiply(xg[other(tp)], other(tp))
    arrive(t_left, 1)
    send(False, t_left, 1, sibling, send_s.at[4])
    arrive(t_right, 0)
    send(False, t_right, 0, sibling, send_s.at[5])
    multiply(xg[t_left], t_left)
    multiply(xg[t_right], t_right)
    for t in (t_left, t_right):
        arrive(other(t), 0)
        arrive(other(t), 1)
        multiply(xg[other(t)], other(t))
    arrive(t_far, 0)
    send(False, t_far, 0, sibling, send_s.at[6])
    arrive(t_far, 1)
    send(False, t_far, 1, sibling, send_s.at[7])
    multiply(xg[t_far], t_far)
    arrive(other(t_far), 0)
    arrive(other(t_far), 1)
    multiply(xg[other(t_far)], other(t_far))

    lane = lax.broadcasted_iota(jnp.int32, (half, 128), 1)
    low = lane < 64
    winq_ref[...] = acc[:, 0:256].astype(jnp.bfloat16)
    for part in range(2):
        rows = pl.ds(part * half, half)
        winvk_ref[rows, :] = jnp.where(low, acc[rows, 256:384], acc[rows, 128:256]).astype(jnp.bfloat16)
    first, second = acc[0:half, DK:DK + 128], acc[half:ROWS, DK:DK + 128]
    msg_ref[0, 0:256, :] = jnp.where(low, first, pltpu.roll(second, 64, 1)).astype(jnp.bfloat16)
    msg_ref[1, 0:256, :] = jnp.where(low, pltpu.roll(first, 64, 1), second).astype(jnp.bfloat16)
    for j in range(4):
        rows = pl.ds(j * 128, 128)
        v_t = acc[rows, DV:DV + 128].T.astype(jnp.bfloat16)
        q_t = (acc[rows, DQ:DQ + 128].T * Q_SCALE).astype(jnp.bfloat16)
        for head in range(2):
            msg_ref[head, 256 + j * 64:256 + (j + 1) * 64, :] = v_t[head * 64:(head + 1) * 64]
            msg_ref[head, 512 + j * 64:512 + (j + 1) * 64, :] = q_t[head * 64:(head + 1) * 64]
    for copy in started:
        copy.wait_send()


def project(inputs, weights):
    bf = jnp.bfloat16
    depth = weights[3].shape[0]
    return pl.pallas_call(
        project_kernel,
        out_shape=(
            jax.ShapeDtypeStruct((ROWS, 256), bf),
            jax.ShapeDtypeStruct((ROWS, 128), bf),
            jax.ShapeDtypeStruct((2, 768, 128), bf),
        ),
        in_specs=[VMEM_SPEC] + [ANY_SPEC] * 6,
        out_specs=(VMEM_SPEC,) * 3,
        scratch_shapes=[
            pltpu.VMEM((2 * NX, ROWS, ROWS), bf),
            pltpu.VMEM((320, depth), bf),
            pltpu.VMEM((depth, 128), bf),
            pltpu.VMEM((depth, 128), bf),
            pltpu.VMEM((depth, 128), bf),
            pltpu.VMEM((ROWS, ACC_COLS), jnp.float32),
            pltpu.SemaphoreType.DMA((6,)),
            pltpu.SemaphoreType.DMA((2 * NX, 2)),
            pltpu.SemaphoreType.DMA((3,)),
            pltpu.SemaphoreType.DMA((3,)),
            pltpu.SemaphoreType.DMA((8,)),
        ],
        compiler_params=pltpu.CompilerParams(
            collective_id=0, has_side_effects=True, vmem_limit_bytes=62 * 1024 * 1024
        ),
        name="project",
    )(inputs, *weights)


def exchange_kernel(
    length_ref, lam_smem, sink_ref, msg_ref, winq_ref, winvk_ref,
    kv_ref, q_ref, lamo_ref, win_ref,
    lam_ref, halo_ref, keys, v_t,
    recv_kv, recv_q, recv_lam, recv_halo, send_a, send_ring, send_sib, send_halo, local_sem,
):
    for i in range(2):
        lam_ref[i] = jnp.full((8, 128), lam_smem[i], jnp.float32)
    z, y, x, c = place()
    sp = z * NY + y
    tp = x * 2 + c
    up = (((z + 1) % NZ) * NY + y, tp)
    down = (((z + NZ - 1) % NZ) * NY + y, tp)
    sibling = (sp, x * 2 + 1 - c)
    after = ((sp + 1) % BLOCKS, tp)
    before = ((sp + BLOCKS - 1) % BLOCKS, tp)
    partners = [(z * NY + 2 * c + i, x * 2 + y // 2) for i in range(2)]
    away = [(2 * c + i) != y for i in range(2)]
    greet((up, down, sibling, after, before) + tuple(partners), (None,) * 5 + tuple(away))
    pl.semaphore_wait(pltpu.get_barrier_semaphore(), 5 + sum(a.astype(jnp.int32) for a in away))

    def remote(src, dst, send_sem, recv_sem, device):
        return pltpu.make_async_remote_copy(
            src_ref=src, dst_ref=dst, send_sem=send_sem, recv_sem=recv_sem,
            device_id=device, device_id_type=MESH,
        )

    mine = z * NY + y
    slot = y % 2
    head_copies = []
    for i in range(2):
        head_copies.append([
            remote(msg_ref.at[i, pl.ds(0, 512)], kv_ref.at[mine], send_a.at[i, 0], recv_kv.at[mine], partners[i]),
            remote(msg_ref.at[i, pl.ds(512, 256)], q_ref.at[slot], send_a.at[i, 1], recv_q.at[slot], partners[i]),
            remote(lam_ref.at[i], lamo_ref.at[slot], send_a.at[i, 2], recv_lam.at[slot], partners[i]),
        ])
        def go(i=i):
            for copy in head_copies[i]:
                copy.start()
        pl.when(away[i])(go)
        def stay(i=i):
            copies = [
                pltpu.make_async_copy(msg_ref.at[i, pl.ds(0, 512)], kv_ref.at[mine], local_sem.at[0]),
                pltpu.make_async_copy(msg_ref.at[i, pl.ds(512, 256)], q_ref.at[slot], local_sem.at[1]),
                pltpu.make_async_copy(lam_ref.at[i], lamo_ref.at[slot], local_sem.at[2]),
            ]
            for copy in copies:
                copy.start()
            for copy in copies:
                copy.wait()
        pl.when(jnp.logical_not(away[i]))(stay)
    edges = [
        remote(winvk_ref.at[pl.ds(ROWS - WINDOW, WINDOW)], halo_ref.at[0], send_halo.at[0], recv_halo.at[0], after),
        remote(winvk_ref.at[pl.ds(0, WINDOW)], halo_ref.at[1], send_halo.at[1], recv_halo.at[1], before),
    ]
    for copy in edges:
        copy.start()

    def band_setup():
        for copy in edges:
            copy.wait_recv()
        keys[0:WINDOW] = halo_ref[0]
        keys[WINDOW:WINDOW + ROWS] = winvk_ref[...]
        keys[WINDOW + ROWS:] = halo_ref[1]
        for i in range(ROWS // 128 + 2):
            pair = keys[i * 128:(i + 1) * 128].astype(jnp.float32)
            v_t[:, i * 128:(i + 1) * 128] = pair.T[0:HEAD].astype(jnp.bfloat16)

    def band(i):
        live = length_ref[0]
        q_t = winq_ref[i * 128:(i + 1) * 128].astype(jnp.float32).T * HEAD ** (-0.5)
        zero = jnp.zeros((HEAD, 128), jnp.float32)
        query = jnp.concatenate(
            [jnp.concatenate([zero, q_t[g * HEAD:(g + 1) * HEAD]], axis=0) for g in range(GROUP)], axis=1
        ).astype(jnp.bfloat16)
        s = jnp.dot(keys[i * 128:i * 128 + 384], query, preferred_element_type=jnp.float32)
        key = lax.broadcasted_iota(jnp.int32, (384, 128), 0)
        ask = lax.broadcasted_iota(jnp.int32, (384, 128), 1)
        start = sp * ROWS + (i - 1) * 128
        allowed = (
            (key - ask >= 0) & (key - ask <= 2 * WINDOW) & (start + key >= 0) & (start + key < live)
        )
        for g in range(GROUP):
            own = jnp.where(allowed, s[:, g * 128:(g + 1) * 128], masked_score)
            top = jnp.maximum(jnp.max(own, axis=0, keepdims=True), sink_ref[g])
            e = jnp.where(allowed, jnp.exp(own - top), 0.0)
            total = jnp.sum(e, axis=0, keepdims=True) + jnp.exp(sink_ref[g] - top)
            o = jnp.dot(v_t[:, i * 128:i * 128 + 384], e.astype(jnp.bfloat16), preferred_element_type=jnp.float32)
            ok = (start + 128 + lax.broadcasted_iota(jnp.int32, (HEAD, 128), 1)) < live
            o = jnp.where(ok, o / total, 0.0)
            both = jnp.concatenate([o, jnp.zeros_like(o)], axis=0).T
            win_ref[i * 128:(i + 1) * 128, g * HEAD:(g + 1) * HEAD] = both[:, 0:HEAD].astype(jnp.bfloat16)

    started = []

    def block(zz, s, core):
        return ((zz + NZ) % NZ) * NY + 2 * core + s

    def forward(b, device, sem):
        copy = remote(kv_ref.at[b], kv_ref.at[b], sem, recv_kv.at[b], device)
        copy.start()
        started.append(copy)

    def arrive(b):
        remote(kv_ref.at[b], kv_ref.at[b], send_sib.at[0], recv_kv.at[b], sibling).wait_recv()

    for s in range(2):
        b = block(z, s, c)
        pl.when(away[s])(lambda: arrive(b))
        forward(b, up, send_ring.at[0, s, 0])
        forward(b, down, send_ring.at[1, s, 0])
        forward(b, sibling, send_sib.at[s])
    count = 2
    for d in range(1, 5):
        for s in range(2):
            for way, (reach, device, sign) in enumerate(((4 - s, up, -1), (3 + s, down, 1))):
                if d > reach:
                    continue
                b = block(z + sign * d, s, c)
                arrive(b)
                if d < reach:
                    forward(b, device, send_ring.at[way, s, d])
                forward(b, sibling, send_sib.at[count])
                count += 1
        if d == 1:
            band_setup()
            band(0)
        elif d == 2:
            band(1)
            band(2)
        elif d == 3:
            band(3)
    for i in range(2):
        pl.when(away[i])(lambda i=i: [
            remote(msg_ref.at[0, pl.ds(512, 256)], q_ref.at[i], send_a.at[0, 1], recv_q.at[i], sibling).wait_recv(),
            remote(lam_ref.at[0], lamo_ref.at[i], send_a.at[0, 2], recv_lam.at[i], sibling).wait_recv(),
        ] and None)
    for zz in range(NZ):
        for s in range(2):
            arrive(block(zz, s, 1 - c))
    for copy in started + edges:
        copy.wait_send()
    for i in range(2):
        pl.when(away[i])(lambda i=i: [copy.wait_send() for copy in head_copies[i]] and None)


def exchange(length, mix_lambda, sink_logit, msg, winq, winvk):
    bf = jnp.bfloat16
    return pl.pallas_call(
        exchange_kernel,
        out_shape=(
            jax.ShapeDtypeStruct((BLOCKS, ROWS, 128), bf),
            jax.ShapeDtypeStruct((2, 256, 128), bf),
            jax.ShapeDtypeStruct((2, 8, 128), jnp.float32),
            jax.ShapeDtypeStruct((ROWS, GROUP * HEAD), bf),
        ),
        in_specs=[SMEM_SPEC] * 3 + [VMEM_SPEC] * 3,
        out_specs=(VMEM_SPEC,) * 4,
        scratch_shapes=[
            pltpu.VMEM((2, 8, 128), jnp.float32),
            pltpu.VMEM((2, WINDOW, 128), bf),
            pltpu.VMEM((ROWS + 2 * WINDOW, 128), bf),
            pltpu.VMEM((HEAD, ROWS + 2 * WINDOW), bf),
            pltpu.SemaphoreType.DMA((BLOCKS,)),
            pltpu.SemaphoreType.DMA((2,)),
            pltpu.SemaphoreType.DMA((2,)),
            pltpu.SemaphoreType.DMA((2,)),
            pltpu.SemaphoreType.DMA((2, 3)),
            pltpu.SemaphoreType.DMA((2, 2, 4)),
            pltpu.SemaphoreType.DMA((16,)),
            pltpu.SemaphoreType.DMA((2,)),
            pltpu.SemaphoreType.DMA((3,)),
        ],
        compiler_params=pltpu.CompilerParams(
            collective_id=1, has_side_effects=True, vmem_limit_bytes=32 * 1024 * 1024
        ),
        name="exchange",
    )(length, mix_lambda, sink_logit, msg, winq, winvk)


NQ = 2 * ROWS
TILE = 1024
UNITS = [(n, h) for n in range(2 * NQ // TILE) for h in range(2)]


def attend_kernel(length_ref, kv_ref, q_ref, lam_ref, gain_ref, o_ref, qz, va, acc, s_buf, m_buf):
    live = length_ref[0]
    z, y, x, c = place()
    first = (z * NY + 2 * c) * ROWS
    count = jnp.where(first < live, (live + ROWS - 1) // ROWS, 0)
    qz[...] = jnp.zeros_like(qz)
    for t in range(NQ // 128):
        q = q_ref[t // 4, (t % 4) * 64:(t % 4 + 1) * 64, :]
        for h in range(2):
            for m in range(2):
                qz[h, h * 64 + m * 32:h * 64 + (m + 1) * 32, m * NQ + t * 128:m * NQ + (t + 1) * 128] = (
                    q[m * 32:(m + 1) * 32]
                )
    acc[...] = jnp.zeros_like(acc)
    va[...] = jnp.zeros_like(va)

    def values(b):
        lane = lax.broadcasted_iota(jnp.int32, (64, 128), 1)
        row = lax.broadcasted_iota(jnp.int32, (16, 128), 0)
        for j in range(4):
            ok = (b * ROWS + j * 128 + lane) < live
            v = kv_ref[b, 256 + j * 64:256 + (j + 1) * 64, :].astype(jnp.float32)
            va[0:64, j * 128:(j + 1) * 128] = jnp.where(ok, v, 0.0).astype(jnp.bfloat16)
            va[64:80, j * 128:(j + 1) * 128] = jnp.where(ok[:16] & (row == 0), 1.0, 0.0).astype(jnp.bfloat16)

    def scores(b, n, h):
        return jnp.dot(
            kv_ref[b, 0:256, :], qz[h, :, n * TILE:(n + 1) * TILE], preferred_element_type=jnp.float32
        )

    def gather(n, h, weight):
        acc[:, n * TILE:(n + 1) * TILE] += jnp.dot(
            va[:, h * 256:(h + 1) * 256], weight, preferred_element_type=jnp.float32
        )

    s_buf[0] = scores(0, *UNITS[0])

    def step(b, carry):
        values(b)
        for i, (n, h) in enumerate(UNITS):
            s = s_buf[i % 2]
            if i + 1 < len(UNITS):
                s_buf[1 - i % 2] = scores(b, *UNITS[i + 1])
            else:
                s_buf[1 - i % 2] = scores(jnp.minimum(b + 1, BLOCKS - 1), *UNITS[0])
            gather(n, h, jnp.exp2(s).astype(jnp.bfloat16))
        return carry

    lax.fori_loop(0, count, step, 0)

    sums = acc[64:65, :]
    fine = (sums > 2.0 ** -80) & (sums < 2.0 ** 100)
    fine_all = jnp.min(jnp.where(fine, 1.0, 0.0)) > 0.5

    @pl.when((count > 0) & jnp.logical_not(fine_all))
    def _():
        m_buf[...] = jnp.full_like(m_buf, masked_score)
        acc[...] = jnp.zeros_like(acc)

        def masked(b, n, h):
            key = b * ROWS + h * 256 + lax.broadcasted_iota(jnp.int32, (256, TILE), 0)
            return jnp.where(key < live, scores(b, n, h), masked_score)

        def maxima(b, carry):
            for n, h in UNITS:
                cols = slice(n * TILE, (n + 1) * TILE)
                m_buf[0:1, cols] = jnp.maximum(
                    m_buf[0:1, cols], jnp.max(masked(b, n, h), axis=0, keepdims=True)
                )
            return carry

        def again(b, carry):
            values(b)
            for n, h in UNITS:
                s = masked(b, n, h) - m_buf[0:1, n * TILE:(n + 1) * TILE]
                gather(n, h, jnp.exp2(s).astype(jnp.bfloat16))
            return carry

        lax.fori_loop(0, count, maxima, 0)
        lax.fori_loop(0, count, again, 0)

    row = gain_ref[...]
    gain = jnp.broadcast_to(jnp.concatenate([row, row], axis=1), (128, 128)).T[0:HEAD]
    lam = lam_ref[0, 0:1, :]
    for t in range(NQ // 128):
        maps = []
        for m in range(2):
            cols = slice(m * NQ + t * 128, m * NQ + (t + 1) * 128)
            total = acc[64:65, cols]
            maps.append(acc[0:64, cols] / jnp.where(total > 0.0, total, 1.0))
        mixed = maps[0] - lam * maps[1]
        normed = mixed * lax.rsqrt(jnp.mean(mixed * mixed, axis=0, keepdims=True) + epsilon) * gain
        ok = (first + t * 128 + lax.broadcasted_iota(jnp.int32, (64, 128), 1)) < live
        o_ref[t // 4, (t % 4) * 64:(t % 4 + 1) * 64, :] = jnp.where(ok, normed, 0.0).astype(jnp.bfloat16)


def attend(length, kv, q, lam, gain):
    return pl.pallas_call(
        attend_kernel,
        out_shape=jax.ShapeDtypeStruct((2, 256, 128), jnp.bfloat16),
        in_specs=[SMEM_SPEC] + [VMEM_SPEC] * 4,
        out_specs=VMEM_SPEC,
        scratch_shapes=[
            pltpu.VMEM((2, 128, 2 * NQ), jnp.bfloat16),
            pltpu.VMEM((80, ROWS), jnp.bfloat16),
            pltpu.VMEM((80, 2 * NQ), jnp.float32),
            pltpu.VMEM((2, 256, TILE), jnp.float32),
            pltpu.VMEM((8, 2 * NQ), jnp.float32),
        ],
        compiler_params=pltpu.CompilerParams(vmem_limit_bytes=48 * 1024 * 1024),
        name="attend",
    )(length, kv, q, lam, gain)


CHUNK = 1024
SHARE = ROWS // (2 * NX)


def merge_kernel(
    o_ref, win_ref, wo_ref, do_ref, out_ref,
    rows_t, diff_rows, lhs_w, lhs_d, total, give, take, mine, far_in, joined, fin,
    recv_o, send_o, local_sem, send_g, recv_g, send_f, recv_f, send_n, recv_n,
):
    z, y, x, c = place()
    sp = z * NY + y
    right = (sp, ((x + 1) % NX) * 2 + c)
    left = (sp, ((x + NX - 1) % NX) * 2 + c)
    sibling = (sp, x * 2 + 1 - c)
    partners = [(z * NY + 2 * c + i, x * 2 + y // 2) for i in range(2)]
    away = [(2 * c + i) != y for i in range(2)]
    greet((right, left, sibling) + tuple(partners), (None,) * 3 + tuple(away))
    pl.semaphore_wait(pltpu.get_barrier_semaphore(), 3 + sum(a.astype(jnp.int32) for a in away))

    def remote(src, dst, send_sem, recv_sem, device):
        return pltpu.make_async_remote_copy(
            src_ref=src, dst_ref=dst, send_sem=send_sem, recv_sem=recv_sem,
            device_id=device, device_id_type=MESH,
        )

    slot = y % 2
    back = [remote(o_ref.at[i], rows_t.at[slot], send_o.at[i], recv_o.at[slot], partners[i]) for i in range(2)]
    for i in range(2):
        pl.when(away[i])(lambda i=i: back[i].start())
        def stay(i=i):
            copy = pltpu.make_async_copy(o_ref.at[i], rows_t.at[slot], local_sem)
            copy.start()
            copy.wait()
        pl.when(jnp.logical_not(away[i]))(stay)

    def rows_of(side, r):
        core = c if side else 1 - c
        return pl.ds(pl.multiple_of(((x + r) % NX) * 2 * SHARE + core * SHARE, SHARE), SHARE)

    for side in range(2):
        for r in range(NX):
            lhs_w[side, r * SHARE:(r + 1) * SHARE] = win_ref[rows_of(side, r)]

    def banded(k, carry):
        cols = pl.ds(pl.multiple_of(k * 512, 512), 512)
        weight = wo_ref[:, cols]
        for side in range(2):
            total[side, :, cols] = jnp.dot(lhs_w[side], weight, preferred_element_type=jnp.float32)
        return carry

    lax.fori_loop(0, 8, banded, 0)
    for i in range(2):
        def wait(i=i):
            remote(o_ref.at[i], rows_t.at[i], send_o.at[i], recv_o.at[i], partners[i]).wait_recv()
        pl.when(away[i])(wait)
    for j in range(4):
        pair = jnp.concatenate(
            [rows_t[0, j * 64:(j + 1) * 64], rows_t[1, j * 64:(j + 1) * 64]], axis=0
        ).astype(jnp.float32)
        diff_rows[j * 128:(j + 1) * 128] = pair.T.astype(jnp.bfloat16)
    for side in range(2):
        for r in range(NX):
            lhs_d[side, r * SHARE:(r + 1) * SHARE] = diff_rows[rows_of(side, r)]

    started = []

    def go(copy):
        copy.start()
        started.append(copy)
        return copy

    order = (0, 2, 1, 3)

    def partial(side, k):
        cols = slice(k * CHUNK, (k + 1) * CHUNK)
        return total[side, :, cols] + jnp.dot(lhs_d[side], do_ref[:, cols], preferred_element_type=jnp.float32)

    for k in order:
        give[k] = partial(0, k).astype(jnp.bfloat16)
        go(remote(give.at[k], take.at[k], send_g.at[k], recv_g.at[k], sibling))
    for k in order:
        own = partial(1, k)
        remote(give.at[k], take.at[k], send_g.at[k], recv_g.at[k], sibling).wait_recv()
        both = (own + take[k].astype(jnp.float32)).astype(jnp.bfloat16)
        for r in range(NX):
            mine[r, k] = both[r * SHARE:(r + 1) * SHARE]
        go(remote(mine.at[2, k], far_in.at[k], send_f.at[k], recv_f.at[k], right if k < 2 else left))

    def near(src, k, way):
        return remote(src, fin.at[way, k], send_n.at[way, k], recv_n.at[way, k], left if way else right)

    for i in range(2):
        go(near(mine.at[1, 2 + i], 2 + i, 0))
        go(near(mine.at[3, i], i, 1))
    for k in order:
        way = 0 if k < 2 else 1
        remote(mine.at[2, k], far_in.at[k], send_f.at[k], recv_f.at[k], right).wait_recv()
        joined[k] = (
            mine[3 if way else 1, k].astype(jnp.float32) + far_in[k].astype(jnp.float32)
        ).astype(jnp.bfloat16)
        go(near(joined.at[k], k, way))
    for k in order:
        near(joined.at[k], k, 0).wait_recv()
        near(joined.at[k], k, 1).wait_recv()
        value = mine[0, k].astype(jnp.float32) + fin[0, k].astype(jnp.float32) + fin[1, k].astype(jnp.float32)
        out_ref[:, k * CHUNK:(k + 1) * CHUNK] = value.astype(jnp.bfloat16)
    for copy in started:
        copy.wait_send()
    for i in range(2):
        pl.when(away[i])(lambda i=i: back[i].wait_send())


def merge(o, win_rows, win_out, diff_out):
    bf = jnp.bfloat16
    width = win_out.shape[1]
    chunks = width // CHUNK
    half = ROWS // 2
    return pl.pallas_call(
        merge_kernel,
        out_shape=jax.ShapeDtypeStruct((SHARE, width), bf),
        in_specs=[VMEM_SPEC] * 4,
        out_specs=VMEM_SPEC,
        scratch_shapes=[
            pltpu.VMEM((2, 256, 128), bf),
            pltpu.VMEM((ROWS, 128), bf),
            pltpu.VMEM((2, half, GROUP * HEAD), bf),
            pltpu.VMEM((2, half, 128), bf),
            pltpu.VMEM((2, half, width), jnp.float32),
            pltpu.VMEM((chunks, half, CHUNK), bf),
            pltpu.VMEM((chunks, half, CHUNK), bf),
            pltpu.VMEM((NX, chunks, SHARE, CHUNK), bf),
            pltpu.VMEM((chunks, SHARE, CHUNK), bf),
            pltpu.VMEM((chunks, SHARE, CHUNK), bf),
            pltpu.VMEM((2, chunks, SHARE, CHUNK), bf),
            pltpu.SemaphoreType.DMA((2,)),
            pltpu.SemaphoreType.DMA((2,)),
            pltpu.SemaphoreType.DMA,
            pltpu.SemaphoreType.DMA((chunks,)),
            pltpu.SemaphoreType.DMA((chunks,)),
            pltpu.SemaphoreType.DMA((chunks,)),
            pltpu.SemaphoreType.DMA((chunks,)),
            pltpu.SemaphoreType.DMA((2, chunks)),
            pltpu.SemaphoreType.DMA((2, chunks)),
        ],
        compiler_params=pltpu.CompilerParams(
            collective_id=2, has_side_effects=True, vmem_limit_bytes=40 * 1024 * 1024
        ),
        name="merge",
    )(o, win_rows, win_out, diff_out)


def body(
    inputs, length, win_query, win_key, win_value, sink_logit,
    diff_query, diff_key, diff_value, mix_lambda, head_gain, win_out, diff_out,
):
    weights = (win_query.T, win_key.T, win_value.T, diff_query, diff_key, diff_value)
    winq, winvk, msg = project(inputs, weights)
    kv, q, lam, win_rows = exchange(length, mix_lambda, sink_logit, msg, winq, winvk)
    rows = attend(length, kv, q, lam, head_gain.reshape(1, HEAD))
    return merge(rows, win_rows, win_out, diff_out)


def solution(mesh):
    placed = (
        P("sp", "tp"), P(), P(None, "tp"), P(None, "tp"), P(None, "tp"), P("tp"), P(None, "tp"),
        P(None, "tp"), P(None, "tp"), P("tp"), P(), P("tp", None), P("tp", None),
    )
    return jax.shard_map(
        body, mesh=mesh, in_specs=placed, out_specs=P(("sp", "tp"), None), check_vma=False
    )
```

```python
import functools

import jax
import jax.numpy as jnp
from jax import lax
from jax.experimental import pallas as pl
from jax.experimental.pallas import tpu as pltpu
from jax.sharding import PartitionSpec as P

HEAD = 64
DQK = 32
GROUP = 3
WINDOW = 128
NX, NY, NZ = 4, 4, 8
ROWS = 512
BLOCKS = NY * NZ
FRONT_VMEM = 62 * 1024 * 1024
ATTEND_VMEM = 60 * 1024 * 1024
Q_SCALE = 1.4426950408889634 * DQK ** (-0.5)
MESH = pl.DeviceIdType.MESH

epsilon = 1e-06
masked_score = -1e30
VMEM_SPEC = pl.BlockSpec(memory_space=pltpu.VMEM)
SMEM_SPEC = pl.BlockSpec(memory_space=pltpu.SMEM)
HBM_SPEC = pl.BlockSpec(memory_space=pltpu.HBM)


def place():
    sp, tp = lax.axis_index("sp"), lax.axis_index("tp")
    return sp // NY, sp % NY, tp // 2, tp % 2


def greet(devices, conditions=None):
    barrier = pltpu.get_barrier_semaphore()
    for i, device in enumerate(devices):
        def signal(device=device):
            pl.semaphore_signal(barrier, inc=1, device_id=device, device_id_type=MESH)
        if conditions is None or conditions[i] is None:
            signal()
        else:
            pl.when(conditions[i])(signal)


WQ, DQ, DK, DV, ACC_COLS = 0, 384, 512, 640, 768
QUARTER = ROWS // 4
HALF = ROWS // 2


def front_kernel(
    length_ref, lam_smem, sink_ref, x_ref, wq_hbm, wk_hbm, wv_hbm, dq_hbm, dk_hbm, dv_hbm,
    kv_ref, q_ref, lamo_ref, win_ref,
    xg, wt, dq, dk, dv, acc, msg, lam_ref, halo_ref, winq, keys, v_t,
    w_sem, recv_x, send_xr, send_xl, send_xs,
    recv_kv, recv_q, recv_lam, recv_halo, send_a, send_lam, send_ring, send_sib, send_halo, local_sem,
):
    z, y, x, c = place()
    sp = z * NY + y
    tp = x * 2 + c
    right = (sp, ((x + 1) % NX) * 2 + c)
    left = (sp, ((x + NX - 1) % NX) * 2 + c)
    sibling = (sp, x * 2 + 1 - c)
    up = (((z + 1) % NZ) * NY + y, tp)
    down = (((z + NZ - 1) % NZ) * NY + y, tp)
    after = ((sp + 1) % BLOCKS, tp)
    before = ((sp + BLOCKS - 1) % BLOCKS, tp)
    partners = [(z * NY + 2 * c + i, x * 2 + y // 2) for i in range(2)]
    away = [(2 * c + i) != y for i in range(2)]

    loads = [
        pltpu.make_async_copy(src, dst, w_sem.at[i])
        for i, (src, dst) in enumerate(
            (
                (wq_hbm, wt.at[pl.ds(0, 192)]),
                (wk_hbm, wt.at[pl.ds(192, 64)]),
                (wv_hbm, wt.at[pl.ds(256, 64)]),
                (dq_hbm, dq),
                (dk_hbm, dk),
                (dv_hbm, dv),
            )
        )
    ]
    for load in loads:
        load.start()
    for i in range(2):
        lam_ref[i] = jnp.full((8, 128), lam_smem[i], jnp.float32)
    greet(
        (right, left, sibling, up, down, after, before) + tuple(partners), (None,) * 7 + tuple(away)
    )
    pl.semaphore_wait(pltpu.get_barrier_semaphore(), 7 + sum(a.astype(jnp.int32) for a in away))

    started = []

    def remote(src, dst, send_sem, recv_sem, device):
        return pltpu.make_async_remote_copy(
            src_ref=src, dst_ref=dst, send_sem=send_sem, recv_sem=recv_sem,
            device_id=device, device_id_type=MESH,
        )

    def go(copy):
        copy.start()
        started.append(copy)

    def send_x(own, t, q, device, sem):
        rows = pl.ds(q * QUARTER, QUARTER)
        go(remote(x_ref.at[rows] if own else xg.at[t, rows], xg.at[t, rows], sem, recv_x.at[t, q], device))

    def arrive_x(t, q):
        rows = pl.ds(q * QUARTER, QUARTER)
        remote(xg.at[t, rows], xg.at[t, rows], send_xr.at[0], recv_x.at[t, q], sibling).wait_recv()

    t_left = ((x + NX - 1) % NX) * 2 + c
    t_right = ((x + 1) % NX) * 2 + c
    t_far = ((x + 2) % NX) * 2 + c

    def other(t):
        return t + 1 - 2 * c

    def multiply(own, t, h):
        rows = pl.ds(h * HALF, HALF)
        block = x_ref[rows] if own else xg[t, rows]
        ks = pl.ds(pl.multiple_of(t * ROWS, ROWS), ROWS)
        acc[rows, WQ:WQ + 320] += lax.dot_general(
            block, wt[:, ks], (((1,), (1,)), ((), ())), preferred_element_type=jnp.float32
        )
        both = jnp.concatenate([dq[ks, :], dk[ks, :]], axis=1)
        acc[rows, DQ:DQ + 256] += jnp.dot(block, both, preferred_element_type=jnp.float32)
        acc[rows, DV:DV + 128] += jnp.dot(block, dv[ks, :], preferred_element_type=jnp.float32)

    def multiply_other(t, h):
        for q in (2 * h, 2 * h + 1):
            arrive_x(other(t), q)
        multiply(False, other(t), h)

    def receive_x(t, q, sem):
        arrive_x(t, q)
        send_x(False, t, q, sibling, sem)

    lane = lax.broadcasted_iota(jnp.int32, (QUARTER, 128), 1)
    low = lane < 64
    mine = sp
    slot = y % 2

    def head_copies(i, u):
        return [
            remote(msg.at[i, u, pl.ds(0, 256)], kv_ref.at[mine, u], send_a.at[i, u, 0], recv_kv.at[mine, u], partners[i]),
            remote(msg.at[i, u, pl.ds(256, 128)], q_ref.at[slot, u], send_a.at[i, u, 1], recv_q.at[slot, u], partners[i]),
        ]

    def lam_copy(i):
        return remote(lam_ref.at[i], lamo_ref.at[slot], send_lam.at[i], recv_lam.at[slot], partners[i])

    edges = [
        remote(keys.at[pl.ds(WINDOW, WINDOW)], halo_ref.at[1], send_halo.at[1], recv_halo.at[1], before),
        remote(keys.at[pl.ds(ROWS, WINDOW)], halo_ref.at[0], send_halo.at[0], recv_halo.at[0], after),
    ]

    def pack(u):
        rows = pl.ds(u * HALF, HALF)
        first, second = pl.ds(u * HALF, QUARTER), pl.ds(u * HALF + QUARTER, QUARTER)
        k0, k1 = acc[first, DK:DK + 128], acc[second, DK:DK + 128]
        msg[0, u, 0:128] = jnp.where(low, k0, pltpu.roll(k1, 64, 1)).astype(jnp.bfloat16)
        msg[1, u, 0:128] = jnp.where(low, pltpu.roll(k0, 64, 1), k1).astype(jnp.bfloat16)
        for j, part in enumerate((first, second)):
            turned = acc[part, DV:DV + 128].T.astype(jnp.bfloat16)
            asked = (acc[part, DQ:DQ + 128].T * Q_SCALE).astype(jnp.bfloat16)
            for head in range(2):
                msg[head, u, 128 + j * 64:128 + (j + 1) * 64] = turned[head * 64:(head + 1) * 64]
                msg[head, u, 256 + j * 64:256 + (j + 1) * 64] = asked[head * 64:(head + 1) * 64]
            keys[pl.ds(WINDOW + u * HALF + j * QUARTER, QUARTER)] = jnp.where(
                low, acc[part, 256:384], acc[part, 128:256]
            ).astype(jnp.bfloat16)
        for i in range(2):
            def leave(i=i):
                for copy in head_copies(i, u):
                    copy.start()
            pl.when(away[i])(leave)
            def stay(i=i):
                copies = [
                    pltpu.make_async_copy(msg.at[i, u, pl.ds(0, 256)], kv_ref.at[mine, u], local_sem.at[0]),
                    pltpu.make_async_copy(msg.at[i, u, pl.ds(256, 128)], q_ref.at[slot, u], local_sem.at[1]),
                ]
                for copy in copies:
                    copy.start()
                for copy in copies:
                    copy.wait()
            pl.when(jnp.logical_not(away[i]))(stay)
        edges[u].start()
        winq[rows] = acc[rows, 0:256].astype(jnp.bfloat16)

    def block(zz, s, core):
        return ((zz + NZ) % NZ) * NY + 2 * core + s

    def forward(b, u, device, sem):
        go(remote(kv_ref.at[b, u], kv_ref.at[b, u], sem, recv_kv.at[b, u], device))

    def arrive(b, u):
        remote(kv_ref.at[b, u], kv_ref.at[b, u], send_sib.at[0, 0], recv_kv.at[b, u], sibling).wait_recv()

    def open_ring(u):
        for s in range(2):
            b = block(z, s, c)
            pl.when(away[s])(lambda: arrive(b, u))
            forward(b, u, up, send_ring.at[0, s, u, 0])
            forward(b, u, down, send_ring.at[1, s, u, 0])
            forward(b, u, sibling, send_sib.at[s, u])

    shared = [2, 2]

    def ring(u, d):
        for s in range(2):
            for way, (reach, device, sign) in enumerate(((4 - s, up, -1), (3 + s, down, 1))):
                if d > reach:
                    continue
                b = block(z + sign * d, s, c)
                arrive(b, u)
                if d < reach:
                    forward(b, u, device, send_ring.at[way, s, u, d])
                forward(b, u, sibling, send_sib.at[shared[u], u])
                shared[u] += 1

    def band_setup():
        for copy in edges:
            copy.wait_recv()
        keys[0:WINDOW] = halo_ref[0]
        keys[WINDOW + ROWS:] = halo_ref[1]
        for i in range(ROWS // 128 + 2):
            pair = keys[i * 128:(i + 1) * 128].astype(jnp.float32)
            v_t[:, i * 128:(i + 1) * 128] = pair.T[0:HEAD].astype(jnp.bfloat16)

    def band(i):
        live = length_ref[0]
        q_t = winq[i * 128:(i + 1) * 128].astype(jnp.float32).T * HEAD ** (-0.5)
        zero = jnp.zeros((HEAD, 128), jnp.float32)
        query = jnp.concatenate(
            [jnp.concatenate([zero, q_t[g * HEAD:(g + 1) * HEAD]], axis=0) for g in range(GROUP)], axis=1
        ).astype(jnp.bfloat16)
        s = jnp.dot(keys[i * 128:i * 128 + 384], query, preferred_element_type=jnp.float32)
        key = lax.broadcasted_iota(jnp.int32, (384, 128), 0)
        ask = lax.broadcasted_iota(jnp.int32, (384, 128), 1)
        start = sp * ROWS + (i - 1) * 128
        allowed = (
            (key - ask >= 0) & (key - ask <= 2 * WINDOW) & (start + key >= 0) & (start + key < live)
        )
        for g in range(GROUP):
            own = jnp.where(allowed, s[:, g * 128:(g + 1) * 128], masked_score)
            top = jnp.maximum(jnp.max(own, axis=0, keepdims=True), sink_ref[g])
            e = jnp.where(allowed, jnp.exp(own - top), 0.0)
            total = jnp.sum(e, axis=0, keepdims=True) + jnp.exp(sink_ref[g] - top)
            o = jnp.dot(v_t[:, i * 128:i * 128 + 384], e.astype(jnp.bfloat16), preferred_element_type=jnp.float32)
            ok = (start + 128 + lax.broadcasted_iota(jnp.int32, (HEAD, 128), 1)) < live
            o = jnp.where(ok, o / total, 0.0)
            both = jnp.concatenate([o, jnp.zeros_like(o)], axis=0).T
            win_ref[i * 128:(i + 1) * 128, g * HEAD:(g + 1) * HEAD] = both[:, 0:HEAD].astype(jnp.bfloat16)

    for q in range(2):
        send_x(True, tp, q, right, send_xr.at[q])
        send_x(True, tp, q, left, send_xl.at[q])
    for q in range(4):
        send_x(True, tp, q, sibling, send_xs.at[q])
    acc[...] = jnp.zeros_like(acc)
    for i in range(2):
        pl.when(away[i])(lambda i=i: lam_copy(i).start())
        def keep(i=i):
            copy = pltpu.make_async_copy(lam_ref.at[i], lamo_ref.at[slot], local_sem.at[2])
            copy.start()
            copy.wait()
        pl.when(jnp.logical_not(away[i]))(keep)
    for load in loads:
        load.wait()
    multiply(True, tp, 0)
    receive_x(t_left, 0, send_xs.at[4])
    send_x(False, t_left, 0, right, send_xr.at[2])
    for q in (2, 3):
        send_x(True, tp, q, right, send_xr.at[q + 1])
    receive_x(t_right, 0, send_xs.at[5])
    multiply(True, tp, 1)
    receive_x(t_right, 1, send_xs.at[6])
    send_x(False, t_right, 1, left, send_xl.at[2])
    for q in (2, 3):
        send_x(True, tp, q, left, send_xl.at[q + 1])
    receive_x(t_left, 1, send_xs.at[7])
    multiply_other(tp, 0)
    multiply_other(tp, 1)
    multiply(False, t_left, 0)
    multiply(False, t_right, 0)
    multiply_other(t_left, 0)
    multiply_other(t_right, 0)
    receive_x(t_far, 0, send_xs.at[8])
    receive_x(t_far, 1, send_xs.at[9])
    multiply(False, t_far, 0)
    multiply_other(t_far, 0)
    pack(0)
    receive_x(t_left, 2, send_xs.at[10])
    send_x(False, t_left, 2, right, send_xr.at[5])
    receive_x(t_right, 2, send_xs.at[11])
    receive_x(t_right, 3, send_xs.at[12])
    send_x(False, t_right, 3, left, send_xl.at[5])
    receive_x(t_left, 3, send_xs.at[13])
    open_ring(0)
    multiply(False, t_left, 1)
    multiply(False, t_right, 1)
    multiply_other(t_left, 1)
    multiply_other(t_right, 1)
    receive_x(t_far, 2, send_xs.at[14])
    receive_x(t_far, 3, send_xs.at[15])
    multiply(False, t_far, 1)
    ring(0, 1)
    multiply_other(t_far, 1)
    pack(1)
    ring(0, 2)
    open_ring(1)
    ring(0, 3)
    ring(1, 1)
    band_setup()
    band(0)
    ring(0, 4)
    band(1)
    ring(1, 2)
    band(2)
    ring(1, 3)
    band(3)
    ring(1, 4)
    for i in range(2):
        def rest(i=i):
            for u in range(2):
                remote(
                    msg.at[0, u, pl.ds(256, 128)], q_ref.at[i, u], send_a.at[0, u, 1], recv_q.at[i, u], sibling
                ).wait_recv()
            remote(lam_ref.at[0], lamo_ref.at[i], send_lam.at[0], recv_lam.at[i], sibling).wait_recv()
        pl.when(away[i])(rest)
    for u in range(2):
        for zz in range(NZ):
            for s in range(2):
                arrive(block(zz, s, 1 - c), u)
    for copy in started + edges:
        copy.wait_send()
    for i in range(2):
        def sent(i=i):
            for u in range(2):
                for copy in head_copies(i, u):
                    copy.wait_send()
            lam_copy(i).wait_send()
        pl.when(away[i])(sent)


def front(length, mix_lambda, sink_logit, inputs, weights):
    bf = jnp.bfloat16
    depth = weights[3].shape[0]
    dma = pltpu.SemaphoreType.DMA
    return pl.pallas_call(
        front_kernel,
        out_shape=(
            jax.ShapeDtypeStruct((BLOCKS, 2, HALF, 128), bf),
            jax.ShapeDtypeStruct((2, 2, 128, 128), bf),
            jax.ShapeDtypeStruct((2, 8, 128), jnp.float32),
            jax.ShapeDtypeStruct((ROWS, GROUP * HEAD), bf),
        ),
        in_specs=[SMEM_SPEC] * 3 + [VMEM_SPEC] + [HBM_SPEC] * 6,
        out_specs=(VMEM_SPEC,) * 4,
        scratch_shapes=[
            pltpu.VMEM((2 * NX, ROWS, ROWS), bf),
            pltpu.VMEM((320, depth), bf),
            pltpu.VMEM((depth, 128), bf),
            pltpu.VMEM((depth, 128), bf),
            pltpu.VMEM((depth, 128), bf),
            pltpu.VMEM((ROWS, ACC_COLS), jnp.float32),
            pltpu.VMEM((2, 2, 384, 128), bf),
            pltpu.VMEM((2, 8, 128), jnp.float32),
            pltpu.VMEM((2, WINDOW, 128), bf),
            pltpu.VMEM((ROWS, 256), bf),
            pltpu.VMEM((ROWS + 2 * WINDOW, 128), bf),
            pltpu.VMEM((HEAD, ROWS + 2 * WINDOW), bf),
            dma((6,)), dma((2 * NX, 4)), dma((6,)), dma((6,)), dma((16,)),
            dma((BLOCKS, 2)), dma((2, 2)), dma((2,)), dma((2,)),
            dma((2, 2, 2)), dma((2,)), dma((2, 2, 2, 4)), dma((16, 2)), dma((2,)), dma((3,)),
        ],
        compiler_params=pltpu.CompilerParams(
            collective_id=0, has_side_effects=True, vmem_limit_bytes=FRONT_VMEM
        ),
        name="front",
    )(length, mix_lambda, sink_logit, inputs, *weights)


NQ = 2 * ROWS
TILE = 1024
UNITS = [(n, h) for n in range(2 * NQ // TILE) for h in range(2)]


def attend_kernel(length_ref, kv_hbm, q_ref, lam_ref, gain_ref, o_ref, kv_ref, qz, va, acc, s_buf, m_buf, kv_sem):
    live = length_ref[0]
    z, y, x, c = place()
    first = (z * NY + 2 * c) * ROWS
    count = jnp.where(first < live, (live + ROWS - 1) // ROWS, 0)

    def load(b):
        return pltpu.make_async_copy(kv_hbm.at[b], kv_ref.at[b], kv_sem.at[b])

    def load_start(b, carry):
        load(b).start()
        return carry

    def load_wait(b, carry):
        load(b).wait()
        return carry

    lax.fori_loop(0, BLOCKS, load_start, 0)
    qz[...] = jnp.zeros_like(qz)
    for t in range(NQ // 128):
        q = q_ref[t // 4, t % 4 // 2, (t % 2) * 64:(t % 2 + 1) * 64, :]
        for h in range(2):
            for m in range(2):
                qz[h, h * 64 + m * 32:h * 64 + (m + 1) * 32, m * NQ + t * 128:m * NQ + (t + 1) * 128] = (
                    q[m * 32:(m + 1) * 32]
                )
    acc[...] = jnp.zeros_like(acc)
    va[...] = jnp.zeros_like(va)

    def values(b):
        lane = lax.broadcasted_iota(jnp.int32, (64, 128), 1)
        row = lax.broadcasted_iota(jnp.int32, (16, 128), 0)
        for h in range(2):
            for u in range(2):
                at = h * 256 + u * 128
                ok = (b * ROWS + u * HALF + h * 128 + lane) < live
                v = kv_ref[b, u, 128 + h * 64:128 + (h + 1) * 64, :].astype(jnp.float32)
                va[0:64, at:at + 128] = jnp.where(ok, v, 0.0).astype(jnp.bfloat16)
                va[64:80, at:at + 128] = jnp.where(ok[:16] & (row == 0), 1.0, 0.0).astype(jnp.bfloat16)

    def scores(b, n, h):
        k = jnp.concatenate([kv_ref[b, 0, 0:128, :], kv_ref[b, 1, 0:128, :]], axis=0)
        return jnp.dot(k, qz[h, :, n * TILE:(n + 1) * TILE], preferred_element_type=jnp.float32)

    def gather(n, h, weight):
        acc[:, n * TILE:(n + 1) * TILE] += jnp.dot(
            va[:, h * 256:(h + 1) * 256], weight, preferred_element_type=jnp.float32
        )

    load(0).wait()
    s_buf[0] = scores(0, *UNITS[0])

    def step(b, carry):
        pl.when(b + 1 < BLOCKS)(lambda: load(b + 1).wait())
        values(b)
        for i, (n, h) in enumerate(UNITS):
            s = s_buf[i % 2]
            if i + 1 < len(UNITS):
                s_buf[1 - i % 2] = scores(b, *UNITS[i + 1])
            else:
                s_buf[1 - i % 2] = scores(jnp.minimum(b + 1, BLOCKS - 1), *UNITS[0])
            gather(n, h, jnp.exp2(s).astype(jnp.bfloat16))
        return carry

    lax.fori_loop(0, count, step, 0)
    lax.fori_loop(count + 1, BLOCKS, load_wait, 0)

    sums = acc[64:65, :]
    fine = (sums > 2.0 ** -80) & (sums < 2.0 ** 100)
    fine_all = jnp.min(jnp.where(fine, 1.0, 0.0)) > 0.5

    @pl.when((count > 0) & jnp.logical_not(fine_all))
    def _():
        m_buf[...] = jnp.full_like(m_buf, masked_score)
        acc[...] = jnp.zeros_like(acc)

        def masked(b, n, h):
            row = lax.broadcasted_iota(jnp.int32, (256, TILE), 0)
            key = b * ROWS + h * 128 + row + jnp.where(row >= 128, 128, 0)
            return jnp.where(key < live, scores(b, n, h), masked_score)

        def maxima(b, carry):
            for n, h in UNITS:
                cols = slice(n * TILE, (n + 1) * TILE)
                m_buf[0:1, cols] = jnp.maximum(
                    m_buf[0:1, cols], jnp.max(masked(b, n, h), axis=0, keepdims=True)
                )
            return carry

        def again(b, carry):
            values(b)
            for n, h in UNITS:
                s = masked(b, n, h) - m_buf[0:1, n * TILE:(n + 1) * TILE]
                gather(n, h, jnp.exp2(s).astype(jnp.bfloat16))
            return carry

        lax.fori_loop(0, count, maxima, 0)
        lax.fori_loop(0, count, again, 0)

    row = gain_ref[...]
    gain = jnp.broadcast_to(jnp.concatenate([row, row], axis=1), (128, 128)).T[0:HEAD]
    lam = lam_ref[0, 0:1, :]
    for t in range(NQ // 128):
        maps = []
        for m in range(2):
            cols = slice(m * NQ + t * 128, m * NQ + (t + 1) * 128)
            total = acc[64:65, cols]
            maps.append(acc[0:64, cols] / jnp.where(total > 0.0, total, 1.0))
        mixed = maps[0] - lam * maps[1]
        normed = mixed * lax.rsqrt(jnp.mean(mixed * mixed, axis=0, keepdims=True) + epsilon) * gain
        ok = (first + t * 128 + lax.broadcasted_iota(jnp.int32, (64, 128), 1)) < live
        o_ref[t // 4, (t % 4) * 64:(t % 4 + 1) * 64, :] = jnp.where(ok, normed, 0.0).astype(jnp.bfloat16)


def attend(length, kv, q, lam, gain):
    return pl.pallas_call(
        attend_kernel,
        out_shape=jax.ShapeDtypeStruct((2, 256, 128), jnp.bfloat16),
        in_specs=[SMEM_SPEC, HBM_SPEC] + [VMEM_SPEC] * 3,
        out_specs=VMEM_SPEC,
        scratch_shapes=[
            pltpu.VMEM((BLOCKS, 2, HALF, 128), jnp.bfloat16),
            pltpu.VMEM((2, 128, 2 * NQ), jnp.bfloat16),
            pltpu.VMEM((80, ROWS), jnp.bfloat16),
            pltpu.VMEM((80, 2 * NQ), jnp.float32),
            pltpu.VMEM((2, 256, TILE), jnp.float32),
            pltpu.VMEM((8, 2 * NQ), jnp.float32),
            pltpu.SemaphoreType.DMA((BLOCKS,)),
        ],
        compiler_params=pltpu.CompilerParams(vmem_limit_bytes=ATTEND_VMEM),
        name="attend",
    )(length, kv, q, lam, gain)


CHUNK = 1024
SHARE = ROWS // (2 * NX)


def merge_kernel(
    o_ref, win_ref, wo_ref, do_ref, out_ref,
    rows_t, diff_rows, lhs_w, lhs_d, total, give, take, mine, far_in, joined, fin,
    recv_o, send_o, local_sem, send_g, recv_g, send_f, recv_f, send_n, recv_n,
):
    z, y, x, c = place()
    sp = z * NY + y
    right = (sp, ((x + 1) % NX) * 2 + c)
    left = (sp, ((x + NX - 1) % NX) * 2 + c)
    sibling = (sp, x * 2 + 1 - c)
    partners = [(z * NY + 2 * c + i, x * 2 + y // 2) for i in range(2)]
    away = [(2 * c + i) != y for i in range(2)]
    greet((right, left, sibling) + tuple(partners), (None,) * 3 + tuple(away))
    pl.semaphore_wait(pltpu.get_barrier_semaphore(), 3 + sum(a.astype(jnp.int32) for a in away))

    def remote(src, dst, send_sem, recv_sem, device):
        return pltpu.make_async_remote_copy(
            src_ref=src, dst_ref=dst, send_sem=send_sem, recv_sem=recv_sem,
            device_id=device, device_id_type=MESH,
        )

    slot = y % 2
    back = [remote(o_ref.at[i], rows_t.at[slot], send_o.at[i], recv_o.at[slot], partners[i]) for i in range(2)]
    for i in range(2):
        pl.when(away[i])(lambda i=i: back[i].start())
        def stay(i=i):
            copy = pltpu.make_async_copy(o_ref.at[i], rows_t.at[slot], local_sem)
            copy.start()
            copy.wait()
        pl.when(jnp.logical_not(away[i]))(stay)

    def rows_of(side, r):
        core = c if side else 1 - c
        return pl.ds(pl.multiple_of(((x + r) % NX) * 2 * SHARE + core * SHARE, SHARE), SHARE)

    for side in range(2):
        for r in range(NX):
            lhs_w[side, r * SHARE:(r + 1) * SHARE] = win_ref[rows_of(side, r)]

    def banded(k, carry):
        cols = pl.ds(pl.multiple_of(k * 512, 512), 512)
        weight = wo_ref[:, cols]
        for side in range(2):
            total[side, :, cols] = jnp.dot(lhs_w[side], weight, preferred_element_type=jnp.float32)
        return carry

    lax.fori_loop(0, 8, banded, 0)
    for i in range(2):
        def wait(i=i):
            remote(o_ref.at[i], rows_t.at[i], send_o.at[i], recv_o.at[i], partners[i]).wait_recv()
        pl.when(away[i])(wait)
    for j in range(4):
        pair = jnp.concatenate(
            [rows_t[0, j * 64:(j + 1) * 64], rows_t[1, j * 64:(j + 1) * 64]], axis=0
        ).astype(jnp.float32)
        diff_rows[j * 128:(j + 1) * 128] = pair.T.astype(jnp.bfloat16)
    for side in range(2):
        for r in range(NX):
            lhs_d[side, r * SHARE:(r + 1) * SHARE] = diff_rows[rows_of(side, r)]

    started = []

    def go(copy):
        copy.start()
        started.append(copy)
        return copy

    order = (0, 2, 1, 3)

    def partial(side, k):
        cols = slice(k * CHUNK, (k + 1) * CHUNK)
        return total[side, :, cols] + jnp.dot(lhs_d[side], do_ref[:, cols], preferred_element_type=jnp.float32)

    for k in order:
        give[k] = partial(0, k).astype(jnp.bfloat16)
        go(remote(give.at[k], take.at[k], send_g.at[k], recv_g.at[k], sibling))
    for k in order:
        own = partial(1, k)
        remote(give.at[k], take.at[k], send_g.at[k], recv_g.at[k], sibling).wait_recv()
        both = (own + take[k].astype(jnp.float32)).astype(jnp.bfloat16)
        for r in range(NX):
            mine[r, k] = both[r * SHARE:(r + 1) * SHARE]
        go(remote(mine.at[2, k], far_in.at[k], send_f.at[k], recv_f.at[k], right if k < 2 else left))

    def near(src, k, way):
        return remote(src, fin.at[way, k], send_n.at[way, k], recv_n.at[way, k], left if way else right)

    for i in range(2):
        go(near(mine.at[1, 2 + i], 2 + i, 0))
        go(near(mine.at[3, i], i, 1))
    for k in order:
        way = 0 if k < 2 else 1
        remote(mine.at[2, k], far_in.at[k], send_f.at[k], recv_f.at[k], right).wait_recv()
        joined[k] = (
            mine[3 if way else 1, k].astype(jnp.float32) + far_in[k].astype(jnp.float32)
        ).astype(jnp.bfloat16)
        go(near(joined.at[k], k, way))
    for k in order:
        near(joined.at[k], k, 0).wait_recv()
        near(joined.at[k], k, 1).wait_recv()
        value = mine[0, k].astype(jnp.float32) + fin[0, k].astype(jnp.float32) + fin[1, k].astype(jnp.float32)
        out_ref[:, k * CHUNK:(k + 1) * CHUNK] = value.astype(jnp.bfloat16)
    for copy in started:
        copy.wait_send()
    for i in range(2):
        pl.when(away[i])(lambda i=i: back[i].wait_send())


def merge(o, win_rows, win_out, diff_out):
    bf = jnp.bfloat16
    width = win_out.shape[1]
    chunks = width // CHUNK
    half = ROWS // 2
    return pl.pallas_call(
        merge_kernel,
        out_shape=jax.ShapeDtypeStruct((SHARE, width), bf),
        in_specs=[VMEM_SPEC] * 4,
        out_specs=VMEM_SPEC,
        scratch_shapes=[
            pltpu.VMEM((2, 256, 128), bf),
            pltpu.VMEM((ROWS, 128), bf),
            pltpu.VMEM((2, half, GROUP * HEAD), bf),
            pltpu.VMEM((2, half, 128), bf),
            pltpu.VMEM((2, half, width), jnp.float32),
            pltpu.VMEM((chunks, half, CHUNK), bf),
            pltpu.VMEM((chunks, half, CHUNK), bf),
            pltpu.VMEM((NX, chunks, SHARE, CHUNK), bf),
            pltpu.VMEM((chunks, SHARE, CHUNK), bf),
            pltpu.VMEM((chunks, SHARE, CHUNK), bf),
            pltpu.VMEM((2, chunks, SHARE, CHUNK), bf),
            pltpu.SemaphoreType.DMA((2,)),
            pltpu.SemaphoreType.DMA((2,)),
            pltpu.SemaphoreType.DMA,
            pltpu.SemaphoreType.DMA((chunks,)),
            pltpu.SemaphoreType.DMA((chunks,)),
            pltpu.SemaphoreType.DMA((chunks,)),
            pltpu.SemaphoreType.DMA((chunks,)),
            pltpu.SemaphoreType.DMA((2, chunks)),
            pltpu.SemaphoreType.DMA((2, chunks)),
        ],
        compiler_params=pltpu.CompilerParams(
            collective_id=1, has_side_effects=True, vmem_limit_bytes=40 * 1024 * 1024
        ),
        name="merge",
    )(o, win_rows, win_out, diff_out)


def body(
    inputs, length, win_query, win_key, win_value, sink_logit,
    diff_query, diff_key, diff_value, mix_lambda, head_gain, win_out, diff_out,
):
    weights = (win_query.T, win_key.T, win_value.T, diff_query, diff_key, diff_value)
    kv, q, lam, win_rows = front(length, mix_lambda, sink_logit, inputs, weights)
    rows = attend(length, kv, q, lam, head_gain.reshape(1, HEAD))
    return merge(rows, win_rows, win_out, diff_out)


def solution(mesh):
    placed = (
        P("sp", "tp"), P(), P(None, "tp"), P(None, "tp"), P(None, "tp"), P("tp"), P(None, "tp"),
        P(None, "tp"), P(None, "tp"), P("tp"), P(), P("tp", None), P("tp", None),
    )
    return jax.shard_map(
        body, mesh=mesh, in_specs=placed, out_specs=P(("sp", "tp"), None), check_vma=False
    )
```

```python
import functools

import jax
import jax.numpy as jnp
from jax import lax
from jax.experimental import pallas as pl
from jax.experimental.pallas import tpu as pltpu
from jax.sharding import PartitionSpec as P

HEAD = 64
DQK = 32
GROUP = 3
WINDOW = 128
NX, NY, NZ = 4, 4, 8
ROWS = 512
QUARTER = ROWS // 4
HALF = ROWS // 2
BLOCKS = NY * NZ
FRONT_VMEM = 62 * 1024 * 1024
ATTEND_VMEM = 60 * 1024 * 1024
Q_SCALE = 1.4426950408889634 * DQK ** (-0.5)
MESH = pl.DeviceIdType.MESH

epsilon = 1e-06
masked_score = -1e30
VMEM_SPEC = pl.BlockSpec(memory_space=pltpu.VMEM)
SMEM_SPEC = pl.BlockSpec(memory_space=pltpu.SMEM)
HBM_SPEC = pl.BlockSpec(memory_space=pltpu.HBM)


def place():
    sp, tp = lax.axis_index("sp"), lax.axis_index("tp")
    return sp // NY, sp % NY, tp // 2, tp % 2


def greet(devices, conditions=None):
    barrier = pltpu.get_barrier_semaphore()
    for i, device in enumerate(devices):
        def signal(device=device):
            pl.semaphore_signal(barrier, inc=1, device_id=device, device_id_type=MESH)
        if conditions is None or conditions[i] is None:
            signal()
        else:
            pl.when(conditions[i])(signal)


NQ = 2 * ROWS
TILE = 1024
UNITS = [(n, h) for n in range(2 * NQ // TILE) for h in range(2)]


def set_queries(qz, q_ref):
    for t in range(NQ // 128):
        q = q_ref[t // 4, t % 4 // 2, (t % 2) * 64:(t % 2 + 1) * 64, :]
        for h in range(2):
            for m in range(2):
                qz[h, h * 64 + m * 32:h * 64 + (m + 1) * 32, m * NQ + t * 128:m * NQ + (t + 1) * 128] = (
                    q[m * 32:(m + 1) * 32]
                )


def set_values(va, kv_ref, b, live):
    lane = lax.broadcasted_iota(jnp.int32, (64, 128), 1)
    row = lax.broadcasted_iota(jnp.int32, (16, 128), 0)
    for h in range(2):
        for u in range(2):
            at = h * 256 + u * 128
            ok = (b * ROWS + u * HALF + h * 128 + lane) < live
            v = kv_ref[b, u, 128 + h * 64:128 + (h + 1) * 64, :].astype(jnp.float32)
            va[0:64, at:at + 128] = jnp.where(ok, v, 0.0).astype(jnp.bfloat16)
            va[64:80, at:at + 128] = jnp.where(ok[:16] & (row == 0), 1.0, 0.0).astype(jnp.bfloat16)


def scores(kv_ref, qz, b, n, h):
    k = jnp.concatenate([kv_ref[b, 0, 0:128, :], kv_ref[b, 1, 0:128, :]], axis=0)
    return jnp.dot(k, qz[h, :, n * TILE:(n + 1) * TILE], preferred_element_type=jnp.float32)


def gather(att, va, n, h, weight):
    att[:, n * TILE:(n + 1) * TILE] += jnp.dot(
        va[:, h * 256:(h + 1) * 256], weight, preferred_element_type=jnp.float32
    )


def finish(o_ref, att, lam_ref, gain_ref, first, live):
    row = gain_ref[...]
    gain = jnp.broadcast_to(jnp.concatenate([row, row], axis=1), (128, 128)).T[0:HEAD]
    lam = lam_ref[0, 0:1, :]
    for t in range(NQ // 128):
        maps = []
        for m in range(2):
            cols = slice(m * NQ + t * 128, m * NQ + (t + 1) * 128)
            total = att[64:65, cols]
            maps.append(att[0:64, cols] / jnp.where(total > 0.0, total, 1.0))
        mixed = maps[0] - lam * maps[1]
        normed = mixed * lax.rsqrt(jnp.mean(mixed * mixed, axis=0, keepdims=True) + epsilon) * gain
        ok = (first + t * 128 + lax.broadcasted_iota(jnp.int32, (64, 128), 1)) < live
        o_ref[t // 4, (t % 4) * 64:(t % 4 + 1) * 64, :] = jnp.where(ok, normed, 0.0).astype(jnp.bfloat16)


WQ, DQ, DK, DV, ACC_COLS = 0, 384, 512, 640, 768


def front_kernel(
    length_ref, lam_smem, sink_ref, x_ref, gain_ref, wq_hbm, wk_hbm, wv_hbm, dq_hbm, dk_hbm, dv_hbm,
    o_ref, flag_ref, kv_out, q_ref, lamo_ref, win_ref,
    kv_ref, qz, va, att, s_buf, kv_sem, xg, wt, dq, dk, dv, acc, msg, lam_ref, halo_ref, winq, keys, v_t,
    w_sem, recv_x, send_xr, send_xl, send_xs,
    recv_kv, recv_q, recv_lam, recv_halo, send_a, send_lam, send_ring, send_sib, send_halo, local_sem,
):
    z, y, x, c = place()
    sp = z * NY + y
    tp = x * 2 + c
    right = (sp, ((x + 1) % NX) * 2 + c)
    left = (sp, ((x + NX - 1) % NX) * 2 + c)
    sibling = (sp, x * 2 + 1 - c)
    up = (((z + 1) % NZ) * NY + y, tp)
    down = (((z + NZ - 1) % NZ) * NY + y, tp)
    after = ((sp + 1) % BLOCKS, tp)
    before = ((sp + BLOCKS - 1) % BLOCKS, tp)
    partners = [(z * NY + 2 * c + i, x * 2 + y // 2) for i in range(2)]
    away = [(2 * c + i) != y for i in range(2)]

    loads = [
        pltpu.make_async_copy(src, dst, w_sem.at[i])
        for i, (src, dst) in enumerate(
            (
                (wq_hbm, wt.at[pl.ds(0, 192)]),
                (wk_hbm, wt.at[pl.ds(192, 64)]),
                (wv_hbm, wt.at[pl.ds(256, 64)]),
                (dq_hbm, dq),
                (dk_hbm, dk),
                (dv_hbm, dv),
            )
        )
    ]
    for load in loads:
        load.start()
    for i in range(2):
        lam_ref[i] = jnp.full((8, 128), lam_smem[i], jnp.float32)
    greet(
        (right, left, sibling, up, down, after, before) + tuple(partners), (None,) * 7 + tuple(away)
    )
    pl.semaphore_wait(pltpu.get_barrier_semaphore(), 7 + sum(a.astype(jnp.int32) for a in away))

    started = []

    def remote(src, dst, send_sem, recv_sem, device):
        return pltpu.make_async_remote_copy(
            src_ref=src, dst_ref=dst, send_sem=send_sem, recv_sem=recv_sem,
            device_id=device, device_id_type=MESH,
        )

    def go(copy):
        copy.start()
        started.append(copy)

    def send_x(own, t, q, device, sem):
        rows = pl.ds(q * QUARTER, QUARTER)
        go(remote(x_ref.at[rows] if own else xg.at[t, rows], xg.at[t, rows], sem, recv_x.at[t, q], device))

    def arrive_x(t, q):
        rows = pl.ds(q * QUARTER, QUARTER)
        remote(xg.at[t, rows], xg.at[t, rows], send_xr.at[0], recv_x.at[t, q], sibling).wait_recv()

    t_left = ((x + NX - 1) % NX) * 2 + c
    t_right = ((x + 1) % NX) * 2 + c
    t_far = ((x + 2) % NX) * 2 + c

    def other(t):
        return t + 1 - 2 * c

    def multiply(own, t, h):
        rows = pl.ds(h * HALF, HALF)
        block = x_ref[rows] if own else xg[t, rows]
        ks = pl.ds(pl.multiple_of(t * ROWS, ROWS), ROWS)
        acc[rows, WQ:WQ + 320] += lax.dot_general(
            block, wt[:, ks], (((1,), (1,)), ((), ())), preferred_element_type=jnp.float32
        )
        both = jnp.concatenate([dq[ks, :], dk[ks, :]], axis=1)
        acc[rows, DQ:DQ + 256] += jnp.dot(block, both, preferred_element_type=jnp.float32)
        acc[rows, DV:DV + 128] += jnp.dot(block, dv[ks, :], preferred_element_type=jnp.float32)

    def multiply_other(t, h):
        for q in (2 * h, 2 * h + 1):
            arrive_x(other(t), q)
        multiply(False, other(t), h)

    def receive_x(t, q, sem):
        arrive_x(t, q)
        send_x(False, t, q, sibling, sem)

    lane = lax.broadcasted_iota(jnp.int32, (QUARTER, 128), 1)
    low = lane < 64
    mine = sp
    slot = y % 2

    def head_copies(i, u):
        return [
            remote(msg.at[i, u, pl.ds(0, 256)], kv_ref.at[mine, u], send_a.at[i, u, 0], recv_kv.at[mine, u], partners[i]),
            remote(msg.at[i, u, pl.ds(256, 128)], q_ref.at[slot, u], send_a.at[i, u, 1], recv_q.at[slot, u], partners[i]),
        ]

    def lam_copy(i):
        return remote(lam_ref.at[i], lamo_ref.at[slot], send_lam.at[i], recv_lam.at[slot], partners[i])

    edges = [
        remote(keys.at[pl.ds(WINDOW, WINDOW)], halo_ref.at[1], send_halo.at[1], recv_halo.at[1], before),
        remote(keys.at[pl.ds(ROWS, WINDOW)], halo_ref.at[0], send_halo.at[0], recv_halo.at[0], after),
    ]

    def pack(u):
        rows = pl.ds(u * HALF, HALF)
        first, second = pl.ds(u * HALF, QUARTER), pl.ds(u * HALF + QUARTER, QUARTER)
        k0, k1 = acc[first, DK:DK + 128], acc[second, DK:DK + 128]
        msg[0, u, 0:128] = jnp.where(low, k0, pltpu.roll(k1, 64, 1)).astype(jnp.bfloat16)
        msg[1, u, 0:128] = jnp.where(low, pltpu.roll(k0, 64, 1), k1).astype(jnp.bfloat16)
        for j, part in enumerate((first, second)):
            turned = acc[part, DV:DV + 128].T.astype(jnp.bfloat16)
            asked = (acc[part, DQ:DQ + 128].T * Q_SCALE).astype(jnp.bfloat16)
            for head in range(2):
                msg[head, u, 128 + j * 64:128 + (j + 1) * 64] = turned[head * 64:(head + 1) * 64]
                msg[head, u, 256 + j * 64:256 + (j + 1) * 64] = asked[head * 64:(head + 1) * 64]
            keys[pl.ds(WINDOW + u * HALF + j * QUARTER, QUARTER)] = jnp.where(
                low, acc[part, 256:384], acc[part, 128:256]
            ).astype(jnp.bfloat16)
        for i in range(2):
            def leave(i=i):
                for copy in head_copies(i, u):
                    copy.start()
            pl.when(away[i])(leave)
            def stay(i=i):
                copies = [
                    pltpu.make_async_copy(msg.at[i, u, pl.ds(0, 256)], kv_ref.at[mine, u], local_sem.at[0]),
                    pltpu.make_async_copy(msg.at[i, u, pl.ds(256, 128)], q_ref.at[slot, u], local_sem.at[1]),
                ]
                for copy in copies:
                    copy.start()
                for copy in copies:
                    copy.wait()
            pl.when(jnp.logical_not(away[i]))(stay)
        edges[u].start()
        winq[rows] = acc[rows, 0:256].astype(jnp.bfloat16)

    def block(zz, s, core):
        return ((zz + NZ) % NZ) * NY + 2 * core + s

    def forward(b, u, device, sem):
        go(remote(kv_ref.at[b, u], kv_ref.at[b, u], sem, recv_kv.at[b, u], device))

    def arrive(b, u):
        remote(kv_ref.at[b, u], kv_ref.at[b, u], send_sib.at[0, 0], recv_kv.at[b, u], sibling).wait_recv()

    def open_ring(u):
        for s in range(2):
            b = block(z, s, c)
            pl.when(away[s])(lambda: arrive(b, u))
            forward(b, u, up, send_ring.at[0, s, u, 0])
            forward(b, u, down, send_ring.at[1, s, u, 0])
            forward(b, u, sibling, send_sib.at[s, u])

    shared = [2, 2]

    def ring(u, d):
        for s in range(2):
            for way, (reach, device, sign) in enumerate(((4 - s, up, -1), (3 + s, down, 1))):
                if d > reach:
                    continue
                b = block(z + sign * d, s, c)
                arrive(b, u)
                if d < reach:
                    forward(b, u, device, send_ring.at[way, s, u, d])
                forward(b, u, sibling, send_sib.at[shared[u], u])
                shared[u] += 1

    def turn(i):
        pair = keys[i * 128:(i + 1) * 128].astype(jnp.float32)
        v_t[:, i * 128:(i + 1) * 128] = pair.T[0:HEAD].astype(jnp.bfloat16)

    def band_edges():
        for copy in edges:
            copy.wait_recv()
        keys[0:WINDOW] = halo_ref[0]
        keys[WINDOW + ROWS:] = halo_ref[1]
        turn(0)
        turn(5)

    def band(i):
        live = length_ref[0]
        q_t = winq[i * 128:(i + 1) * 128].astype(jnp.float32).T * HEAD ** (-0.5)
        zero = jnp.zeros((HEAD, 128), jnp.float32)
        query = jnp.concatenate(
            [jnp.concatenate([zero, q_t[g * HEAD:(g + 1) * HEAD]], axis=0) for g in range(GROUP)], axis=1
        ).astype(jnp.bfloat16)
        s = jnp.dot(keys[i * 128:i * 128 + 384], query, preferred_element_type=jnp.float32)
        key = lax.broadcasted_iota(jnp.int32, (384, 128), 0)
        ask = lax.broadcasted_iota(jnp.int32, (384, 128), 1)
        start = sp * ROWS + (i - 1) * 128
        allowed = (
            (key - ask >= 0) & (key - ask <= 2 * WINDOW) & (start + key >= 0) & (start + key < live)
        )
        for g in range(GROUP):
            own = jnp.where(allowed, s[:, g * 128:(g + 1) * 128], masked_score)
            top = jnp.maximum(jnp.max(own, axis=0, keepdims=True), sink_ref[g])
            e = jnp.where(allowed, jnp.exp(own - top), 0.0)
            total = jnp.sum(e, axis=0, keepdims=True) + jnp.exp(sink_ref[g] - top)
            o = jnp.dot(v_t[:, i * 128:i * 128 + 384], e.astype(jnp.bfloat16), preferred_element_type=jnp.float32)
            ok = (start + 128 + lax.broadcasted_iota(jnp.int32, (HEAD, 128), 1)) < live
            o = jnp.where(ok, o / total, 0.0)
            both = jnp.concatenate([o, jnp.zeros_like(o)], axis=0).T
            win_ref[i * 128:(i + 1) * 128, g * HEAD:(g + 1) * HEAD] = both[:, 0:HEAD].astype(jnp.bfloat16)

    live = length_ref[0]

    def nth(i):
        at = i + 4
        d, r = at // 8, at % 8
        sign, core = 2 * (r // 4) - 1, r % 4 // 2
        zz = (z + sign * d + NZ) % NZ
        return zz * NY + 2 * (c + core - 2 * c * core) + r % 2, core == 1

    def step(i, carry):
        b, _ = nth(i)
        following, foreign = nth(jnp.minimum(i + 1, BLOCKS - 1))

        @pl.when(jnp.logical_and(foreign, i + 1 < BLOCKS))
        def _():
            arrive(following, 0)
            arrive(following, 1)

        pltpu.make_async_copy(kv_ref.at[b], kv_out.at[b], kv_sem.at[b]).start()
        set_values(va, kv_ref, b, live)
        for j, (n, h) in enumerate(UNITS):
            s = s_buf[j % 2]
            if j + 1 < len(UNITS):
                s_buf[1 - j % 2] = scores(kv_ref, qz, b, *UNITS[j + 1])
            else:
                s_buf[1 - j % 2] = scores(kv_ref, qz, following, *UNITS[0])
            gather(att, va, n, h, jnp.exp2(s).astype(jnp.bfloat16))
        return carry

    for q in range(2):
        send_x(True, tp, q, right, send_xr.at[q])
        send_x(True, tp, q, left, send_xl.at[q])
    for q in range(4):
        send_x(True, tp, q, sibling, send_xs.at[q])
    acc[...] = jnp.zeros_like(acc)
    for i in range(2):
        pl.when(away[i])(lambda i=i: lam_copy(i).start())
        def keep(i=i):
            copy = pltpu.make_async_copy(lam_ref.at[i], lamo_ref.at[slot], local_sem.at[2])
            copy.start()
            copy.wait()
        pl.when(jnp.logical_not(away[i]))(keep)
    for load in loads:
        load.wait()
    multiply(True, tp, 0)
    receive_x(t_left, 0, send_xs.at[4])
    send_x(False, t_left, 0, right, send_xr.at[2])
    for q in (2, 3):
        send_x(True, tp, q, right, send_xr.at[q + 1])
    receive_x(t_right, 0, send_xs.at[5])
    multiply(True, tp, 1)
    receive_x(t_right, 1, send_xs.at[6])
    send_x(False, t_right, 1, left, send_xl.at[2])
    for q in (2, 3):
        send_x(True, tp, q, left, send_xl.at[q + 1])
    receive_x(t_left, 1, send_xs.at[7])
    multiply_other(tp, 0)
    multiply_other(tp, 1)
    multiply(False, t_left, 0)
    multiply(False, t_right, 0)
    multiply_other(t_left, 0)
    multiply_other(t_right, 0)
    receive_x(t_far, 0, send_xs.at[8])
    receive_x(t_far, 1, send_xs.at[9])
    multiply(False, t_far, 0)
    multiply_other(t_far, 0)
    pack(0)
    receive_x(t_left, 2, send_xs.at[10])
    send_x(False, t_left, 2, right, send_xr.at[5])
    receive_x(t_right, 2, send_xs.at[11])
    receive_x(t_right, 3, send_xs.at[12])
    send_x(False, t_right, 3, left, send_xl.at[5])
    receive_x(t_left, 3, send_xs.at[13])
    open_ring(0)
    multiply(False, t_left, 1)
    multiply(False, t_right, 1)
    multiply_other(t_left, 1)
    multiply_other(t_right, 1)
    receive_x(t_far, 2, send_xs.at[14])
    receive_x(t_far, 3, send_xs.at[15])
    multiply(False, t_far, 1)
    ring(0, 1)
    multiply_other(t_far, 1)
    pack(1)
    att[...] = jnp.zeros_like(att)
    va[...] = jnp.zeros_like(va)
    qz[...] = jnp.zeros_like(qz)
    for i in range(1, 5):
        turn(i)
    band(1)
    band(2)
    open_ring(1)
    for i in range(2):
        def rest(i=i):
            for u in range(2):
                remote(
                    msg.at[0, u, pl.ds(256, 128)], q_ref.at[i, u], send_a.at[0, u, 1], recv_q.at[i, u], sibling
                ).wait_recv()
            remote(lam_ref.at[0], lamo_ref.at[i], send_lam.at[0], recv_lam.at[i], sibling).wait_recv()
        pl.when(away[i])(rest)
    set_queries(qz, q_ref)
    ring(0, 2)
    s_buf[0] = scores(kv_ref, qz, nth(0)[0], *UNITS[0])
    lax.fori_loop(0, 3, step, 0)
    ring(0, 3)
    ring(1, 1)
    lax.fori_loop(3, 7, step, 0)
    ring(0, 4)
    ring(1, 2)
    lax.fori_loop(7, 12, step, 0)
    ring(1, 3)
    lax.fori_loop(12, 20, step, 0)
    ring(1, 4)
    band_edges()
    band(0)
    band(3)
    lax.fori_loop(20, BLOCKS, step, 0)
    sums = att[64:65, :]
    flag_ref[0] = jnp.min(jnp.where((sums > 2.0 ** -80) & (sums < 2.0 ** 100), 1.0, 0.0))
    finish(o_ref, att, lamo_ref, gain_ref, (z * NY + 2 * c) * ROWS, live)
    for b in range(BLOCKS):
        pltpu.make_async_copy(kv_ref.at[b], kv_out.at[b], kv_sem.at[b]).wait()
    for copy in started + edges:
        copy.wait_send()
    for i in range(2):
        def sent(i=i):
            for u in range(2):
                for copy in head_copies(i, u):
                    copy.wait_send()
            lam_copy(i).wait_send()
        pl.when(away[i])(sent)


def front(length, mix_lambda, sink_logit, inputs, gain, weights):
    bf = jnp.bfloat16
    depth = weights[3].shape[0]
    dma = pltpu.SemaphoreType.DMA
    return pl.pallas_call(
        front_kernel,
        out_shape=(
            jax.ShapeDtypeStruct((2, 256, 128), bf),
            jax.ShapeDtypeStruct((1,), jnp.float32),
            jax.ShapeDtypeStruct((BLOCKS, 2, HALF, 128), bf),
            jax.ShapeDtypeStruct((2, 2, 128, 128), bf),
            jax.ShapeDtypeStruct((2, 8, 128), jnp.float32),
            jax.ShapeDtypeStruct((ROWS, GROUP * HEAD), bf),
        ),
        in_specs=[SMEM_SPEC] * 3 + [VMEM_SPEC] * 2 + [HBM_SPEC] * 6,
        out_specs=(VMEM_SPEC, SMEM_SPEC, HBM_SPEC, VMEM_SPEC, VMEM_SPEC, VMEM_SPEC),
        scratch_shapes=[
            pltpu.VMEM((BLOCKS, 2, HALF, 128), bf),
            pltpu.VMEM((2, 128, 2 * NQ), bf),
            pltpu.VMEM((80, ROWS), bf),
            pltpu.VMEM((80, 2 * NQ), jnp.float32),
            pltpu.VMEM((2, 256, TILE), jnp.float32),
            dma((BLOCKS,)),
            pltpu.VMEM((2 * NX, ROWS, ROWS), bf),
            pltpu.VMEM((320, depth), bf),
            pltpu.VMEM((depth, 128), bf),
            pltpu.VMEM((depth, 128), bf),
            pltpu.VMEM((depth, 128), bf),
            pltpu.VMEM((ROWS, ACC_COLS), jnp.float32),
            pltpu.VMEM((2, 2, 384, 128), bf),
            pltpu.VMEM((2, 8, 128), jnp.float32),
            pltpu.VMEM((2, WINDOW, 128), bf),
            pltpu.VMEM((ROWS, 256), bf),
            pltpu.VMEM((ROWS + 2 * WINDOW, 128), bf),
            pltpu.VMEM((HEAD, ROWS + 2 * WINDOW), bf),
            dma((6,)), dma((2 * NX, 4)), dma((6,)), dma((6,)), dma((16,)),
            dma((BLOCKS, 2)), dma((2, 2)), dma((2,)), dma((2,)),
            dma((2, 2, 2)), dma((2,)), dma((2, 2, 2, 4)), dma((16, 2)), dma((2,)), dma((3,)),
        ],
        compiler_params=pltpu.CompilerParams(
            collective_id=0, has_side_effects=True, vmem_limit_bytes=FRONT_VMEM
        ),
        name="front",
    )(length, mix_lambda, sink_logit, inputs, gain, *weights)


def fix_kernel(length_ref, flag_ref, o_in, kv_hbm, q_hbm, lam_hbm, gain_hbm, o_ref, kv_ref, q_ref, lam_ref, gain_ref, rows, qz, va, att, m_buf, sem):
    live = length_ref[0]
    z, y, x, c = place()
    first = (z * NY + 2 * c) * ROWS

    @pl.when((first < live) & jnp.logical_not(flag_ref[0] > 0.5))
    def _():
        count = (live + ROWS - 1) // ROWS
        for src, dst in ((kv_hbm, kv_ref), (q_hbm, q_ref), (lam_hbm, lam_ref), (gain_hbm, gain_ref)):
            copy = pltpu.make_async_copy(src, dst, sem)
            copy.start()
            copy.wait()
        qz[...] = jnp.zeros_like(qz)
        va[...] = jnp.zeros_like(va)
        att[...] = jnp.zeros_like(att)
        m_buf[...] = jnp.full_like(m_buf, masked_score)
        set_queries(qz, q_ref)

        def masked(b, n, h):
            row = lax.broadcasted_iota(jnp.int32, (256, TILE), 0)
            key = b * ROWS + h * 128 + row + jnp.where(row >= 128, 128, 0)
            return jnp.where(key < live, scores(kv_ref, qz, b, n, h), masked_score)

        def maxima(b, carry):
            for n, h in UNITS:
                cols = slice(n * TILE, (n + 1) * TILE)
                m_buf[0:1, cols] = jnp.maximum(
                    m_buf[0:1, cols], jnp.max(masked(b, n, h), axis=0, keepdims=True)
                )
            return carry

        def again(b, carry):
            set_values(va, kv_ref, b, live)
            for n, h in UNITS:
                s = masked(b, n, h) - m_buf[0:1, n * TILE:(n + 1) * TILE]
                gather(att, va, n, h, jnp.exp2(s).astype(jnp.bfloat16))
            return carry

        lax.fori_loop(0, count, maxima, 0)
        lax.fori_loop(0, count, again, 0)
        finish(rows, att, lam_ref, gain_ref, first, live)
        copy = pltpu.make_async_copy(rows, o_ref, sem)
        copy.start()
        copy.wait()


def fix(length, flag, o, kv, q, lam, gain):
    bf = jnp.bfloat16
    return pl.pallas_call(
        fix_kernel,
        out_shape=jax.ShapeDtypeStruct((2, 256, 128), bf),
        in_specs=[SMEM_SPEC] * 2 + [HBM_SPEC] * 5,
        out_specs=HBM_SPEC,
        input_output_aliases={2: 0},
        scratch_shapes=[
            pltpu.VMEM((BLOCKS, 2, HALF, 128), bf),
            pltpu.VMEM((2, 2, 128, 128), bf),
            pltpu.VMEM((2, 8, 128), jnp.float32),
            pltpu.VMEM((1, HEAD), jnp.float32),
            pltpu.VMEM((2, 256, 128), bf),
            pltpu.VMEM((2, 128, 2 * NQ), bf),
            pltpu.VMEM((80, ROWS), bf),
            pltpu.VMEM((80, 2 * NQ), jnp.float32),
            pltpu.VMEM((8, 2 * NQ), jnp.float32),
            pltpu.SemaphoreType.DMA,
        ],
        compiler_params=pltpu.CompilerParams(vmem_limit_bytes=ATTEND_VMEM),
        name="fix",
    )(length, flag, o, kv, q, lam, gain)


CHUNK = 1024
SHARE = ROWS // (2 * NX)


def merge_kernel(
    o_ref, win_ref, wo_ref, do_ref, out_ref,
    rows_t, diff_rows, lhs_w, lhs_d, total, give, take, mine, far_in, joined, fin,
    recv_o, send_o, local_sem, send_g, recv_g, send_f, recv_f, send_n, recv_n,
):
    z, y, x, c = place()
    sp = z * NY + y
    right = (sp, ((x + 1) % NX) * 2 + c)
    left = (sp, ((x + NX - 1) % NX) * 2 + c)
    sibling = (sp, x * 2 + 1 - c)
    partners = [(z * NY + 2 * c + i, x * 2 + y // 2) for i in range(2)]
    away = [(2 * c + i) != y for i in range(2)]
    greet((right, left, sibling) + tuple(partners), (None,) * 3 + tuple(away))
    pl.semaphore_wait(pltpu.get_barrier_semaphore(), 3 + sum(a.astype(jnp.int32) for a in away))

    def remote(src, dst, send_sem, recv_sem, device):
        return pltpu.make_async_remote_copy(
            src_ref=src, dst_ref=dst, send_sem=send_sem, recv_sem=recv_sem,
            device_id=device, device_id_type=MESH,
        )

    slot = y % 2
    back = [remote(o_ref.at[i], rows_t.at[slot], send_o.at[i], recv_o.at[slot], partners[i]) for i in range(2)]
    for i in range(2):
        pl.when(away[i])(lambda i=i: back[i].start())
        def stay(i=i):
            copy = pltpu.make_async_copy(o_ref.at[i], rows_t.at[slot], local_sem)
            copy.start()
            copy.wait()
        pl.when(jnp.logical_not(away[i]))(stay)

    def rows_of(side, r):
        core = c if side else 1 - c
        return pl.ds(pl.multiple_of(((x + r) % NX) * 2 * SHARE + core * SHARE, SHARE), SHARE)

    for side in range(2):
        for r in range(NX):
            lhs_w[side, r * SHARE:(r + 1) * SHARE] = win_ref[rows_of(side, r)]

    def banded(k, carry):
        cols = pl.ds(pl.multiple_of(k * 512, 512), 512)
        weight = wo_ref[:, cols]
        for side in range(2):
            total[side, :, cols] = jnp.dot(lhs_w[side], weight, preferred_element_type=jnp.float32)
        return carry

    lax.fori_loop(0, 8, banded, 0)
    for i in range(2):
        def wait(i=i):
            remote(o_ref.at[i], rows_t.at[i], send_o.at[i], recv_o.at[i], partners[i]).wait_recv()
        pl.when(away[i])(wait)
    for j in range(4):
        pair = jnp.concatenate(
            [rows_t[0, j * 64:(j + 1) * 64], rows_t[1, j * 64:(j + 1) * 64]], axis=0
        ).astype(jnp.float32)
        diff_rows[j * 128:(j + 1) * 128] = pair.T.astype(jnp.bfloat16)
    for side in range(2):
        for r in range(NX):
            lhs_d[side, r * SHARE:(r + 1) * SHARE] = diff_rows[rows_of(side, r)]

    started = []

    def go(copy):
        copy.start()
        started.append(copy)
        return copy

    order = (0, 2, 1, 3)

    def partial(side, k):
        cols = slice(k * CHUNK, (k + 1) * CHUNK)
        return total[side, :, cols] + jnp.dot(lhs_d[side], do_ref[:, cols], preferred_element_type=jnp.float32)

    for k in order:
        give[k] = partial(0, k).astype(jnp.bfloat16)
        go(remote(give.at[k], take.at[k], send_g.at[k], recv_g.at[k], sibling))
    for k in order:
        own = partial(1, k)
        remote(give.at[k], take.at[k], send_g.at[k], recv_g.at[k], sibling).wait_recv()
        both = (own + take[k].astype(jnp.float32)).astype(jnp.bfloat16)
        for r in range(NX):
            mine[r, k] = both[r * SHARE:(r + 1) * SHARE]
        go(remote(mine.at[2, k], far_in.at[k], send_f.at[k], recv_f.at[k], right if k < 2 else left))

    def near(src, k, way):
        return remote(src, fin.at[way, k], send_n.at[way, k], recv_n.at[way, k], left if way else right)

    for i in range(2):
        go(near(mine.at[1, 2 + i], 2 + i, 0))
        go(near(mine.at[3, i], i, 1))
    for k in order:
        way = 0 if k < 2 else 1
        remote(mine.at[2, k], far_in.at[k], send_f.at[k], recv_f.at[k], right).wait_recv()
        joined[k] = (
            mine[3 if way else 1, k].astype(jnp.float32) + far_in[k].astype(jnp.float32)
        ).astype(jnp.bfloat16)
        go(near(joined.at[k], k, way))
    for k in order:
        near(joined.at[k], k, 0).wait_recv()
        near(joined.at[k], k, 1).wait_recv()
        value = mine[0, k].astype(jnp.float32) + fin[0, k].astype(jnp.float32) + fin[1, k].astype(jnp.float32)
        out_ref[:, k * CHUNK:(k + 1) * CHUNK] = value.astype(jnp.bfloat16)
    for copy in started:
        copy.wait_send()
    for i in range(2):
        pl.when(away[i])(lambda i=i: back[i].wait_send())


def merge(o, win_rows, win_out, diff_out):
    bf = jnp.bfloat16
    width = win_out.shape[1]
    chunks = width // CHUNK
    half = ROWS // 2
    return pl.pallas_call(
        merge_kernel,
        out_shape=jax.ShapeDtypeStruct((SHARE, width), bf),
        in_specs=[VMEM_SPEC] * 4,
        out_specs=VMEM_SPEC,
        scratch_shapes=[
            pltpu.VMEM((2, 256, 128), bf),
            pltpu.VMEM((ROWS, 128), bf),
            pltpu.VMEM((2, half, GROUP * HEAD), bf),
            pltpu.VMEM((2, half, 128), bf),
            pltpu.VMEM((2, half, width), jnp.float32),
            pltpu.VMEM((chunks, half, CHUNK), bf),
            pltpu.VMEM((chunks, half, CHUNK), bf),
            pltpu.VMEM((NX, chunks, SHARE, CHUNK), bf),
            pltpu.VMEM((chunks, SHARE, CHUNK), bf),
            pltpu.VMEM((chunks, SHARE, CHUNK), bf),
            pltpu.VMEM((2, chunks, SHARE, CHUNK), bf),
            pltpu.SemaphoreType.DMA((2,)),
            pltpu.SemaphoreType.DMA((2,)),
            pltpu.SemaphoreType.DMA,
            pltpu.SemaphoreType.DMA((chunks,)),
            pltpu.SemaphoreType.DMA((chunks,)),
            pltpu.SemaphoreType.DMA((chunks,)),
            pltpu.SemaphoreType.DMA((chunks,)),
            pltpu.SemaphoreType.DMA((2, chunks)),
            pltpu.SemaphoreType.DMA((2, chunks)),
        ],
        compiler_params=pltpu.CompilerParams(
            collective_id=1, has_side_effects=True, vmem_limit_bytes=40 * 1024 * 1024
        ),
        name="merge",
    )(o, win_rows, win_out, diff_out)


def body(
    inputs, length, win_query, win_key, win_value, sink_logit,
    diff_query, diff_key, diff_value, mix_lambda, head_gain, win_out, diff_out,
):
    weights = (win_query.T, win_key.T, win_value.T, diff_query, diff_key, diff_value)
    gain = head_gain.reshape(1, HEAD)
    rows, flag, kv, q, lam, win_rows = front(length, mix_lambda, sink_logit, inputs, gain, weights)
    rows = fix(length, flag, rows, kv, q, lam, gain)
    return merge(rows, win_rows, win_out, diff_out)


def solution(mesh):
    placed = (
        P("sp", "tp"), P(), P(None, "tp"), P(None, "tp"), P(None, "tp"), P("tp"), P(None, "tp"),
        P(None, "tp"), P(None, "tp"), P("tp"), P(), P("tp", None), P("tp", None),
    )
    return jax.shard_map(
        body, mesh=mesh, in_specs=placed, out_specs=P(("sp", "tp"), None), check_vma=False
    )
```

```python
import functools

import jax
import jax.numpy as jnp
from jax import lax
from jax.experimental import pallas as pl
from jax.experimental.pallas import tpu as pltpu
from jax.sharding import PartitionSpec as P

HEAD = 64
DQK = 32
GROUP = 3
WINDOW = 128
NX, NY, NZ = 4, 4, 8
ROWS = 512
QUARTER = ROWS // 4
HALF = ROWS // 2
BLOCKS = NY * NZ
Q_SCALE = 1.4426950408889634 * DQK ** (-0.5)
MESH = pl.DeviceIdType.MESH

epsilon = 1e-06
masked_score = -1e30
VMEM_SPEC = pl.BlockSpec(memory_space=pltpu.VMEM)
SMEM_SPEC = pl.BlockSpec(memory_space=pltpu.SMEM)
HBM_SPEC = pl.BlockSpec(memory_space=pltpu.HBM)


def place():
    sp, tp = lax.axis_index("sp"), lax.axis_index("tp")
    return sp // NY, sp % NY, tp // 2, tp % 2


def greet(devices, conditions=None):
    barrier = pltpu.get_barrier_semaphore()
    for i, device in enumerate(devices):
        def signal(device=device):
            pl.semaphore_signal(barrier, inc=1, device_id=device, device_id_type=MESH)
        if conditions is None or conditions[i] is None:
            signal()
        else:
            pl.when(conditions[i])(signal)


WQ, DQ, DK, DV, ACC_COLS = 0, 384, 512, 640, 768
TILE = 2 * ROWS
CHUNK = 1024
CHUNKS = 4
SHARE = 32
GROUPS = 2 * NX


def natural(r, u):
    return (r // SHARE) * 2 * SHARE + u * SHARE + r % SHARE


def layer_kernel(
    length_ref, lam_smem, sink_ref, x_ref, gain_ref, wq_hbm, wk_hbm, wv_hbm, dq_hbm, dk_hbm, dv_hbm, wo_hbm, do_hbm,
    out_ref,
    xg, wt, dq, dk, dv, wo, do, acc, msg, lam_ref, lamo_ref, halo_ref, winq, keys, v_t, win_ref,
    kv_ref, q_ref, qz, va, att, s_buf, t_buf, m_buf, bias,
    o_buf, rows_t, diff_rows, lhs_w, lhs_d, give, take, mine, far_in, joined, fin,
    w_sem, recv_x, send_xr, send_xl, send_xs,
    recv_kv, recv_q, recv_lam, recv_halo, send_a, send_lam, send_ring, send_sib, send_halo, local_sem,
    recv_o, send_o, send_g, recv_g, send_f, recv_f, send_n, recv_n,
):
    z, y, x, c = place()
    sp = z * NY + y
    tp = x * 2 + c
    live = length_ref[0]
    right = (sp, ((x + 1) % NX) * 2 + c)
    left = (sp, ((x + NX - 1) % NX) * 2 + c)
    sibling = (sp, x * 2 + 1 - c)
    up = (((z + 1) % NZ) * NY + y, tp)
    down = (((z + NZ - 1) % NZ) * NY + y, tp)
    after = ((sp + 1) % BLOCKS, tp)
    before = ((sp + BLOCKS - 1) % BLOCKS, tp)
    partners = [(z * NY + 2 * c + i, x * 2 + y // 2) for i in range(2)]
    away = [(2 * c + i) != y for i in range(2)]

    loads = [
        pltpu.make_async_copy(src, dst, w_sem.at[i])
        for i, (src, dst) in enumerate(
            (
                (wq_hbm, wt.at[pl.ds(0, 192)]),
                (wk_hbm, wt.at[pl.ds(192, 64)]),
                (wv_hbm, wt.at[pl.ds(256, 64)]),
                (dq_hbm, dq),
                (dk_hbm, dk),
                (dv_hbm, dv),
                (wo_hbm, wo),
                (do_hbm, do),
            )
        )
    ]
    for load in loads:
        load.start()
    for i in range(2):
        lam_ref[i] = jnp.full((8, 128), lam_smem[i], jnp.float32)
    greet(
        (right, left, sibling, up, down, after, before) + tuple(partners), (None,) * 7 + tuple(away)
    )
    pl.semaphore_wait(pltpu.get_barrier_semaphore(), 7 + sum(a.astype(jnp.int32) for a in away))

    started = []

    def remote(src, dst, send_sem, recv_sem, device):
        return pltpu.make_async_remote_copy(
            src_ref=src, dst_ref=dst, send_sem=send_sem, recv_sem=recv_sem,
            device_id=device, device_id_type=MESH,
        )

    def go(copy):
        copy.start()
        started.append(copy)

    def send_x(own, t, q, device, sem):
        part = pl.ds(q % 2 * 4, 4)
        src = x_ref.at[part, q // 2] if own else xg.at[t, q // 2, part]
        go(remote(src, xg.at[t, q // 2, part], sem, recv_x.at[t, q], device))

    def arrive_x(t, q):
        part = xg.at[t, q // 2, pl.ds(q % 2 * 4, 4)]
        remote(part, part, send_xr.at[0], recv_x.at[t, q], sibling).wait_recv()

    t_left = ((x + NX - 1) % NX) * 2 + c
    t_right = ((x + 1) % NX) * 2 + c
    t_far = ((x + 2) % NX) * 2 + c

    def other(t):
        return t + 1 - 2 * c

    def multiply(own, t, h):
        rows = pl.ds(h * HALF, HALF)
        block = (x_ref[:, h] if own else xg[t, h]).reshape(HALF, ROWS)
        ks = pl.ds(pl.multiple_of(t * ROWS, ROWS), ROWS)
        acc[rows, WQ:WQ + 320] += lax.dot_general(
            block, wt[:, ks], (((1,), (1,)), ((), ())), preferred_element_type=jnp.float32
        )
        both = jnp.concatenate([dq[ks, :], dk[ks, :]], axis=1)
        acc[rows, DQ:DQ + 256] += jnp.dot(block, both, preferred_element_type=jnp.float32)
        acc[rows, DV:DV + 128] += jnp.dot(block, dv[ks, :], preferred_element_type=jnp.float32)

    def multiply_other(t, h):
        for q in (2 * h, 2 * h + 1):
            arrive_x(other(t), q)
        multiply(False, other(t), h)

    def receive_x(t, q, sem):
        arrive_x(t, q)
        send_x(False, t, q, sibling, sem)

    low = lax.broadcasted_iota(jnp.int32, (QUARTER, 128), 1) < 64
    slot = y % 2

    def head_copies(i, u):
        return [
            remote(msg.at[i, u, pl.ds(0, 256)], kv_ref.at[sp, u], send_a.at[i, u, 0], recv_kv.at[sp, u], partners[i]),
            remote(msg.at[i, u, pl.ds(256, 128)], q_ref.at[slot, u], send_a.at[i, u, 1], recv_q.at[slot, u], partners[i]),
        ]

    def lam_copy(i):
        return remote(lam_ref.at[i], lamo_ref.at[slot], send_lam.at[i], recv_lam.at[slot], partners[i])

    edges = [
        remote(keys.at[pl.ds(WINDOW, WINDOW)], halo_ref.at[1], send_halo.at[1], recv_halo.at[1], before),
        remote(keys.at[pl.ds(ROWS, WINDOW)], halo_ref.at[0], send_halo.at[0], recv_halo.at[0], after),
    ]

    def pack(u):
        first, second = pl.ds(u * HALF, QUARTER), pl.ds(u * HALF + QUARTER, QUARTER)
        k0, k1 = acc[first, DK:DK + 128], acc[second, DK:DK + 128]
        msg[0, u, 0:128] = jnp.where(low, k0, pltpu.roll(k1, 64, 1)).astype(jnp.bfloat16)
        msg[1, u, 0:128] = jnp.where(low, pltpu.roll(k0, 64, 1), k1).astype(jnp.bfloat16)
        for j, part in enumerate((first, second)):
            turned = acc[part, DV:DV + 128].T.astype(jnp.bfloat16)
            asked = (acc[part, DQ:DQ + 128].T * Q_SCALE).astype(jnp.bfloat16)
            for head in range(2):
                msg[head, u, 128 + j * 64:128 + (j + 1) * 64] = turned[head * 64:(head + 1) * 64]
                msg[head, u, 256 + j * 64:256 + (j + 1) * 64] = asked[head * 64:(head + 1) * 64]
        for i in range(2):
            def leave(i=i):
                for copy in head_copies(i, u):
                    copy.start()
            pl.when(away[i])(leave)
            def stay(i=i):
                copies = [
                    pltpu.make_async_copy(msg.at[i, u, pl.ds(0, 256)], kv_ref.at[sp, u], local_sem.at[0]),
                    pltpu.make_async_copy(msg.at[i, u, pl.ds(256, 128)], q_ref.at[slot, u], local_sem.at[1]),
                ]
                for copy in copies:
                    copy.start()
                for copy in copies:
                    copy.wait()
            pl.when(jnp.logical_not(away[i]))(stay)
        for j, part in enumerate((first, second)):
            pair = jnp.where(low, acc[part, 256:384], acc[part, 128:256]).astype(jnp.bfloat16)
            asks = acc[part, 0:256].astype(jnp.bfloat16)
            for g in range(4):
                at = (j * 4 + g) * 2 * SHARE + u * SHARE
                keys[WINDOW + at:WINDOW + at + SHARE] = pair[g * SHARE:(g + 1) * SHARE]
                winq[at:at + SHARE] = asks[g * SHARE:(g + 1) * SHARE]

    def block(zz, s, core):
        return ((zz + NZ) % NZ) * NY + 2 * core + s

    def forward(b, u, device, sem):
        go(remote(kv_ref.at[b, u], kv_ref.at[b, u], sem, recv_kv.at[b, u], device))

    def arrive(b, u):
        remote(kv_ref.at[b, u], kv_ref.at[b, u], send_sib.at[0, 0], recv_kv.at[b, u], sibling).wait_recv()

    def open_ring(u):
        for s in range(2):
            b = block(z, s, c)
            pl.when(away[s])(lambda: arrive(b, u))
            forward(b, u, up, send_ring.at[0, s, u, 0])
            forward(b, u, down, send_ring.at[1, s, u, 0])
            forward(b, u, sibling, send_sib.at[s, u])

    shared = [2, 2]

    def ring(u, d):
        for s in range(2):
            for way, (reach, device, sign) in enumerate(((4 - s, up, -1), (3 + s, down, 1))):
                if d > reach:
                    continue
                b = block(z + sign * d, s, c)
                arrive(b, u)
                if d < reach:
                    forward(b, u, device, send_ring.at[way, s, u, d])
                forward(b, u, sibling, send_sib.at[shared[u], u])
                shared[u] += 1

    def turn(i):
        pair = keys[i * 128:(i + 1) * 128].astype(jnp.float32)
        v_t[:, i * 128:(i + 1) * 128] = pair.T[0:HEAD].astype(jnp.bfloat16)

    def band_edges():
        for copy in edges:
            copy.wait_recv()
        keys[0:WINDOW] = halo_ref[0]
        keys[WINDOW + ROWS:] = halo_ref[1]
        turn(0)
        turn(5)

    def band(i):
        q_t = winq[i * 128:(i + 1) * 128].astype(jnp.float32).T * HEAD ** (-0.5)
        zero = jnp.zeros((HEAD, 128), jnp.float32)
        query = jnp.concatenate(
            [jnp.concatenate([zero, q_t[g * HEAD:(g + 1) * HEAD]], axis=0) for g in range(GROUP)], axis=1
        ).astype(jnp.bfloat16)
        s = jnp.dot(keys[i * 128:i * 128 + 384], query, preferred_element_type=jnp.float32)
        key = lax.broadcasted_iota(jnp.int32, (384, 128), 0)
        ask = lax.broadcasted_iota(jnp.int32, (384, 128), 1)
        start = sp * ROWS + (i - 1) * 128
        allowed = (
            (key - ask >= 0) & (key - ask <= 2 * WINDOW) & (start + key >= 0) & (start + key < live)
        )
        for g in range(GROUP):
            own = jnp.where(allowed, s[:, g * 128:(g + 1) * 128], masked_score)
            top = jnp.maximum(jnp.max(own, axis=0, keepdims=True), sink_ref[g])
            e = jnp.where(allowed, jnp.exp(own - top), 0.0)
            total = jnp.sum(e, axis=0, keepdims=True) + jnp.exp(sink_ref[g] - top)
            o = jnp.dot(v_t[:, i * 128:i * 128 + 384], e.astype(jnp.bfloat16), preferred_element_type=jnp.float32)
            ok = (start + 128 + lax.broadcasted_iota(jnp.int32, (HEAD, 128), 1)) < live
            o = jnp.where(ok, o / total, 0.0)
            both = jnp.concatenate([o, jnp.zeros_like(o)], axis=0).T
            win_ref[i * 128:(i + 1) * 128, g * HEAD:(g + 1) * HEAD] = both[:, 0:HEAD].astype(jnp.bfloat16)

    def nth(i):
        at = i + 4
        d, r = at // 8, at % 8
        sign, core = 2 * (r // 4) - 1, r % 4 // 2
        zz = (z + sign * d + NZ) % NZ
        return zz * NY + 2 * (c + core - 2 * c * core) + r % 2, core == 1

    def set_queries():
        for s in range(2):
            for u in range(2):
                for j in range(2):
                    q = q_ref[s, u, j * 64:(j + 1) * 64, :]
                    for h in range(2):
                        for m in range(2):
                            at = u * TILE + m * ROWS + s * HALF + j * 128
                            qz[h, h * 64 + m * 32:h * 64 + (m + 1) * 32, at:at + 128] = q[m * 32:(m + 1) * 32]

    def set_values(b):
        lane = lax.broadcasted_iota(jnp.int32, (64, 128), 1)
        row = lax.broadcasted_iota(jnp.int32, (16, 128), 0)
        for h in range(2):
            for u in range(2):
                at = h * 256 + u * 128
                ok = b * ROWS + natural(h * 128 + lane, u) < live
                v = kv_ref[b, u, 128 + h * 64:128 + (h + 1) * 64, :].astype(jnp.float32)
                va[0:64, at:at + 128] = jnp.where(ok, v, 0.0).astype(jnp.bfloat16)
                va[64:80, at:at + 128] = jnp.where(ok[:16] & (row == 0), 1.0, 0.0).astype(jnp.bfloat16)

    def set_bias(b):
        row = lax.broadcasted_iota(jnp.int32, (128, 128), 0)
        for h in range(2):
            for u in range(2):
                ok = b * ROWS + natural(h * 128 + row, u) < live
                bias[h, u * 128:(u + 1) * 128] = jnp.where(ok, 0.0, masked_score)

    def score(b, n, h, to):
        k = jnp.concatenate([kv_ref[b, 0, 0:128, :], kv_ref[b, 1, 0:128, :]], axis=0)
        s = jnp.dot(k, qz[h, :, n * TILE:(n + 1) * TILE], preferred_element_type=jnp.float32)
        s = s + jnp.concatenate([bias[h]] * (TILE // 128), axis=1)
        s_buf[to] = s
        t_buf[to] = jnp.max(s.reshape(32, 8, TILE), axis=0)

    def segment(low_i, high_i, ns, fresh):
        units = [(n, h) for n in ns for h in range(2)]
        start = nth(low_i)[0]
        set_bias(start)
        score(start, *units[0], 0)

        def step(i, carry):
            b, _ = nth(i)
            following, foreign = nth(jnp.minimum(i + 1, high_i - 1))
            if fresh:
                @pl.when(jnp.logical_and(foreign, i + 1 < high_i))
                def _():
                    arrive(following, 0)
                    arrive(following, 1)

            set_values(b)
            for j, (n, h) in enumerate(units):
                cols = slice(n * TILE, (n + 1) * TILE)
                s = s_buf[j % 2]
                top = t_buf[j % 2]
                if j + 1 < len(units):
                    score(b, *units[j + 1], 1 - j % 2)
                else:
                    set_bias(following)
                    score(following, *units[0], 1 - j % 2)
                old = m_buf[:, cols]
                new = jnp.maximum(old, jnp.broadcast_to(jnp.max(top, axis=0, keepdims=True), (8, TILE)))
                m_buf[:, cols] = new
                e = jnp.exp2(s.reshape(32, 8, TILE) - new[None]).reshape(256, TILE).astype(jnp.bfloat16)
                held = (att[:, cols].reshape(10, 8, TILE) * jnp.exp2(old - new)[None]).reshape(80, TILE)
                att[:, cols] = held + jnp.dot(
                    va[:, h * 256:(h + 1) * 256], e, preferred_element_type=jnp.float32
                )
            return carry

        lax.fori_loop(low_i, high_i, step, 0)

    def back(n, i):
        return remote(o_buf.at[n, i], rows_t.at[n, slot], send_o.at[n, i], recv_o.at[n, slot], partners[i])

    def finish(n):
        row = gain_ref[...]
        gain = jnp.broadcast_to(jnp.concatenate([row, row], axis=1), (128, 128)).T[0:HEAD]
        lam = lamo_ref[0, 0:1, :]
        lane = lax.broadcasted_iota(jnp.int32, (HEAD, 128), 1)
        for s in range(2):
            for j in range(2):
                maps = []
                for m in range(2):
                    at = n * TILE + m * ROWS + s * HALF + j * 128
                    total = att[64:65, at:at + 128]
                    maps.append(att[0:64, at:at + 128] / jnp.where(total > 0.0, total, 1.0))
                mixed = maps[0] - lam * maps[1]
                normed = mixed * lax.rsqrt(jnp.mean(mixed * mixed, axis=0, keepdims=True) + epsilon) * gain
                ok = (z * NY + 2 * c + s) * ROWS + natural(j * 128 + lane, n) < live
                o_buf[n, s, j * 64:(j + 1) * 64, :] = jnp.where(ok, normed, 0.0).astype(jnp.bfloat16)
        for i in range(2):
            pl.when(away[i])(lambda i=i: back(n, i).start())
            def stay(i=i):
                copy = pltpu.make_async_copy(o_buf.at[n, i], rows_t.at[n, slot], local_sem.at[0])
                copy.start()
                copy.wait()
            pl.when(jnp.logical_not(away[i]))(stay)

    order = (0, 2, 1, 3)

    def owner(side, r):
        return ((x + r) % NX) * 2 + (c if side else 1 - c)

    def partial(n, side, k):
        cols = slice(k * CHUNK, (k + 1) * CHUNK)
        return jnp.dot(lhs_w[n, side], wo[:, cols], preferred_element_type=jnp.float32) + jnp.dot(
            lhs_d[n, side], do[:, cols], preferred_element_type=jnp.float32
        )

    def given(n, k):
        return remote(give.at[n, k], take.at[n, k], send_g.at[n, k], recv_g.at[n, k], sibling)

    def far(n, k):
        return remote(mine.at[n, 2, k], far_in.at[n, k], send_f.at[n, k], recv_f.at[n, k], right if k < 2 else left)

    def near(n, src, k, way):
        return remote(src, fin.at[n, way, k], send_n.at[n, way, k], recv_n.at[n, way, k], left if way else right)

    def merge_give(n):
        for i in range(2):
            def wait(i=i):
                remote(o_buf.at[n, i], rows_t.at[n, i], send_o.at[n, i], recv_o.at[n, i], partners[i]).wait_recv()
            pl.when(away[i])(wait)
        for j in range(2):
            pair = jnp.concatenate(
                [rows_t[n, 0, j * 64:(j + 1) * 64], rows_t[n, 1, j * 64:(j + 1) * 64]], axis=0
            ).astype(jnp.float32)
            diff_rows[j * 128:(j + 1) * 128] = pair.T.astype(jnp.bfloat16)
        for side in range(2):
            for r in range(NX):
                t = owner(side, r)
                to = slice(r * SHARE, (r + 1) * SHARE)
                lhs_w[n, side, to] = win_ref[pl.ds(pl.multiple_of(t * 2 * SHARE + n * SHARE, SHARE), SHARE)]
                lhs_d[n, side, to] = diff_rows[pl.ds(pl.multiple_of(t * SHARE, SHARE), SHARE)]
        for k in order:
            give[n, k] = partial(n, 0, k).astype(jnp.bfloat16)
            go(given(n, k))

    def merge_send(n):
        for k in order:
            own = partial(n, 1, k)
            given(n, k).wait_recv()
            both = (own + take[n, k].astype(jnp.float32)).astype(jnp.bfloat16)
            for r in range(NX):
                mine[n, r, k] = both[r * SHARE:(r + 1) * SHARE]
            go(far(n, k))
        for i in range(2):
            go(near(n, mine.at[n, 1, 2 + i], 2 + i, 0))
            go(near(n, mine.at[n, 3, i], i, 1))

    def merge_join(n):
        for k in order:
            way = 0 if k < 2 else 1
            far(n, k).wait_recv()
            joined[n, k] = (
                mine[n, 3 if way else 1, k].astype(jnp.float32) + far_in[n, k].astype(jnp.float32)
            ).astype(jnp.bfloat16)
            go(near(n, joined.at[n, k], k, way))

    def merge_out(n):
        for k in order:
            near(n, joined.at[n, k], k, 0).wait_recv()
            near(n, joined.at[n, k], k, 1).wait_recv()
            value = (
                mine[n, 0, k].astype(jnp.float32)
                + fin[n, 0, k].astype(jnp.float32)
                + fin[n, 1, k].astype(jnp.float32)
            )
            out_ref[n * SHARE:(n + 1) * SHARE, k * CHUNK:(k + 1) * CHUNK] = value.astype(jnp.bfloat16)

    for q in range(2):
        send_x(True, tp, q, right, send_xr.at[q])
        send_x(True, tp, q, left, send_xl.at[q])
    for q in range(4):
        send_x(True, tp, q, sibling, send_xs.at[q])
    acc[...] = jnp.zeros_like(acc)
    for i in range(2):
        pl.when(away[i])(lambda i=i: lam_copy(i).start())
        def keep(i=i):
            copy = pltpu.make_async_copy(lam_ref.at[i], lamo_ref.at[slot], local_sem.at[2])
            copy.start()
            copy.wait()
        pl.when(jnp.logical_not(away[i]))(keep)
    for load in loads:
        load.wait()
    multiply(True, tp, 0)
    receive_x(t_left, 0, send_xs.at[4])
    send_x(False, t_left, 0, right, send_xr.at[2])
    for q in (2, 3):
        send_x(True, tp, q, right, send_xr.at[q + 1])
    receive_x(t_right, 0, send_xs.at[5])
    multiply(True, tp, 1)
    receive_x(t_right, 1, send_xs.at[6])
    send_x(False, t_right, 1, left, send_xl.at[2])
    for q in (2, 3):
        send_x(True, tp, q, left, send_xl.at[q + 1])
    receive_x(t_left, 1, send_xs.at[7])
    multiply_other(tp, 0)
    multiply_other(tp, 1)
    multiply(False, t_left, 0)
    multiply(False, t_right, 0)
    multiply_other(t_left, 0)
    multiply_other(t_right, 0)
    receive_x(t_far, 0, send_xs.at[8])
    receive_x(t_far, 1, send_xs.at[9])
    multiply(False, t_far, 0)
    multiply_other(t_far, 0)
    pack(0)
    receive_x(t_left, 2, send_xs.at[10])
    send_x(False, t_left, 2, right, send_xr.at[5])
    receive_x(t_right, 2, send_xs.at[11])
    receive_x(t_right, 3, send_xs.at[12])
    send_x(False, t_right, 3, left, send_xl.at[5])
    receive_x(t_left, 3, send_xs.at[13])
    open_ring(0)
    multiply(False, t_left, 1)
    multiply(False, t_right, 1)
    multiply_other(t_left, 1)
    multiply_other(t_right, 1)
    receive_x(t_far, 2, send_xs.at[14])
    receive_x(t_far, 3, send_xs.at[15])
    multiply(False, t_far, 1)
    ring(0, 1)
    multiply_other(t_far, 1)
    pack(1)
    for copy in edges:
        copy.start()
    att[...] = jnp.zeros_like(att)
    va[...] = jnp.zeros_like(va)
    qz[...] = jnp.zeros_like(qz)
    m_buf[...] = jnp.full_like(m_buf, masked_score)
    for i in range(1, 5):
        turn(i)
    band(1)
    band(2)
    open_ring(1)
    for i in range(2):
        def rest(i=i):
            for u in range(2):
                remote(
                    msg.at[0, u, pl.ds(256, 128)], q_ref.at[i, u], send_a.at[0, u, 1], recv_q.at[i, u], sibling
                ).wait_recv()
            remote(lam_ref.at[0], lamo_ref.at[i], send_lam.at[0], recv_lam.at[i], sibling).wait_recv()
        pl.when(away[i])(rest)
    set_queries()
    ring(0, 2)
    segment(0, 4, (0, 1), True)
    ring(0, 3)
    ring(1, 1)
    segment(4, 12, (0, 1), True)
    ring(1, 2)
    ring(0, 4)
    segment(12, 20, (0,), True)
    ring(1, 3)
    segment(20, 28, (0,), True)
    ring(1, 4)
    band_edges()
    band(0)
    band(3)
    segment(28, 32, (0,), True)
    finish(0)
    segment(12, 18, (1,), False)
    merge_give(0)
    segment(18, 20, (1,), False)
    merge_send(0)
    segment(20, 26, (1,), False)
    merge_join(0)
    segment(26, 32, (1,), False)
    finish(1)
    merge_out(0)
    merge_give(1)
    merge_send(1)
    merge_join(1)
    merge_out(1)
    for copy in started + edges:
        copy.wait_send()
    for i in range(2):
        def sent(i=i):
            for u in range(2):
                for copy in head_copies(i, u):
                    copy.wait_send()
                back(u, i).wait_send()
            lam_copy(i).wait_send()
        pl.when(away[i])(sent)


def layer(length, mix_lambda, sink_logit, inputs, gain, weights):
    bf, f32 = jnp.bfloat16, jnp.float32
    depth = weights[3].shape[0]
    width = weights[6].shape[1]
    dma = pltpu.SemaphoreType.DMA
    vmem = pltpu.VMEM
    return pl.pallas_call(
        layer_kernel,
        out_shape=jax.ShapeDtypeStruct((2 * SHARE, width), bf),
        in_specs=[SMEM_SPEC] * 3 + [VMEM_SPEC] * 2 + [HBM_SPEC] * 8,
        out_specs=VMEM_SPEC,
        scratch_shapes=[
            vmem((GROUPS, 2, GROUPS, SHARE, ROWS), bf),
            vmem((320, depth), bf),
            vmem((depth, 128), bf),
            vmem((depth, 128), bf),
            vmem((depth, 128), bf),
            vmem((GROUP * HEAD, width), bf),
            vmem((128, width), bf),
            vmem((ROWS, ACC_COLS), f32),
            vmem((2, 2, 384, 128), bf),
            vmem((2, 8, 128), f32),
            vmem((2, 8, 128), f32),
            vmem((2, WINDOW, 128), bf),
            vmem((ROWS, 256), bf),
            vmem((ROWS + 2 * WINDOW, 128), bf),
            vmem((HEAD, ROWS + 2 * WINDOW), bf),
            vmem((ROWS, GROUP * HEAD), bf),
            vmem((BLOCKS, 2, HALF, 128), bf),
            vmem((2, 2, 128, 128), bf),
            vmem((2, 128, 2 * TILE), bf),
            vmem((80, ROWS), bf),
            vmem((80, 2 * TILE), f32),
            vmem((2, 256, TILE), f32),
            vmem((2, 8, TILE), f32),
            vmem((8, 2 * TILE), f32),
            vmem((2, 256, 128), f32),
            vmem((2, 2, 128, 128), bf),
            vmem((2, 2, 128, 128), bf),
            vmem((HALF, 128), bf),
            vmem((2, 2, 128, GROUP * HEAD), bf),
            vmem((2, 2, 128, 128), bf),
            vmem((2, CHUNKS, 128, CHUNK), bf),
            vmem((2, CHUNKS, 128, CHUNK), bf),
            vmem((2, NX, CHUNKS, SHARE, CHUNK), bf),
            vmem((2, CHUNKS, SHARE, CHUNK), bf),
            vmem((2, CHUNKS, SHARE, CHUNK), bf),
            vmem((2, 2, CHUNKS, SHARE, CHUNK), bf),
            dma((8,)), dma((GROUPS, 4)), dma((6,)), dma((6,)), dma((16,)),
            dma((BLOCKS, 2)), dma((2, 2)), dma((2,)), dma((2,)),
            dma((2, 2, 2)), dma((2,)), dma((2, 2, 2, 4)), dma((16, 2)), dma((2,)), dma((3,)),
            dma((2, 2)), dma((2, 2)), dma((2, CHUNKS)), dma((2, CHUNKS)), dma((2, CHUNKS)), dma((2, CHUNKS)),
            dma((2, 2, CHUNKS)), dma((2, 2, CHUNKS)),
        ],
        compiler_params=pltpu.CompilerParams(
            collective_id=0, has_side_effects=True, vmem_limit_bytes=62 * 1024 * 1024
        ),
        name="layer",
    )(length, mix_lambda, sink_logit, inputs, gain, *weights)


def body(
    inputs, length, win_query, win_key, win_value, sink_logit,
    diff_query, diff_key, diff_value, mix_lambda, head_gain, win_out, diff_out,
):
    weights = (
        win_query.T, win_key.T, win_value.T, diff_query, diff_key, diff_value, win_out, diff_out,
    )
    rows = inputs.reshape(GROUPS, 2, SHARE, inputs.shape[1])
    return layer(length, mix_lambda, sink_logit, rows, head_gain.reshape(1, HEAD), weights)


def solution(mesh):
    placed = (
        P("sp", "tp"), P(), P(None, "tp"), P(None, "tp"), P(None, "tp"), P("tp"), P(None, "tp"),
        P(None, "tp"), P(None, "tp"), P("tp"), P(), P("tp", None), P("tp", None),
    )
    return jax.shard_map(
        body, mesh=mesh, in_specs=placed, out_specs=P(("sp", "tp"), None), check_vma=False
    )
```

```python
import functools

import jax
import jax.numpy as jnp
from jax import lax
from jax.experimental import pallas as pl
from jax.experimental.pallas import tpu as pltpu
from jax.sharding import PartitionSpec as P

HEAD = 64
DQK = 32
GROUP = 3
WINDOW = 128
NX, NY, NZ = 4, 4, 8
ROWS = 512
QUARTER = ROWS // 4
HALF = ROWS // 2
BLOCKS = NY * NZ
Q_SCALE = 1.4426950408889634 * DQK ** (-0.5)
MESH = pl.DeviceIdType.MESH

epsilon = 1e-06
masked_score = -1e30
VMEM_SPEC = pl.BlockSpec(memory_space=pltpu.VMEM)
SMEM_SPEC = pl.BlockSpec(memory_space=pltpu.SMEM)
HBM_SPEC = pl.BlockSpec(memory_space=pltpu.HBM)


def place():
    sp, tp = lax.axis_index("sp"), lax.axis_index("tp")
    return sp // NY, sp % NY, tp // 2, tp % 2


def greet(devices, conditions=None):
    barrier = pltpu.get_barrier_semaphore()
    for i, device in enumerate(devices):
        def signal(device=device):
            pl.semaphore_signal(barrier, inc=1, device_id=device, device_id_type=MESH)
        if conditions is None or conditions[i] is None:
            signal()
        else:
            pl.when(conditions[i])(signal)


WQ, DQ, DK, DV, ACC_COLS = 0, 384, 512, 640, 768
TILE = 2 * ROWS
CHUNK = 1024
CHUNKS = 4
SHARE = 32
GROUPS = 2 * NX


def natural(r, u):
    return (r // SHARE) * 2 * SHARE + u * SHARE + r % SHARE


def layer_kernel(
    length_ref, lam_smem, sink_ref, x_ref, gain_ref, wq_hbm, wk_hbm, wv_hbm, dq_hbm, dk_hbm, dv_hbm, wo_hbm, do_hbm,
    out_ref,
    xg, wt, dq, dk, dv, wo, do, acc, msg, lam_ref, lamo_ref, halo_ref, winq, keys, v_t, win_ref,
    kv_ref, q_ref, qz, va, att, s_buf, t_buf, m_buf, bias, row_at, lane_at,
    o_buf, rows_t, diff_rows, lhs_w, lhs_d, give, take, mine, far_in, joined, fin,
    w_sem, recv_x, send_xs,
    recv_kv, recv_q, recv_lam, recv_halo, send_a, send_lam, send_ring, send_sib, send_halo, local_sem,
    recv_o, send_o, send_g, recv_g, send_f, recv_f, send_n, recv_n,
):
    z, y, x, c = place()
    sp = z * NY + y
    tp = x * 2 + c
    live = length_ref[0]
    right = (sp, ((x + 1) % NX) * 2 + c)
    left = (sp, ((x + NX - 1) % NX) * 2 + c)
    sibling = (sp, x * 2 + 1 - c)
    up = (((z + 1) % NZ) * NY + y, tp)
    down = (((z + NZ - 1) % NZ) * NY + y, tp)
    after = ((sp + 1) % BLOCKS, tp)
    before = ((sp + BLOCKS - 1) % BLOCKS, tp)
    partners = [(z * NY + 2 * c + i, x * 2 + y // 2) for i in range(2)]
    away = [(2 * c + i) != y for i in range(2)]

    loads = [
        pltpu.make_async_copy(src, dst, w_sem.at[i])
        for i, (src, dst) in enumerate(
            (
                (wq_hbm, wt.at[pl.ds(0, 192)]),
                (wk_hbm, wt.at[pl.ds(192, 64)]),
                (wv_hbm, wt.at[pl.ds(256, 64)]),
                (dq_hbm, dq),
                (dk_hbm, dk),
                (dv_hbm, dv),
                (wo_hbm, wo),
                (do_hbm, do),
            )
        )
    ]
    for load in loads:
        load.start()
    for i in range(2):
        lam_ref[i] = jnp.full((8, 128), lam_smem[i], jnp.float32)
    greet(
        (right, left, sibling, up, down, after, before) + tuple(partners), (None,) * 7 + tuple(away)
    )
    pl.semaphore_wait(pltpu.get_barrier_semaphore(), 7 + sum(a.astype(jnp.int32) for a in away))

    def remote(src, dst, send_sem, recv_sem, device):
        return pltpu.make_async_remote_copy(
            src_ref=src, dst_ref=dst, send_sem=send_sem, recv_sem=recv_sem,
            device_id=device, device_id_type=MESH,
        )

    def go(copy):
        copy.start()

    def send_x(own, t, q, device):
        part = pl.ds(q % 2 * 4, 4)
        src = x_ref.at[part, q // 2] if own else xg.at[t, q // 2, part]
        go(remote(src, xg.at[t, q // 2, part], send_xs, recv_x.at[t, q], device))

    def arrive_x(t, q):
        part = xg.at[t, q // 2, pl.ds(q % 2 * 4, 4)]
        remote(part, part, send_xs, recv_x.at[t, q], sibling).wait_recv()

    t_left = ((x + NX - 1) % NX) * 2 + c
    t_right = ((x + 1) % NX) * 2 + c
    t_far = ((x + 2) % NX) * 2 + c

    def other(t):
        return t + 1 - 2 * c

    def multiply(own, t, h):
        rows = pl.ds(h * HALF, HALF)
        block = (x_ref[:, h] if own else xg[t, h]).reshape(HALF, ROWS)
        ks = pl.ds(pl.multiple_of(t * ROWS, ROWS), ROWS)
        acc[rows, WQ:WQ + 320] += lax.dot_general(
            block, wt[:, ks], (((1,), (1,)), ((), ())), preferred_element_type=jnp.float32
        )
        both = jnp.concatenate([dq[ks, :], dk[ks, :]], axis=1)
        acc[rows, DQ:DQ + 256] += jnp.dot(block, both, preferred_element_type=jnp.float32)
        acc[rows, DV:DV + 128] += jnp.dot(block, dv[ks, :], preferred_element_type=jnp.float32)

    def multiply_other(t, h):
        for q in (2 * h, 2 * h + 1):
            arrive_x(other(t), q)
        multiply(False, other(t), h)

    def receive_x(t, q):
        arrive_x(t, q)
        send_x(False, t, q, sibling)

    low = lax.broadcasted_iota(jnp.int32, (QUARTER, 128), 1) < 64
    slot = y % 2

    def head_copies(i, u):
        return [
            remote(msg.at[i, u, pl.ds(0, 256)], kv_ref.at[sp, u], send_a.at[i, u, 0], recv_kv.at[sp, u], partners[i]),
            remote(msg.at[i, u, pl.ds(256, 128)], q_ref.at[slot, u], send_a.at[i, u, 1], recv_q.at[slot, u], partners[i]),
        ]

    def lam_copy(i):
        return remote(lam_ref.at[i], lamo_ref.at[slot], send_lam.at[i], recv_lam.at[slot], partners[i])

    edges = [
        remote(keys.at[pl.ds(WINDOW, WINDOW)], halo_ref.at[1], send_halo.at[1], recv_halo.at[1], before),
        remote(keys.at[pl.ds(ROWS, WINDOW)], halo_ref.at[0], send_halo.at[0], recv_halo.at[0], after),
    ]

    def pack(u):
        first, second = pl.ds(u * HALF, QUARTER), pl.ds(u * HALF + QUARTER, QUARTER)
        k0, k1 = acc[first, DK:DK + 128], acc[second, DK:DK + 128]
        msg[0, u, 0:128] = jnp.where(low, k0, pltpu.roll(k1, 64, 1)).astype(jnp.bfloat16)
        msg[1, u, 0:128] = jnp.where(low, pltpu.roll(k0, 64, 1), k1).astype(jnp.bfloat16)
        for j, part in enumerate((first, second)):
            turned = acc[part, DV:DV + 128].T.astype(jnp.bfloat16)
            asked = (acc[part, DQ:DQ + 128].T * Q_SCALE).astype(jnp.bfloat16)
            for head in range(2):
                msg[head, u, 128 + j * 64:128 + (j + 1) * 64] = turned[head * 64:(head + 1) * 64]
                msg[head, u, 256 + j * 64:256 + (j + 1) * 64] = asked[head * 64:(head + 1) * 64]
        for i in range(2):
            def leave(i=i):
                for copy in head_copies(i, u):
                    copy.start()
            pl.when(away[i])(leave)
            def stay(i=i):
                copies = [
                    pltpu.make_async_copy(msg.at[i, u, pl.ds(0, 256)], kv_ref.at[sp, u], local_sem.at[0]),
                    pltpu.make_async_copy(msg.at[i, u, pl.ds(256, 128)], q_ref.at[slot, u], local_sem.at[1]),
                ]
                for copy in copies:
                    copy.start()
                for copy in copies:
                    copy.wait()
            pl.when(jnp.logical_not(away[i]))(stay)
        for j, part in enumerate((first, second)):
            pair = jnp.where(low, acc[part, 256:384], acc[part, 128:256]).astype(jnp.bfloat16)
            asks = acc[part, 0:256].astype(jnp.bfloat16)
            for g in range(4):
                at = (j * 4 + g) * 2 * SHARE + u * SHARE
                keys[WINDOW + at:WINDOW + at + SHARE] = pair[g * SHARE:(g + 1) * SHARE]
                winq[at:at + SHARE] = asks[g * SHARE:(g + 1) * SHARE]

    def block(zz, s, core):
        return ((zz + NZ) % NZ) * NY + 2 * core + s

    def forward(b, u, device, sem):
        go(remote(kv_ref.at[b, u], kv_ref.at[b, u], sem, recv_kv.at[b, u], device))

    def arrive(b, u):
        remote(kv_ref.at[b, u], kv_ref.at[b, u], send_sib, recv_kv.at[b, u], sibling).wait_recv()

    def open_ring(u):
        for s in range(2):
            b = block(z, s, c)
            pl.when(away[s])(lambda: arrive(b, u))
            forward(b, u, up, send_ring)
            forward(b, u, down, send_ring)
            forward(b, u, sibling, send_sib)

    def ring(u, d):
        for s in range(2):
            for way, (reach, device, sign) in enumerate(((4 - s, up, -1), (3 + s, down, 1))):
                if d > reach:
                    continue
                b = block(z + sign * d, s, c)
                arrive(b, u)
                if d < reach:
                    forward(b, u, device, send_ring)
                forward(b, u, sibling, send_sib)

    def turn(i):
        pair = keys[i * 128:(i + 1) * 128].astype(jnp.float32)
        v_t[:, i * 128:(i + 1) * 128] = pair.T[0:HEAD].astype(jnp.bfloat16)

    def band_edges():
        for copy in edges:
            copy.wait_recv()
        keys[0:WINDOW] = halo_ref[0]
        keys[WINDOW + ROWS:] = halo_ref[1]
        turn(0)
        turn(5)

    def band(i):
        q_t = winq[i * 128:(i + 1) * 128].astype(jnp.float32).T * HEAD ** (-0.5)
        zero = jnp.zeros((HEAD, 128), jnp.float32)
        query = jnp.concatenate(
            [jnp.concatenate([zero, q_t[g * HEAD:(g + 1) * HEAD]], axis=0) for g in range(GROUP)], axis=1
        ).astype(jnp.bfloat16)
        s = jnp.dot(keys[i * 128:i * 128 + 384], query, preferred_element_type=jnp.float32)
        key = lax.broadcasted_iota(jnp.int32, (384, 128), 0)
        ask = lax.broadcasted_iota(jnp.int32, (384, 128), 1)
        start = sp * ROWS + (i - 1) * 128
        allowed = (
            (key - ask >= 0) & (key - ask <= 2 * WINDOW) & (start + key >= 0) & (start + key < live)
        )
        for g in range(GROUP):
            own = jnp.where(allowed, s[:, g * 128:(g + 1) * 128], masked_score)
            top = jnp.maximum(jnp.max(own, axis=0, keepdims=True), sink_ref[g])
            e = jnp.where(allowed, jnp.exp(own - top), 0.0)
            total = jnp.sum(e, axis=0, keepdims=True) + jnp.exp(sink_ref[g] - top)
            o = jnp.dot(v_t[:, i * 128:i * 128 + 384], e.astype(jnp.bfloat16), preferred_element_type=jnp.float32)
            ok = (start + 128 + lax.broadcasted_iota(jnp.int32, (HEAD, 128), 1)) < live
            o = jnp.where(ok, o / total, 0.0)
            both = jnp.concatenate([o, jnp.zeros_like(o)], axis=0).T
            win_ref[i * 128:(i + 1) * 128, g * HEAD:(g + 1) * HEAD] = both[:, 0:HEAD].astype(jnp.bfloat16)

    def nth(i):
        at = i + 4
        d, r = at // 8, at % 8
        sign, core = 2 * (r // 4) - 1, r % 4 // 2
        zz = (z + sign * d + NZ) % NZ
        return zz * NY + 2 * (c + core - 2 * c * core) + r % 2, core == 1

    def set_queries():
        for s in range(2):
            for u in range(2):
                for j in range(2):
                    q = q_ref[s, u, j * 64:(j + 1) * 64, :]
                    for h in range(2):
                        for m in range(2):
                            at = u * TILE + m * ROWS + s * HALF + j * 128
                            qz[h, h * 64 + m * 32:h * 64 + (m + 1) * 32, at:at + 128] = q[m * 32:(m + 1) * 32]

    def set_table():
        row = lax.broadcasted_iota(jnp.int32, (128, 128), 0)
        lane = lax.broadcasted_iota(jnp.int32, (8, 128), 1)
        for h in range(2):
            for u in range(2):
                row_at[h, u * 128:(u + 1) * 128] = natural(h * 128 + row, u)
                lane_at[h, u] = natural(h * 128 + lane, u)

    def set_values(b):
        top = lax.broadcasted_iota(jnp.int32, (8, 128), 0) == 0
        zero = jnp.zeros((8, 128), jnp.float32)
        for h in range(2):
            for u in range(2):
                at = h * 256 + u * 128
                ok = lane_at[h, u] < live - b * ROWS
                v = kv_ref[b, u, 128 + h * 64:128 + (h + 1) * 64, :].astype(jnp.float32)
                v = jnp.where(ok[None], v.reshape(8, 8, 128), 0.0).reshape(64, 128)
                ones = jnp.concatenate([jnp.where(ok & top, 1.0, zero), zero], axis=0)
                va[0:64, at:at + 128] = v.astype(jnp.bfloat16)
                va[64:80, at:at + 128] = ones.astype(jnp.bfloat16)

    def set_bias(b):
        for h in range(2):
            bias[h] = jnp.where(row_at[h] < live - b * ROWS, 0.0, masked_score)

    def score(b, n, h, to):
        k = jnp.concatenate([kv_ref[b, 0, 0:128, :], kv_ref[b, 1, 0:128, :]], axis=0)
        s = jnp.dot(k, qz[h, :, n * TILE:(n + 1) * TILE], preferred_element_type=jnp.float32)
        s = s + jnp.concatenate([bias[h]] * (TILE // 128), axis=1)
        s_buf[to] = s
        t_buf[to] = jnp.max(s.reshape(32, 8, TILE), axis=0)

    def segment(low_i, high_i, ns, fresh):
        units = [(n, h) for n in ns for h in range(2)]
        start = nth(low_i)[0]
        set_bias(start)
        score(start, *units[0], 0)

        def step(i, carry):
            b, _ = nth(i)
            following, foreign = nth(jnp.minimum(i + 1, high_i - 1))
            if fresh:
                @pl.when(jnp.logical_and(foreign, i + 1 < high_i))
                def _():
                    arrive(following, 0)
                    arrive(following, 1)

            set_values(b)
            for j, (n, h) in enumerate(units):
                cols = slice(n * TILE, (n + 1) * TILE)
                s = s_buf[j % 2]
                top = t_buf[j % 2]
                if j + 1 < len(units):
                    score(b, *units[j + 1], 1 - j % 2)
                else:
                    set_bias(following)
                    score(following, *units[0], 1 - j % 2)
                old = m_buf[:, cols]
                new = jnp.maximum(old, jnp.broadcast_to(jnp.max(top, axis=0, keepdims=True), (8, TILE)))
                m_buf[:, cols] = new
                e = jnp.exp2(s.reshape(32, 8, TILE) - new[None]).reshape(256, TILE).astype(jnp.bfloat16)
                held = (att[:, cols].reshape(10, 8, TILE) * jnp.exp2(old - new)[None]).reshape(80, TILE)
                att[:, cols] = held + jnp.dot(
                    va[:, h * 256:(h + 1) * 256], e, preferred_element_type=jnp.float32
                )
            return carry

        lax.fori_loop(low_i, high_i, step, 0)

    def back(n, i):
        return remote(o_buf.at[n, i], rows_t.at[n, slot], send_o.at[n, i], recv_o.at[n, slot], partners[i])

    def finish(n):
        row = gain_ref[...]
        gain = jnp.broadcast_to(jnp.concatenate([row, row], axis=1), (128, 128)).T[0:HEAD]
        lam = lamo_ref[0, 0:1, :]
        for s in range(2):
            for j in range(2):
                maps = []
                for m in range(2):
                    at = n * TILE + m * ROWS + s * HALF + j * 128
                    total = att[64:65, at:at + 128]
                    maps.append(att[0:64, at:at + 128] / jnp.where(total > 0.0, total, 1.0))
                mixed = maps[0] - lam * maps[1]
                normed = mixed * lax.rsqrt(jnp.mean(mixed * mixed, axis=0, keepdims=True) + epsilon) * gain
                ok = (z * NY + 2 * c + s) * ROWS + lane_at[j, n, 0:1] < live
                o_buf[n, s, j * 64:(j + 1) * 64, :] = jnp.where(ok, normed, 0.0).astype(jnp.bfloat16)
        for i in range(2):
            pl.when(away[i])(lambda i=i: back(n, i).start())
            def stay(i=i):
                copy = pltpu.make_async_copy(o_buf.at[n, i], rows_t.at[n, slot], local_sem.at[0])
                copy.start()
                copy.wait()
            pl.when(jnp.logical_not(away[i]))(stay)

    order = (0, 2, 1, 3)

    def owner(side, r):
        return ((x + r) % NX) * 2 + (c if side else 1 - c)

    def partial(n, side, k):
        cols = slice(k * CHUNK, (k + 1) * CHUNK)
        return jnp.dot(lhs_w[n, side], wo[:, cols], preferred_element_type=jnp.float32) + jnp.dot(
            lhs_d[n, side], do[:, cols], preferred_element_type=jnp.float32
        )

    def given(n, k):
        return remote(give.at[n, k], take.at[n, k], send_g, recv_g.at[n, k], sibling)

    def far(n, k):
        return remote(mine.at[n, 2, k], far_in.at[n, k], send_f, recv_f.at[n, k], right if k < 2 else left)

    def near(n, src, k, way):
        return remote(src, fin.at[n, way, k], send_n, recv_n.at[n, way, k], left if way else right)

    def merge_give(n):
        for i in range(2):
            def wait(i=i):
                remote(o_buf.at[n, i], rows_t.at[n, i], send_o.at[n, i], recv_o.at[n, i], partners[i]).wait_recv()
            pl.when(away[i])(wait)
        for j in range(2):
            pair = jnp.concatenate(
                [rows_t[n, 0, j * 64:(j + 1) * 64], rows_t[n, 1, j * 64:(j + 1) * 64]], axis=0
            ).astype(jnp.float32)
            diff_rows[j * 128:(j + 1) * 128] = pair.T.astype(jnp.bfloat16)
        for side in range(2):
            for r in range(NX):
                t = owner(side, r)
                to = slice(r * SHARE, (r + 1) * SHARE)
                lhs_w[n, side, to] = win_ref[pl.ds(pl.multiple_of(t * 2 * SHARE + n * SHARE, SHARE), SHARE)]
                lhs_d[n, side, to] = diff_rows[pl.ds(pl.multiple_of(t * SHARE, SHARE), SHARE)]
        for k in order:
            give[n, k] = partial(n, 0, k).astype(jnp.bfloat16)
            go(given(n, k))

    def merge_send(n):
        for k in order:
            own = partial(n, 1, k)
            given(n, k).wait_recv()
            both = (own + take[n, k].astype(jnp.float32)).astype(jnp.bfloat16)
            for r in range(NX):
                mine[n, r, k] = both[r * SHARE:(r + 1) * SHARE]
            go(far(n, k))
        for i in range(2):
            go(near(n, mine.at[n, 1, 2 + i], 2 + i, 0))
            go(near(n, mine.at[n, 3, i], i, 1))

    def merge_join(n):
        for k in order:
            way = 0 if k < 2 else 1
            far(n, k).wait_recv()
            joined[n, k] = (
                mine[n, 3 if way else 1, k].astype(jnp.float32) + far_in[n, k].astype(jnp.float32)
            ).astype(jnp.bfloat16)
            go(near(n, joined.at[n, k], k, way))

    def merge_out(n):
        for k in order:
            near(n, joined.at[n, k], k, 0).wait_recv()
            near(n, joined.at[n, k], k, 1).wait_recv()
            value = (
                mine[n, 0, k].astype(jnp.float32)
                + fin[n, 0, k].astype(jnp.float32)
                + fin[n, 1, k].astype(jnp.float32)
            )
            out_ref[n * SHARE:(n + 1) * SHARE, k * CHUNK:(k + 1) * CHUNK] = value.astype(jnp.bfloat16)

    for q in range(2):
        send_x(True, tp, q, right)
        send_x(True, tp, q, left)
    for q in range(4):
        send_x(True, tp, q, sibling)
    acc[...] = jnp.zeros_like(acc)
    set_table()
    for i in range(2):
        pl.when(away[i])(lambda i=i: lam_copy(i).start())
        def keep(i=i):
            copy = pltpu.make_async_copy(lam_ref.at[i], lamo_ref.at[slot], local_sem.at[2])
            copy.start()
            copy.wait()
        pl.when(jnp.logical_not(away[i]))(keep)
    for load in loads:
        load.wait()
    multiply(True, tp, 0)
    receive_x(t_left, 0)
    send_x(False, t_left, 0, right)
    for q in (2, 3):
        send_x(True, tp, q, right)
    receive_x(t_right, 0)
    multiply(True, tp, 1)
    receive_x(t_right, 1)
    send_x(False, t_right, 1, left)
    for q in (2, 3):
        send_x(True, tp, q, left)
    receive_x(t_left, 1)
    multiply_other(tp, 0)
    multiply_other(tp, 1)
    multiply(False, t_left, 0)
    multiply(False, t_right, 0)
    multiply_other(t_left, 0)
    multiply_other(t_right, 0)
    receive_x(t_far, 0)
    receive_x(t_far, 1)
    multiply(False, t_far, 0)
    multiply_other(t_far, 0)
    pack(0)
    receive_x(t_left, 2)
    send_x(False, t_left, 2, right)
    receive_x(t_right, 2)
    receive_x(t_right, 3)
    send_x(False, t_right, 3, left)
    receive_x(t_left, 3)
    open_ring(0)
    multiply(False, t_left, 1)
    multiply(False, t_right, 1)
    multiply_other(t_left, 1)
    multiply_other(t_right, 1)
    receive_x(t_far, 2)
    receive_x(t_far, 3)
    multiply(False, t_far, 1)
    ring(0, 1)
    multiply_other(t_far, 1)
    pack(1)
    for copy in edges:
        copy.start()
    att[...] = jnp.zeros_like(att)
    va[...] = jnp.zeros_like(va)
    qz[...] = jnp.zeros_like(qz)
    m_buf[...] = jnp.full_like(m_buf, masked_score)
    for i in range(1, 5):
        turn(i)
    band(1)
    band(2)
    open_ring(1)
    for i in range(2):
        def rest(i=i):
            for u in range(2):
                remote(
                    msg.at[0, u, pl.ds(256, 128)], q_ref.at[i, u], send_a.at[0, u, 1], recv_q.at[i, u], sibling
                ).wait_recv()
            remote(lam_ref.at[0], lamo_ref.at[i], send_lam.at[0], recv_lam.at[i], sibling).wait_recv()
        pl.when(away[i])(rest)
    set_queries()
    ring(0, 2)
    segment(0, 4, (0, 1), True)
    ring(0, 3)
    ring(1, 1)
    segment(4, 12, (0, 1), True)
    ring(1, 2)
    ring(0, 4)
    segment(12, 20, (0,), True)
    ring(1, 3)
    segment(20, 28, (0,), True)
    ring(1, 4)
    band_edges()
    band(0)
    band(3)
    segment(28, 32, (0,), True)
    finish(0)
    segment(12, 18, (1,), False)
    merge_give(0)
    segment(18, 20, (1,), False)
    merge_send(0)
    segment(20, 26, (1,), False)
    merge_join(0)
    segment(26, 32, (1,), False)
    finish(1)
    merge_out(0)
    merge_give(1)
    merge_send(1)
    merge_join(1)
    merge_out(1)
    for ref, sem in (
        (xg.at[pl.ds(0, 7)], send_xs),
        (kv_ref.at[pl.ds(0, 14)], send_ring),
        (kv_ref.at[pl.ds(0, 16)], send_sib),
        (give, send_g),
        (joined, send_f),
        (fin, send_n),
    ):
        remote(ref, ref, sem, recv_x.at[0, 0], sibling).wait_send()
    for copy in edges:
        copy.wait_send()
    for i in range(2):
        def sent(i=i):
            for u in range(2):
                for copy in head_copies(i, u):
                    copy.wait_send()
                back(u, i).wait_send()
            lam_copy(i).wait_send()
        pl.when(away[i])(sent)


def layer(length, mix_lambda, sink_logit, inputs, gain, weights):
    bf, f32 = jnp.bfloat16, jnp.float32
    depth = weights[3].shape[0]
    width = weights[6].shape[1]
    dma = pltpu.SemaphoreType.DMA
    vmem = pltpu.VMEM
    return pl.pallas_call(
        layer_kernel,
        out_shape=jax.ShapeDtypeStruct((2 * SHARE, width), bf),
        in_specs=[SMEM_SPEC] * 3 + [VMEM_SPEC] * 2 + [HBM_SPEC] * 8,
        out_specs=VMEM_SPEC,
        scratch_shapes=[
            vmem((GROUPS, 2, GROUPS, SHARE, ROWS), bf),
            vmem((320, depth), bf),
            vmem((depth, 128), bf),
            vmem((depth, 128), bf),
            vmem((depth, 128), bf),
            vmem((GROUP * HEAD, width), bf),
            vmem((128, width), bf),
            vmem((ROWS, ACC_COLS), f32),
            vmem((2, 2, 384, 128), bf),
            vmem((2, 8, 128), f32),
            vmem((2, 8, 128), f32),
            vmem((2, WINDOW, 128), bf),
            vmem((ROWS, 256), bf),
            vmem((ROWS + 2 * WINDOW, 128), bf),
            vmem((HEAD, ROWS + 2 * WINDOW), bf),
            vmem((ROWS, GROUP * HEAD), bf),
            vmem((BLOCKS, 2, HALF, 128), bf),
            vmem((2, 2, 128, 128), bf),
            vmem((2, 128, 2 * TILE), bf),
            vmem((80, ROWS), bf),
            vmem((80, 2 * TILE), f32),
            vmem((2, 256, TILE), f32),
            vmem((2, 8, TILE), f32),
            vmem((8, 2 * TILE), f32),
            vmem((2, 256, 128), f32),
            vmem((2, 256, 128), jnp.int32),
            vmem((2, 2, 8, 128), jnp.int32),
            vmem((2, 2, 128, 128), bf),
            vmem((2, 2, 128, 128), bf),
            vmem((HALF, 128), bf),
            vmem((2, 2, 128, GROUP * HEAD), bf),
            vmem((2, 2, 128, 128), bf),
            vmem((2, CHUNKS, 128, CHUNK), bf),
            vmem((2, CHUNKS, 128, CHUNK), bf),
            vmem((2, NX, CHUNKS, SHARE, CHUNK), bf),
            vmem((2, CHUNKS, SHARE, CHUNK), bf),
            vmem((2, CHUNKS, SHARE, CHUNK), bf),
            vmem((2, 2, CHUNKS, SHARE, CHUNK), bf),
            dma((8,)), dma((GROUPS, 4)), dma,
            dma((BLOCKS, 2)), dma((2, 2)), dma((2,)), dma((2,)),
            dma((2, 2, 2)), dma((2,)), dma, dma, dma((2,)), dma((3,)),
            dma((2, 2)), dma((2, 2)), dma, dma((2, CHUNKS)), dma, dma((2, CHUNKS)),
            dma, dma((2, 2, CHUNKS)),
        ],
        compiler_params=pltpu.CompilerParams(
            collective_id=0, has_side_effects=True, vmem_limit_bytes=62 * 1024 * 1024
        ),
        name="layer",
    )(length, mix_lambda, sink_logit, inputs, gain, *weights)


def body(
    inputs, length, win_query, win_key, win_value, sink_logit,
    diff_query, diff_key, diff_value, mix_lambda, head_gain, win_out, diff_out,
):
    weights = (
        win_query.T, win_key.T, win_value.T, diff_query, diff_key, diff_value, win_out, diff_out,
    )
    rows = inputs.reshape(GROUPS, 2, SHARE, inputs.shape[1])
    return layer(length, mix_lambda, sink_logit, rows, head_gain.reshape(1, HEAD), weights)


def solution(mesh):
    placed = (
        P("sp", "tp"), P(), P(None, "tp"), P(None, "tp"), P(None, "tp"), P("tp"), P(None, "tp"),
        P(None, "tp"), P(None, "tp"), P("tp"), P(), P("tp", None), P("tp", None),
    )
    return jax.shard_map(
        body, mesh=mesh, in_specs=placed, out_specs=P(("sp", "tp"), None), check_vma=False
    )
```

```python
import functools

import jax
import jax.numpy as jnp
from jax import lax
from jax.experimental import pallas as pl
from jax.experimental.pallas import tpu as pltpu
from jax.sharding import PartitionSpec as P

HEAD = 64
DQK = 32
GROUP = 3
WINDOW = 128
NX, NY, NZ = 4, 4, 8
ROWS = 512
QUARTER = ROWS // 4
HALF = ROWS // 2
BLOCKS = NY * NZ
Q_SCALE = 1.4426950408889634 * DQK ** (-0.5)
MESH = pl.DeviceIdType.MESH

epsilon = 1e-06
masked_score = -1e30
VMEM_SPEC = pl.BlockSpec(memory_space=pltpu.VMEM)
SMEM_SPEC = pl.BlockSpec(memory_space=pltpu.SMEM)
HBM_SPEC = pl.BlockSpec(memory_space=pltpu.HBM)


def place():
    sp, tp = lax.axis_index("sp"), lax.axis_index("tp")
    return sp // NY, sp % NY, tp // 2, tp % 2


def greet(devices, conditions=None):
    barrier = pltpu.get_barrier_semaphore()
    for i, device in enumerate(devices):
        def signal(device=device):
            pl.semaphore_signal(barrier, inc=1, device_id=device, device_id_type=MESH)
        if conditions is None or conditions[i] is None:
            signal()
        else:
            pl.when(conditions[i])(signal)


WQ, DQ, DK, DV, ACC_COLS = 0, 384, 512, 640, 768
TILE = 2 * ROWS
CHUNK = 1024
CHUNKS = 4
SHARE = 32
GROUPS = 2 * NX


def natural(r, u):
    return (r // SHARE) * 2 * SHARE + u * SHARE + r % SHARE


def layer_kernel(
    length_ref, lam_smem, sink_ref, x_ref, gain_ref, wq_hbm, wk_hbm, wv_hbm, dq_hbm, dk_hbm, dv_hbm, wo_hbm, do_hbm,
    out_ref,
    xg, wt, dq, dk, dv, wo, do, acc, msg, lam_ref, lamo_ref, halo_ref, winq, keys, v_t, win_ref,
    kv_ref, q_ref, qz, va, att, s_buf, t_buf, m_buf, bias, row_at, lane_at,
    o_buf, rows_t, diff_rows, lhs_w, lhs_d, give, take, mine, far_in, joined, fin,
    w_sem, recv_x, send_xs,
    recv_kv, recv_q, recv_lam, recv_halo, send_a, send_lam, send_ring, send_sib, send_halo, local_sem,
    recv_o, send_o, send_g, recv_g, send_f, recv_f, send_n, recv_n,
):
    z, y, x, c = place()
    sp = z * NY + y
    tp = x * 2 + c
    live = length_ref[0]
    right = (sp, ((x + 1) % NX) * 2 + c)
    left = (sp, ((x + NX - 1) % NX) * 2 + c)
    sibling = (sp, x * 2 + 1 - c)
    up = (((z + 1) % NZ) * NY + y, tp)
    down = (((z + NZ - 1) % NZ) * NY + y, tp)
    after = ((sp + 1) % BLOCKS, tp)
    before = ((sp + BLOCKS - 1) % BLOCKS, tp)
    partners = [(z * NY + 2 * c + i, x * 2 + y // 2) for i in range(2)]
    away = [(2 * c + i) != y for i in range(2)]

    loads = [
        pltpu.make_async_copy(src, dst, w_sem.at[i])
        for i, (src, dst) in enumerate(
            (
                (wq_hbm, wt.at[pl.ds(0, 192)]),
                (wk_hbm, wt.at[pl.ds(192, 64)]),
                (wv_hbm, wt.at[pl.ds(256, 64)]),
                (dq_hbm, dq),
                (dk_hbm, dk),
                (dv_hbm, dv),
                (wo_hbm, wo),
                (do_hbm, do),
            )
        )
    ]
    for load in loads:
        load.start()
    for i in range(2):
        lam_ref[i] = jnp.full((8, 128), lam_smem[i], jnp.float32)
    greet(
        (right, left, sibling, up, down, after, before) + tuple(partners), (None,) * 7 + tuple(away)
    )
    pl.semaphore_wait(pltpu.get_barrier_semaphore(), 7 + sum(a.astype(jnp.int32) for a in away))

    def remote(src, dst, send_sem, recv_sem, device):
        return pltpu.make_async_remote_copy(
            src_ref=src, dst_ref=dst, send_sem=send_sem, recv_sem=recv_sem,
            device_id=device, device_id_type=MESH,
        )

    def go(copy):
        copy.start()

    def send_x(own, t, q, device):
        part = pl.ds(q % 2 * 4, 4)
        src = x_ref.at[part, q // 2] if own else xg.at[t, q // 2, part]
        go(remote(src, xg.at[t, q // 2, part], send_xs, recv_x.at[t, q], device))

    def arrive_x(t, q):
        part = xg.at[t, q // 2, pl.ds(q % 2 * 4, 4)]
        remote(part, part, send_xs, recv_x.at[t, q], sibling).wait_recv()

    t_left = ((x + NX - 1) % NX) * 2 + c
    t_right = ((x + 1) % NX) * 2 + c
    t_far = ((x + 2) % NX) * 2 + c

    def other(t):
        return t + 1 - 2 * c

    def multiply(own, t, h):
        rows = pl.ds(h * HALF, HALF)
        block = (x_ref[:, h] if own else xg[t, h]).reshape(HALF, ROWS)
        ks = pl.ds(pl.multiple_of(t * ROWS, ROWS), ROWS)
        acc[rows, WQ:WQ + 320] += lax.dot_general(
            block, wt[:, ks], (((1,), (1,)), ((), ())), preferred_element_type=jnp.float32
        )
        both = jnp.concatenate([dq[ks, :], dk[ks, :]], axis=1)
        acc[rows, DQ:DQ + 256] += jnp.dot(block, both, preferred_element_type=jnp.float32)
        acc[rows, DV:DV + 128] += jnp.dot(block, dv[ks, :], preferred_element_type=jnp.float32)

    def multiply_other(t, h):
        for q in (2 * h, 2 * h + 1):
            arrive_x(other(t), q)
        multiply(False, other(t), h)

    def receive_x(t, q):
        arrive_x(t, q)
        send_x(False, t, q, sibling)

    low = lax.broadcasted_iota(jnp.int32, (QUARTER, 128), 1) < 64
    slot = y % 2

    def head_copies(i, u):
        return [
            remote(msg.at[i, u, pl.ds(0, 256)], kv_ref.at[sp, u], send_a.at[i, u, 0], recv_kv.at[sp, u], partners[i]),
            remote(msg.at[i, u, pl.ds(256, 128)], q_ref.at[slot, u], send_a.at[i, u, 1], recv_q.at[slot, u], partners[i]),
        ]

    def lam_copy(i):
        return remote(lam_ref.at[i], lamo_ref.at[slot], send_lam.at[i], recv_lam.at[slot], partners[i])

    edges = [
        remote(keys.at[pl.ds(WINDOW, WINDOW)], halo_ref.at[1], send_halo.at[1], recv_halo.at[1], before),
        remote(keys.at[pl.ds(ROWS, WINDOW)], halo_ref.at[0], send_halo.at[0], recv_halo.at[0], after),
    ]

    def pack(u):
        first, second = pl.ds(u * HALF, QUARTER), pl.ds(u * HALF + QUARTER, QUARTER)
        k0, k1 = acc[first, DK:DK + 128], acc[second, DK:DK + 128]
        msg[0, u, 0:128] = jnp.where(low, k0, pltpu.roll(k1, 64, 1)).astype(jnp.bfloat16)
        msg[1, u, 0:128] = jnp.where(low, pltpu.roll(k0, 64, 1), k1).astype(jnp.bfloat16)
        for j, part in enumerate((first, second)):
            turned = jnp.where(
                lane_at[j, u, 0:1] < live - sp * ROWS, acc[part, DV:DV + 128].T, 0.0
            ).astype(jnp.bfloat16)
            asked = (acc[part, DQ:DQ + 128].T * Q_SCALE).astype(jnp.bfloat16)
            for head in range(2):
                msg[head, u, 128 + j * 64:128 + (j + 1) * 64] = turned[head * 64:(head + 1) * 64]
                msg[head, u, 256 + j * 64:256 + (j + 1) * 64] = asked[head * 64:(head + 1) * 64]
        for i in range(2):
            def leave(i=i):
                for copy in head_copies(i, u):
                    copy.start()
            pl.when(away[i])(leave)
            def stay(i=i):
                copies = [
                    pltpu.make_async_copy(msg.at[i, u, pl.ds(0, 256)], kv_ref.at[sp, u], local_sem.at[0]),
                    pltpu.make_async_copy(msg.at[i, u, pl.ds(256, 128)], q_ref.at[slot, u], local_sem.at[1]),
                ]
                for copy in copies:
                    copy.start()
                for copy in copies:
                    copy.wait()
            pl.when(jnp.logical_not(away[i]))(stay)
        for j, part in enumerate((first, second)):
            pair = jnp.where(low, acc[part, 256:384], acc[part, 128:256]).astype(jnp.bfloat16)
            asks = acc[part, 0:256].astype(jnp.bfloat16)
            for g in range(4):
                at = (j * 4 + g) * 2 * SHARE + u * SHARE
                keys[WINDOW + at:WINDOW + at + SHARE] = pair[g * SHARE:(g + 1) * SHARE]
                winq[at:at + SHARE] = asks[g * SHARE:(g + 1) * SHARE]

    def block(zz, s, core):
        return ((zz + NZ) % NZ) * NY + 2 * core + s

    def forward(b, u, device, sem):
        go(remote(kv_ref.at[b, u], kv_ref.at[b, u], sem, recv_kv.at[b, u], device))

    def arrive(b, u):
        remote(kv_ref.at[b, u], kv_ref.at[b, u], send_sib, recv_kv.at[b, u], sibling).wait_recv()

    def open_ring(u):
        for s in range(2):
            b = block(z, s, c)
            pl.when(away[s])(lambda: arrive(b, u))
            forward(b, u, up, send_ring)
            forward(b, u, down, send_ring)
            forward(b, u, sibling, send_sib)

    def ring(u, d):
        for s in range(2):
            for way, (reach, device, sign) in enumerate(((4 - s, up, -1), (3 + s, down, 1))):
                if d > reach:
                    continue
                b = block(z + sign * d, s, c)
                arrive(b, u)
                if d < reach:
                    forward(b, u, device, send_ring)
                forward(b, u, sibling, send_sib)

    def turn(i):
        pair = keys[i * 128:(i + 1) * 128].astype(jnp.float32)
        v_t[:, i * 128:(i + 1) * 128] = pair.T[0:HEAD].astype(jnp.bfloat16)

    def band_edges():
        for copy in edges:
            copy.wait_recv()
        keys[0:WINDOW] = halo_ref[0]
        keys[WINDOW + ROWS:] = halo_ref[1]
        turn(0)
        turn(5)

    def band(i):
        q_t = winq[i * 128:(i + 1) * 128].astype(jnp.float32).T * HEAD ** (-0.5)
        zero = jnp.zeros((HEAD, 128), jnp.float32)
        query = jnp.concatenate(
            [jnp.concatenate([zero, q_t[g * HEAD:(g + 1) * HEAD]], axis=0) for g in range(GROUP)], axis=1
        ).astype(jnp.bfloat16)
        s = jnp.dot(keys[i * 128:i * 128 + 384], query, preferred_element_type=jnp.float32)
        key = lax.broadcasted_iota(jnp.int32, (384, 128), 0)
        ask = lax.broadcasted_iota(jnp.int32, (384, 128), 1)
        start = sp * ROWS + (i - 1) * 128
        allowed = (
            (key - ask >= 0) & (key - ask <= 2 * WINDOW) & (start + key >= 0) & (start + key < live)
        )
        for g in range(GROUP):
            own = jnp.where(allowed, s[:, g * 128:(g + 1) * 128], masked_score)
            top = jnp.maximum(jnp.max(own, axis=0, keepdims=True), sink_ref[g])
            e = jnp.where(allowed, jnp.exp(own - top), 0.0)
            total = jnp.sum(e, axis=0, keepdims=True) + jnp.exp(sink_ref[g] - top)
            o = jnp.dot(v_t[:, i * 128:i * 128 + 384], e.astype(jnp.bfloat16), preferred_element_type=jnp.float32)
            ok = (start + 128 + lax.broadcasted_iota(jnp.int32, (HEAD, 128), 1)) < live
            o = jnp.where(ok, o / total, 0.0)
            both = jnp.concatenate([o, jnp.zeros_like(o)], axis=0).T
            win_ref[i * 128:(i + 1) * 128, g * HEAD:(g + 1) * HEAD] = both[:, 0:HEAD].astype(jnp.bfloat16)

    def nth(i):
        at = i + 4
        d, r = at // 8, at % 8
        sign, core = 2 * (r // 4) - 1, r % 4 // 2
        zz = (z + sign * d + NZ) % NZ
        return zz * NY + 2 * (c + core - 2 * c * core) + r % 2, core == 1

    def set_queries():
        for s in range(2):
            for u in range(2):
                for j in range(2):
                    q = q_ref[s, u, j * 64:(j + 1) * 64, :]
                    for h in range(2):
                        for m in range(2):
                            at = u * TILE + m * ROWS + s * HALF + j * 128
                            qz[h, h * 64 + m * 32:h * 64 + (m + 1) * 32, at:at + 128] = q[m * 32:(m + 1) * 32]

    def set_table():
        row = lax.broadcasted_iota(jnp.int32, (128, 128), 0)
        lane = lax.broadcasted_iota(jnp.int32, (8, 128), 1)
        for h in range(2):
            for u in range(2):
                row_at[h, u * 128:(u + 1) * 128] = natural(h * 128 + row, u)
                lane_at[h, u] = natural(h * 128 + lane, u)

    def set_ones(b, g):
        top = lax.broadcasted_iota(jnp.int32, (8, 128), 0) == 0
        zero = jnp.zeros((8, 128), jnp.float32)
        for h in range(2):
            for u in range(2):
                at = h * 256 + u * 128
                ok = lane_at[h, u] < live - b * ROWS
                ones = jnp.concatenate([jnp.where(ok & top, 1.0, zero), zero], axis=0)
                va[g, :, at:at + 128] = ones.astype(jnp.bfloat16)

    def set_bias(b):
        for h in range(2):
            bias[h] = jnp.where(row_at[h] < live - b * ROWS, 0.0, masked_score)

    def score(b, n, h, to):
        k = jnp.concatenate([kv_ref[b, 0, 0:128, :], kv_ref[b, 1, 0:128, :]], axis=0)
        s = jnp.dot(k, qz[h, :, n * TILE:(n + 1) * TILE], preferred_element_type=jnp.float32)
        s = s + jnp.concatenate([bias[h]] * (TILE // 128), axis=1)
        s_buf[to] = s
        t_buf[to] = jnp.max(s.reshape(32, 8, TILE), axis=0)

    def segment(low_i, high_i, ns, fresh):
        group = 2 // len(ns)
        units = [(g, n, h) for g in range(group) for n in ns for h in range(2)]
        start = nth(low_i)[0]
        set_bias(start)
        score(start, *units[0][1:], 0)

        def step(trip, carry):
            i = low_i + trip * group
            blocks = [nth(i)[0]]
            for g in range(1, group + 1):
                following, foreign = nth(jnp.minimum(i + g, high_i - 1))
                blocks.append(following)
                if fresh:
                    def wait(following=following):
                        arrive(following, 0)
                        arrive(following, 1)
                    pl.when(jnp.logical_and(foreign, i + g < high_i))(wait)

            for j, (g, n, h) in enumerate(units):
                b = blocks[g]
                cols = slice(n * TILE, (n + 1) * TILE)
                if j == 0 or units[j - 1][0] != g:
                    set_ones(b, g)
                s = s_buf[j % 2]
                top = t_buf[j % 2]
                g_next, n_next, h_next = units[j + 1] if j + 1 < len(units) else (group,) + units[0][1:]
                if g_next != g:
                    set_bias(blocks[g_next])
                score(blocks[g_next], n_next, h_next, 1 - j % 2)
                old = m_buf[:, cols]
                new = jnp.maximum(old, jnp.broadcast_to(jnp.max(top, axis=0, keepdims=True), (8, TILE)))
                m_buf[:, cols] = new
                e = jnp.exp2(s.reshape(32, 8, TILE) - new[None]).reshape(256, TILE).astype(jnp.bfloat16)
                held = (att[:, cols].reshape(10, 8, TILE) * jnp.exp2(old - new)[None]).reshape(80, TILE)
                value = jnp.concatenate(
                    [
                        jnp.concatenate([kv_ref[b, u, 128 + h * 64:192 + h * 64, :] for u in range(2)], axis=1),
                        va[g, :, h * 256:(h + 1) * 256],
                    ],
                    axis=0,
                )
                att[:, cols] = held + jnp.dot(value, e, preferred_element_type=jnp.float32)
            return carry

        lax.fori_loop(0, (high_i - low_i) // group, step, 0)

    def back(n, i):
        return remote(o_buf.at[n, i], rows_t.at[n, slot], send_o.at[n, i], recv_o.at[n, slot], partners[i])

    def finish(n):
        row = gain_ref[...]
        gain = jnp.broadcast_to(jnp.concatenate([row, row], axis=1), (128, 128)).T[0:HEAD]
        lam = lamo_ref[0, 0:1, :]
        for s in range(2):
            for j in range(2):
                maps = []
                for m in range(2):
                    at = n * TILE + m * ROWS + s * HALF + j * 128
                    total = att[64:65, at:at + 128]
                    maps.append(att[0:64, at:at + 128] / jnp.where(total > 0.0, total, 1.0))
                mixed = maps[0] - lam * maps[1]
                normed = mixed * lax.rsqrt(jnp.mean(mixed * mixed, axis=0, keepdims=True) + epsilon) * gain
                ok = (z * NY + 2 * c + s) * ROWS + lane_at[j, n, 0:1] < live
                o_buf[n, s, j * 64:(j + 1) * 64, :] = jnp.where(ok, normed, 0.0).astype(jnp.bfloat16)
        for i in range(2):
            pl.when(away[i])(lambda i=i: back(n, i).start())
            def stay(i=i):
                copy = pltpu.make_async_copy(o_buf.at[n, i], rows_t.at[n, slot], local_sem.at[0])
                copy.start()
                copy.wait()
            pl.when(jnp.logical_not(away[i]))(stay)

    order = (0, 2, 1, 3)

    def owner(side, r):
        return ((x + r) % NX) * 2 + (c if side else 1 - c)

    def partial(n, side, k):
        cols = slice(k * CHUNK, (k + 1) * CHUNK)
        return jnp.dot(lhs_w[n, side], wo[:, cols], preferred_element_type=jnp.float32) + jnp.dot(
            lhs_d[n, side], do[:, cols], preferred_element_type=jnp.float32
        )

    def given(n, k):
        return remote(give.at[n, k], take.at[n, k], send_g, recv_g.at[n, k], sibling)

    def far(n, k):
        return remote(mine.at[n, 2, k], far_in.at[n, k], send_f, recv_f.at[n, k], right if k < 2 else left)

    def near(n, src, k, way):
        return remote(src, fin.at[n, way, k], send_n, recv_n.at[n, way, k], left if way else right)

    def merge_give(n):
        for i in range(2):
            def wait(i=i):
                remote(o_buf.at[n, i], rows_t.at[n, i], send_o.at[n, i], recv_o.at[n, i], partners[i]).wait_recv()
            pl.when(away[i])(wait)
        for j in range(2):
            pair = jnp.concatenate(
                [rows_t[n, 0, j * 64:(j + 1) * 64], rows_t[n, 1, j * 64:(j + 1) * 64]], axis=0
            ).astype(jnp.float32)
            diff_rows[j * 128:(j + 1) * 128] = pair.T.astype(jnp.bfloat16)
        for side in range(2):
            for r in range(NX):
                t = owner(side, r)
                to = slice(r * SHARE, (r + 1) * SHARE)
                lhs_w[n, side, to] = win_ref[pl.ds(pl.multiple_of(t * 2 * SHARE + n * SHARE, SHARE), SHARE)]
                lhs_d[n, side, to] = diff_rows[pl.ds(pl.multiple_of(t * SHARE, SHARE), SHARE)]
        for k in order:
            give[n, k] = partial(n, 0, k).astype(jnp.bfloat16)
            go(given(n, k))

    def merge_send(n):
        for k in order:
            own = partial(n, 1, k)
            given(n, k).wait_recv()
            both = (own + take[n, k].astype(jnp.float32)).astype(jnp.bfloat16)
            for r in range(NX):
                mine[n, r, k] = both[r * SHARE:(r + 1) * SHARE]
            go(far(n, k))
        for i in range(2):
            go(near(n, mine.at[n, 1, 2 + i], 2 + i, 0))
            go(near(n, mine.at[n, 3, i], i, 1))

    def merge_join(n):
        for k in order:
            way = 0 if k < 2 else 1
            far(n, k).wait_recv()
            joined[n, k] = (
                mine[n, 3 if way else 1, k].astype(jnp.float32) + far_in[n, k].astype(jnp.float32)
            ).astype(jnp.bfloat16)
            go(near(n, joined.at[n, k], k, way))

    def merge_out(n):
        for k in order:
            near(n, joined.at[n, k], k, 0).wait_recv()
            near(n, joined.at[n, k], k, 1).wait_recv()
            value = (
                mine[n, 0, k].astype(jnp.float32)
                + fin[n, 0, k].astype(jnp.float32)
                + fin[n, 1, k].astype(jnp.float32)
            )
            out_ref[n * SHARE:(n + 1) * SHARE, k * CHUNK:(k + 1) * CHUNK] = value.astype(jnp.bfloat16)

    for q in range(2):
        send_x(True, tp, q, right)
        send_x(True, tp, 1 - q, left)
    for q in range(4):
        send_x(True, tp, q, sibling)
    acc[...] = jnp.zeros_like(acc)
    set_table()
    for i in range(2):
        pl.when(away[i])(lambda i=i: lam_copy(i).start())
        def keep(i=i):
            copy = pltpu.make_async_copy(lam_ref.at[i], lamo_ref.at[slot], local_sem.at[2])
            copy.start()
            copy.wait()
        pl.when(jnp.logical_not(away[i]))(keep)
    for load in loads:
        load.wait()
    multiply(True, tp, 0)
    receive_x(t_left, 0)
    send_x(False, t_left, 0, right)
    for q in (2, 3):
        send_x(True, tp, q, right)
    receive_x(t_right, 1)
    send_x(False, t_right, 1, left)
    for q in (3, 2):
        send_x(True, tp, q, left)
    multiply(True, tp, 1)
    receive_x(t_left, 1)
    receive_x(t_right, 0)
    multiply_other(tp, 0)
    multiply_other(tp, 1)
    multiply(False, t_left, 0)
    multiply(False, t_right, 0)
    multiply_other(t_left, 0)
    multiply_other(t_right, 0)
    receive_x(t_far, 0)
    receive_x(t_far, 1)
    multiply(False, t_far, 0)
    multiply_other(t_far, 0)
    pack(0)
    receive_x(t_left, 2)
    send_x(False, t_left, 2, right)
    receive_x(t_right, 3)
    send_x(False, t_right, 3, left)
    receive_x(t_right, 2)
    receive_x(t_left, 3)
    open_ring(0)
    multiply(False, t_left, 1)
    multiply(False, t_right, 1)
    multiply_other(t_left, 1)
    multiply_other(t_right, 1)
    receive_x(t_far, 2)
    receive_x(t_far, 3)
    multiply(False, t_far, 1)
    ring(0, 1)
    multiply_other(t_far, 1)
    pack(1)
    for copy in edges:
        copy.start()
    att[...] = jnp.zeros_like(att)
    qz[...] = jnp.zeros_like(qz)
    m_buf[...] = jnp.full_like(m_buf, masked_score)
    for i in range(1, 5):
        turn(i)
    band(1)
    band(2)
    open_ring(1)
    for i in range(2):
        def rest(i=i):
            for u in range(2):
                remote(
                    msg.at[0, u, pl.ds(256, 128)], q_ref.at[i, u], send_a.at[0, u, 1], recv_q.at[i, u], sibling
                ).wait_recv()
            remote(lam_ref.at[0], lamo_ref.at[i], send_lam.at[0], recv_lam.at[i], sibling).wait_recv()
        pl.when(away[i])(rest)
    set_queries()
    ring(0, 2)
    segment(0, 4, (0, 1), True)
    ring(0, 3)
    ring(1, 1)
    segment(4, 12, (0, 1), True)
    ring(1, 2)
    ring(0, 4)
    segment(12, 20, (0,), True)
    ring(1, 3)
    segment(20, 28, (0,), True)
    ring(1, 4)
    band_edges()
    band(0)
    band(3)
    segment(28, 32, (0,), True)
    finish(0)
    segment(12, 18, (1,), False)
    merge_give(0)
    segment(18, 20, (1,), False)
    merge_send(0)
    segment(20, 26, (1,), False)
    merge_join(0)
    segment(26, 32, (1,), False)
    finish(1)
    merge_out(0)
    merge_give(1)
    merge_send(1)
    merge_join(1)
    merge_out(1)
    for ref, sem in (
        (xg.at[pl.ds(0, 7)], send_xs),
        (kv_ref.at[pl.ds(0, 14)], send_ring),
        (kv_ref.at[pl.ds(0, 16)], send_sib),
        (give, send_g),
        (joined, send_f),
        (fin, send_n),
    ):
        remote(ref, ref, sem, recv_x.at[0, 0], sibling).wait_send()
    for copy in edges:
        copy.wait_send()
    for i in range(2):
        def sent(i=i):
            for u in range(2):
                for copy in head_copies(i, u):
                    copy.wait_send()
                back(u, i).wait_send()
            lam_copy(i).wait_send()
        pl.when(away[i])(sent)


def layer(length, mix_lambda, sink_logit, inputs, gain, weights):
    bf, f32 = jnp.bfloat16, jnp.float32
    depth = weights[3].shape[0]
    width = weights[6].shape[1]
    dma = pltpu.SemaphoreType.DMA
    vmem = pltpu.VMEM
    return pl.pallas_call(
        layer_kernel,
        out_shape=jax.ShapeDtypeStruct((2 * SHARE, width), bf),
        in_specs=[SMEM_SPEC] * 3 + [VMEM_SPEC] * 2 + [HBM_SPEC] * 8,
        out_specs=VMEM_SPEC,
        scratch_shapes=[
            vmem((GROUPS, 2, GROUPS, SHARE, ROWS), bf),
            vmem((320, depth), bf),
            vmem((depth, 128), bf),
            vmem((depth, 128), bf),
            vmem((depth, 128), bf),
            vmem((GROUP * HEAD, width), bf),
            vmem((128, width), bf),
            vmem((ROWS, ACC_COLS), f32),
            vmem((2, 2, 384, 128), bf),
            vmem((2, 8, 128), f32),
            vmem((2, 8, 128), f32),
            vmem((2, WINDOW, 128), bf),
            vmem((ROWS, 256), bf),
            vmem((ROWS + 2 * WINDOW, 128), bf),
            vmem((HEAD, ROWS + 2 * WINDOW), bf),
            vmem((ROWS, GROUP * HEAD), bf),
            vmem((BLOCKS, 2, HALF, 128), bf),
            vmem((2, 2, 128, 128), bf),
            vmem((2, 128, 2 * TILE), bf),
            vmem((2, 16, ROWS), bf),
            vmem((80, 2 * TILE), f32),
            vmem((2, 256, TILE), f32),
            vmem((2, 8, TILE), f32),
            vmem((8, 2 * TILE), f32),
            vmem((2, 256, 128), f32),
            vmem((2, 256, 128), jnp.int32),
            vmem((2, 2, 8, 128), jnp.int32),
            vmem((2, 2, 128, 128), bf),
            vmem((2, 2, 128, 128), bf),
            vmem((HALF, 128), bf),
            vmem((2, 2, 128, GROUP * HEAD), bf),
            vmem((2, 2, 128, 128), bf),
            vmem((2, CHUNKS, 128, CHUNK), bf),
            vmem((2, CHUNKS, 128, CHUNK), bf),
            vmem((2, NX, CHUNKS, SHARE, CHUNK), bf),
            vmem((2, CHUNKS, SHARE, CHUNK), bf),
            vmem((2, CHUNKS, SHARE, CHUNK), bf),
            vmem((2, 2, CHUNKS, SHARE, CHUNK), bf),
            dma((8,)), dma((GROUPS, 4)), dma,
            dma((BLOCKS, 2)), dma((2, 2)), dma((2,)), dma((2,)),
            dma((2, 2, 2)), dma((2,)), dma, dma, dma((2,)), dma((3,)),
            dma((2, 2)), dma((2, 2)), dma, dma((2, CHUNKS)), dma, dma((2, CHUNKS)),
            dma, dma((2, 2, CHUNKS)),
        ],
        compiler_params=pltpu.CompilerParams(
            collective_id=0, has_side_effects=True, vmem_limit_bytes=62 * 1024 * 1024
        ),
        name="layer",
    )(length, mix_lambda, sink_logit, inputs, gain, *weights)


def body(
    inputs, length, win_query, win_key, win_value, sink_logit,
    diff_query, diff_key, diff_value, mix_lambda, head_gain, win_out, diff_out,
):
    weights = (
        win_query.T, win_key.T, win_value.T, diff_query, diff_key, diff_value, win_out, diff_out,
    )
    rows = inputs.reshape(GROUPS, 2, SHARE, inputs.shape[1])
    return layer(length, mix_lambda, sink_logit, rows, head_gain.reshape(1, HEAD), weights)


def solution(mesh):
    placed = (
        P("sp", "tp"), P(), P(None, "tp"), P(None, "tp"), P(None, "tp"), P("tp"), P(None, "tp"),
        P(None, "tp"), P(None, "tp"), P("tp"), P(), P("tp", None), P("tp", None),
    )
    return jax.shard_map(
        body, mesh=mesh, in_specs=placed, out_specs=P(("sp", "tp"), None), check_vma=False
    )
```

```python
import functools

import jax
import jax.numpy as jnp
from jax import lax
from jax.experimental import pallas as pl
from jax.experimental.pallas import tpu as pltpu
from jax.sharding import PartitionSpec as P

HEAD = 64
DQK = 32
GROUP = 3
WINDOW = 128
NX, NY, NZ = 4, 4, 8
ROWS = 512
QUARTER = ROWS // 4
HALF = ROWS // 2
BLOCKS = NY * NZ
Q_SCALE = 1.4426950408889634 * DQK ** (-0.5)
MESH = pl.DeviceIdType.MESH

epsilon = 1e-06
masked_score = -1e30
VMEM_SPEC = pl.BlockSpec(memory_space=pltpu.VMEM)
SMEM_SPEC = pl.BlockSpec(memory_space=pltpu.SMEM)
HBM_SPEC = pl.BlockSpec(memory_space=pltpu.HBM)


def place():
    sp, tp = lax.axis_index("sp"), lax.axis_index("tp")
    return sp // NY, sp % NY, tp // 2, tp % 2


def greet(devices, conditions=None):
    barrier = pltpu.get_barrier_semaphore()
    for i, device in enumerate(devices):
        def signal(device=device):
            pl.semaphore_signal(barrier, inc=1, device_id=device, device_id_type=MESH)
        if conditions is None or conditions[i] is None:
            signal()
        else:
            pl.when(conditions[i])(signal)


WQ, DQ, DK, DV, ACC_COLS = 0, 384, 512, 640, 768
TILE = 2 * ROWS
CHUNK = 1024
CHUNKS = 4
SHARE = 32
GROUPS = 2 * NX


def natural(r, u):
    return (r // SHARE) * 2 * SHARE + u * SHARE + r % SHARE


def layer_kernel(
    length_ref, lam_smem, sink_ref, x_ref, gain_ref, wq_hbm, wk_hbm, wv_hbm, dq_hbm, dk_hbm, dv_hbm, wo_hbm, do_hbm,
    out_ref,
    xg, wt, dq, dk, dv, wo, do, acc, msg, lam_ref, lamo_ref, halo_ref, winq, keys, v_t, win_ref,
    kv_ref, q_ref, qz, va, att, s_buf, t_buf, m_buf, bias, row_at, lane_at,
    o_buf, rows_t, diff_rows, lhs_w, lhs_d, give, take, mine, far_in, joined, fin,
    w_sem, recv_x, send_xs,
    recv_kv, recv_q, recv_lam, recv_halo, send_a, send_lam, send_ring, send_sib, send_halo, local_sem,
    recv_o, send_o, send_g, recv_g, send_f, recv_f, send_n, recv_n,
):
    z, y, x, c = place()
    sp = z * NY + y
    tp = x * 2 + c
    live = length_ref[0]
    right = (sp, ((x + 1) % NX) * 2 + c)
    left = (sp, ((x + NX - 1) % NX) * 2 + c)
    sibling = (sp, x * 2 + 1 - c)
    up = (((z + 1) % NZ) * NY + y, tp)
    down = (((z + NZ - 1) % NZ) * NY + y, tp)
    after = ((sp + 1) % BLOCKS, tp)
    before = ((sp + BLOCKS - 1) % BLOCKS, tp)
    partners = [(z * NY + 2 * c + i, x * 2 + y // 2) for i in range(2)]
    away = [(2 * c + i) != y for i in range(2)]

    loads = [
        pltpu.make_async_copy(src, dst, w_sem.at[i])
        for i, (src, dst) in enumerate(
            (
                (wq_hbm, wt.at[pl.ds(0, 192)]),
                (wk_hbm, wt.at[pl.ds(192, 64)]),
                (wv_hbm, wt.at[pl.ds(256, 64)]),
                (dq_hbm, dq),
                (dk_hbm, dk),
                (dv_hbm, dv),
                (wo_hbm, wo),
                (do_hbm, do),
            )
        )
    ]
    for load in loads:
        load.start()
    for i in range(2):
        lam_ref[i] = jnp.full((8, 128), lam_smem[i], jnp.float32)
    greet(
        (right, left, sibling, up, down, after, before) + tuple(partners), (None,) * 7 + tuple(away)
    )
    pl.semaphore_wait(pltpu.get_barrier_semaphore(), 7 + sum(a.astype(jnp.int32) for a in away))

    def remote(src, dst, send_sem, recv_sem, device):
        return pltpu.make_async_remote_copy(
            src_ref=src, dst_ref=dst, send_sem=send_sem, recv_sem=recv_sem,
            device_id=device, device_id_type=MESH,
        )

    def go(copy):
        copy.start()

    def send_x(own, t, q, device):
        part = pl.ds(q % 2 * 4, 4)
        src = x_ref.at[part, q // 2] if own else xg.at[t, q // 2, part]
        go(remote(src, xg.at[t, q // 2, part], send_xs, recv_x.at[t, q], device))

    def arrive_x(t, q):
        part = xg.at[t, q // 2, pl.ds(q % 2 * 4, 4)]
        remote(part, part, send_xs, recv_x.at[t, q], sibling).wait_recv()

    t_left = ((x + NX - 1) % NX) * 2 + c
    t_right = ((x + 1) % NX) * 2 + c
    t_far = ((x + 2) % NX) * 2 + c

    def other(t):
        return t + 1 - 2 * c

    def multiply(own, t, h):
        rows = pl.ds(h * HALF, HALF)
        block = (x_ref[:, h] if own else xg[t, h]).reshape(HALF, ROWS)
        ks = pl.ds(pl.multiple_of(t * ROWS, ROWS), ROWS)
        acc[rows, WQ:WQ + 320] += lax.dot_general(
            block, wt[:, ks], (((1,), (1,)), ((), ())), preferred_element_type=jnp.float32
        )
        both = jnp.concatenate([dq[ks, :], dk[ks, :]], axis=1)
        acc[rows, DQ:DQ + 256] += jnp.dot(block, both, preferred_element_type=jnp.float32)
        acc[rows, DV:DV + 128] += jnp.dot(block, dv[ks, :], preferred_element_type=jnp.float32)

    def multiply_other(t, h):
        for q in (2 * h, 2 * h + 1):
            arrive_x(other(t), q)
        multiply(False, other(t), h)

    def receive_x(t, q):
        arrive_x(t, q)
        send_x(False, t, q, sibling)

    low = lax.broadcasted_iota(jnp.int32, (QUARTER, 128), 1) < 64
    slot = y % 2

    def head_copies(i, u):
        return [
            remote(msg.at[i, u, pl.ds(0, 256)], kv_ref.at[sp, u], send_a.at[i, u, 0], recv_kv.at[sp, u], partners[i]),
            remote(msg.at[i, u, pl.ds(256, 128)], q_ref.at[slot, u], send_a.at[i, u, 1], recv_q.at[slot, u], partners[i]),
        ]

    def lam_copy(i):
        return remote(lam_ref.at[i], lamo_ref.at[slot], send_lam.at[i], recv_lam.at[slot], partners[i])

    edges = [
        remote(keys.at[pl.ds(WINDOW, WINDOW)], halo_ref.at[1], send_halo.at[1], recv_halo.at[1], before),
        remote(keys.at[pl.ds(ROWS, WINDOW)], halo_ref.at[0], send_halo.at[0], recv_halo.at[0], after),
    ]

    def pack(u):
        first, second = pl.ds(u * HALF, QUARTER), pl.ds(u * HALF + QUARTER, QUARTER)
        k0, k1 = acc[first, DK:DK + 128], acc[second, DK:DK + 128]
        msg[0, u, 0:128] = jnp.where(low, k0, pltpu.roll(k1, 64, 1)).astype(jnp.bfloat16)
        msg[1, u, 0:128] = jnp.where(low, pltpu.roll(k0, 64, 1), k1).astype(jnp.bfloat16)
        for j, part in enumerate((first, second)):
            turned = jnp.where(
                lane_at[j, u, 0:1] < live - sp * ROWS, acc[part, DV:DV + 128].T, 0.0
            ).astype(jnp.bfloat16)
            asked = (acc[part, DQ:DQ + 128].T * Q_SCALE).astype(jnp.bfloat16)
            for head in range(2):
                msg[head, u, 128 + j * 64:128 + (j + 1) * 64] = turned[head * 64:(head + 1) * 64]
                msg[head, u, 256 + j * 64:256 + (j + 1) * 64] = asked[head * 64:(head + 1) * 64]
        for i in range(2):
            def leave(i=i):
                for copy in head_copies(i, u):
                    copy.start()
            pl.when(away[i])(leave)
            def stay(i=i):
                copies = [
                    pltpu.make_async_copy(msg.at[i, u, pl.ds(0, 256)], kv_ref.at[sp, u], local_sem.at[0]),
                    pltpu.make_async_copy(msg.at[i, u, pl.ds(256, 128)], q_ref.at[slot, u], local_sem.at[1]),
                ]
                for copy in copies:
                    copy.start()
                for copy in copies:
                    copy.wait()
            pl.when(jnp.logical_not(away[i]))(stay)
        for j, part in enumerate((first, second)):
            pair = jnp.where(low, acc[part, 256:384], acc[part, 128:256]).astype(jnp.bfloat16)
            asks = acc[part, 0:256].astype(jnp.bfloat16)
            for g in range(4):
                at = (j * 4 + g) * 2 * SHARE + u * SHARE
                keys[WINDOW + at:WINDOW + at + SHARE] = pair[g * SHARE:(g + 1) * SHARE]
                winq[at:at + SHARE] = asks[g * SHARE:(g + 1) * SHARE]

    def block(zz, s, core):
        return ((zz + NZ) % NZ) * NY + 2 * core + s

    def forward(b, u, device, sem):
        go(remote(kv_ref.at[b, u], kv_ref.at[b, u], sem, recv_kv.at[b, u], device))

    def arrive(b, u):
        remote(kv_ref.at[b, u], kv_ref.at[b, u], send_sib, recv_kv.at[b, u], sibling).wait_recv()

    def open_ring(u):
        for s in range(2):
            b = block(z, s, c)
            pl.when(away[s])(lambda: arrive(b, u))
            forward(b, u, up, send_ring)
            forward(b, u, down, send_ring)
            forward(b, u, sibling, send_sib)

    def ring(u, d):
        for s in range(2):
            for way, (reach, device, sign) in enumerate(((4 - s, up, -1), (3 + s, down, 1))):
                if d > reach:
                    continue
                b = block(z + sign * d, s, c)
                arrive(b, u)
                if d < reach:
                    forward(b, u, device, send_ring)
                forward(b, u, sibling, send_sib)

    def turn(i):
        pair = keys[i * 128:(i + 1) * 128].astype(jnp.float32)
        v_t[:, i * 128:(i + 1) * 128] = pair.T[0:HEAD].astype(jnp.bfloat16)

    def band_edges():
        for copy in edges:
            copy.wait_recv()
        keys[0:WINDOW] = halo_ref[0]
        keys[WINDOW + ROWS:] = halo_ref[1]
        turn(0)
        turn(5)

    def band(i):
        q_t = winq[i * 128:(i + 1) * 128].astype(jnp.float32).T * HEAD ** (-0.5)
        zero = jnp.zeros((HEAD, 128), jnp.float32)
        query = jnp.concatenate(
            [jnp.concatenate([zero, q_t[g * HEAD:(g + 1) * HEAD]], axis=0) for g in range(GROUP)], axis=1
        ).astype(jnp.bfloat16)
        s = jnp.dot(keys[i * 128:i * 128 + 384], query, preferred_element_type=jnp.float32)
        key = lax.broadcasted_iota(jnp.int32, (384, 128), 0)
        ask = lax.broadcasted_iota(jnp.int32, (384, 128), 1)
        start = sp * ROWS + (i - 1) * 128
        allowed = (
            (key - ask >= 0) & (key - ask <= 2 * WINDOW) & (start + key >= 0) & (start + key < live)
        )
        for g in range(GROUP):
            own = jnp.where(allowed, s[:, g * 128:(g + 1) * 128], masked_score)
            top = jnp.maximum(jnp.max(own, axis=0, keepdims=True), sink_ref[g])
            e = jnp.where(allowed, jnp.exp(own - top), 0.0)
            total = jnp.sum(e, axis=0, keepdims=True) + jnp.exp(sink_ref[g] - top)
            o = jnp.dot(v_t[:, i * 128:i * 128 + 384], e.astype(jnp.bfloat16), preferred_element_type=jnp.float32)
            ok = (start + 128 + lax.broadcasted_iota(jnp.int32, (HEAD, 128), 1)) < live
            o = jnp.where(ok, o / total, 0.0)
            both = jnp.concatenate([o, jnp.zeros_like(o)], axis=0).T
            win_ref[i * 128:(i + 1) * 128, g * HEAD:(g + 1) * HEAD] = both[:, 0:HEAD].astype(jnp.bfloat16)

    def nth(i):
        at = i + 4
        d, r = at // 8, at % 8
        sign, core = 2 * (r // 4) - 1, r % 4 // 2
        zz = (z + sign * d + NZ) % NZ
        return zz * NY + 2 * (c + core - 2 * c * core) + r % 2, core == 1

    def set_queries():
        for s in range(2):
            for u in range(2):
                for j in range(2):
                    q = q_ref[s, u, j * 64:(j + 1) * 64, :]
                    for h in range(2):
                        for m in range(2):
                            at = u * TILE + m * ROWS + s * HALF + j * 128
                            qz[h, h * 64 + m * 32:h * 64 + (m + 1) * 32, at:at + 128] = q[m * 32:(m + 1) * 32]

    def set_table():
        row = lax.broadcasted_iota(jnp.int32, (128, 128), 0)
        lane = lax.broadcasted_iota(jnp.int32, (8, 128), 1)
        for h in range(2):
            for u in range(2):
                row_at[h, u * 128:(u + 1) * 128] = natural(h * 128 + row, u)
                lane_at[h, u] = natural(h * 128 + lane, u)

    def set_ones(b, g):
        top = lax.broadcasted_iota(jnp.int32, (8, 128), 0) == 0
        zero = jnp.zeros((8, 128), jnp.float32)
        for h in range(2):
            for u in range(2):
                at = h * 256 + u * 128
                ok = lane_at[h, u] < live - b * ROWS
                ones = jnp.concatenate([jnp.where(ok & top, 1.0, zero), zero], axis=0)
                va[g, :, at:at + 128] = ones.astype(jnp.bfloat16)

    def set_bias(b):
        for h in range(2):
            bias[h] = jnp.where(row_at[h] < live - b * ROWS, 0.0, masked_score)

    def score(b, n, h, to):
        k = jnp.concatenate([kv_ref[b, 0, 0:128, :], kv_ref[b, 1, 0:128, :]], axis=0)
        s = jnp.dot(k, qz[h, :, n * TILE:(n + 1) * TILE], preferred_element_type=jnp.float32)
        s = s + jnp.concatenate([bias[h]] * (TILE // 128), axis=1)
        s_buf[to] = s
        t_buf[to] = jnp.max(s.reshape(32, 8, TILE), axis=0)

    def segment(low_i, high_i, ns, fresh):
        group = 2
        units = [(g, n, h) for g in range(group) for n in ns for h in range(2)]
        start = nth(low_i)[0]
        set_bias(start)
        score(start, *units[0][1:], 0)

        def step(trip, carry):
            i = low_i + trip * group
            blocks = [nth(i)[0]]
            for g in range(1, group + 1):
                following, foreign = nth(jnp.minimum(i + g, high_i - 1))
                blocks.append(following)
                if fresh:
                    def wait(following=following):
                        arrive(following, 0)
                        arrive(following, 1)
                    pl.when(jnp.logical_and(foreign, i + g < high_i))(wait)

            for j, (g, n, h) in enumerate(units):
                b = blocks[g]
                cols = slice(n * TILE, (n + 1) * TILE)
                if j == 0 or units[j - 1][0] != g:
                    set_ones(b, g)
                s = s_buf[j % 2]
                top = t_buf[j % 2]
                g_next, n_next, h_next = units[j + 1] if j + 1 < len(units) else (group,) + units[0][1:]
                if g_next != g:
                    set_bias(blocks[g_next])
                score(blocks[g_next], n_next, h_next, 1 - j % 2)
                old = m_buf[:, cols]
                new = jnp.maximum(old, jnp.broadcast_to(jnp.max(top, axis=0, keepdims=True), (8, TILE)))
                m_buf[:, cols] = new
                e = jnp.exp2(s.reshape(32, 8, TILE) - new[None]).reshape(256, TILE).astype(jnp.bfloat16)
                held = (att[:, cols].reshape(10, 8, TILE) * jnp.exp2(old - new)[None]).reshape(80, TILE)
                value = jnp.concatenate(
                    [
                        jnp.concatenate([kv_ref[b, u, 128 + h * 64:192 + h * 64, :] for u in range(2)], axis=1),
                        va[g, :, h * 256:(h + 1) * 256],
                    ],
                    axis=0,
                )
                att[:, cols] = held + jnp.dot(value, e, preferred_element_type=jnp.float32)
            return carry

        lax.fori_loop(0, (high_i - low_i) // group, step, 0)

    def back(n, i):
        return remote(o_buf.at[n, i], rows_t.at[n, slot], send_o.at[n, i], recv_o.at[n, slot], partners[i])

    def finish(n):
        row = gain_ref[...]
        gain = jnp.broadcast_to(jnp.concatenate([row, row], axis=1), (128, 128)).T[0:HEAD]
        lam = lamo_ref[0, 0:1, :]
        for s in range(2):
            for j in range(2):
                maps = []
                for m in range(2):
                    at = n * TILE + m * ROWS + s * HALF + j * 128
                    total = att[64:65, at:at + 128]
                    maps.append(att[0:64, at:at + 128] / jnp.where(total > 0.0, total, 1.0))
                mixed = maps[0] - lam * maps[1]
                normed = mixed * lax.rsqrt(jnp.mean(mixed * mixed, axis=0, keepdims=True) + epsilon) * gain
                ok = (z * NY + 2 * c + s) * ROWS + lane_at[j, n, 0:1] < live
                o_buf[n, s, j * 64:(j + 1) * 64, :] = jnp.where(ok, normed, 0.0).astype(jnp.bfloat16)
        for i in range(2):
            pl.when(away[i])(lambda i=i: back(n, i).start())
            def stay(i=i):
                copy = pltpu.make_async_copy(o_buf.at[n, i], rows_t.at[n, slot], local_sem.at[0])
                copy.start()
                copy.wait()
            pl.when(jnp.logical_not(away[i]))(stay)

    order = (0, 2, 1, 3)

    def owner(side, r):
        return ((x + r) % NX) * 2 + (c if side else 1 - c)

    def partial(n, side, k):
        cols = slice(k * CHUNK, (k + 1) * CHUNK)
        return jnp.dot(lhs_w[n, side], wo[:, cols], preferred_element_type=jnp.float32) + jnp.dot(
            lhs_d[n, side], do[:, cols], preferred_element_type=jnp.float32
        )

    def given(n, k):
        return remote(give.at[n, k], take.at[n, k], send_g, recv_g.at[n, k], sibling)

    def far(n, k):
        return remote(mine.at[n, 2, k], far_in.at[n, k], send_f, recv_f.at[n, k], right if k < 2 else left)

    def near(n, src, k, way):
        return remote(src, fin.at[n, way, k], send_n, recv_n.at[n, way, k], left if way else right)

    def merge_give(n):
        for i in range(2):
            def wait(i=i):
                remote(o_buf.at[n, i], rows_t.at[n, i], send_o.at[n, i], recv_o.at[n, i], partners[i]).wait_recv()
            pl.when(away[i])(wait)
        for j in range(2):
            pair = jnp.concatenate(
                [rows_t[n, 0, j * 64:(j + 1) * 64], rows_t[n, 1, j * 64:(j + 1) * 64]], axis=0
            ).astype(jnp.float32)
            diff_rows[j * 128:(j + 1) * 128] = pair.T.astype(jnp.bfloat16)
        for side in range(2):
            for r in range(NX):
                t = owner(side, r)
                to = slice(r * SHARE, (r + 1) * SHARE)
                lhs_w[n, side, to] = win_ref[pl.ds(pl.multiple_of(t * 2 * SHARE + n * SHARE, SHARE), SHARE)]
                lhs_d[n, side, to] = diff_rows[pl.ds(pl.multiple_of(t * SHARE, SHARE), SHARE)]
        for k in order:
            give[n, k] = partial(n, 0, k).astype(jnp.bfloat16)
            go(given(n, k))

    def merge_send(n):
        for k in order:
            own = partial(n, 1, k)
            given(n, k).wait_recv()
            both = (own + take[n, k].astype(jnp.float32)).astype(jnp.bfloat16)
            for r in range(NX):
                mine[n, r, k] = both[r * SHARE:(r + 1) * SHARE]
            go(far(n, k))
        for i in range(2):
            go(near(n, mine.at[n, 1, 2 + i], 2 + i, 0))
            go(near(n, mine.at[n, 3, i], i, 1))

    def merge_join(n):
        for k in order:
            way = 0 if k < 2 else 1
            far(n, k).wait_recv()
            joined[n, k] = (
                mine[n, 3 if way else 1, k].astype(jnp.float32) + far_in[n, k].astype(jnp.float32)
            ).astype(jnp.bfloat16)
            go(near(n, joined.at[n, k], k, way))

    def merge_out(n):
        for k in order:
            near(n, joined.at[n, k], k, 0).wait_recv()
            near(n, joined.at[n, k], k, 1).wait_recv()
            value = (
                mine[n, 0, k].astype(jnp.float32)
                + fin[n, 0, k].astype(jnp.float32)
                + fin[n, 1, k].astype(jnp.float32)
            )
            out_ref[n * SHARE:(n + 1) * SHARE, k * CHUNK:(k + 1) * CHUNK] = value.astype(jnp.bfloat16)

    for q in range(2):
        send_x(True, tp, q, right)
        send_x(True, tp, 1 - q, left)
    for q in range(4):
        send_x(True, tp, q, sibling)
    acc[...] = jnp.zeros_like(acc)
    set_table()
    for i in range(2):
        pl.when(away[i])(lambda i=i: lam_copy(i).start())
        def keep(i=i):
            copy = pltpu.make_async_copy(lam_ref.at[i], lamo_ref.at[slot], local_sem.at[2])
            copy.start()
            copy.wait()
        pl.when(jnp.logical_not(away[i]))(keep)
    for load in loads:
        load.wait()
    multiply(True, tp, 0)
    receive_x(t_left, 0)
    send_x(False, t_left, 0, right)
    for q in (2, 3):
        send_x(True, tp, q, right)
    receive_x(t_right, 1)
    send_x(False, t_right, 1, left)
    for q in (3, 2):
        send_x(True, tp, q, left)
    multiply(True, tp, 1)
    receive_x(t_left, 1)
    receive_x(t_right, 0)
    multiply_other(tp, 0)
    multiply_other(tp, 1)
    multiply(False, t_left, 0)
    multiply(False, t_right, 0)
    multiply_other(t_left, 0)
    multiply_other(t_right, 0)
    receive_x(t_far, 0)
    receive_x(t_far, 1)
    multiply(False, t_far, 0)
    multiply_other(t_far, 0)
    pack(0)
    receive_x(t_left, 2)
    send_x(False, t_left, 2, right)
    receive_x(t_right, 3)
    send_x(False, t_right, 3, left)
    receive_x(t_right, 2)
    receive_x(t_left, 3)
    open_ring(0)
    multiply(False, t_left, 1)
    multiply(False, t_right, 1)
    multiply_other(t_left, 1)
    multiply_other(t_right, 1)
    receive_x(t_far, 2)
    receive_x(t_far, 3)
    multiply(False, t_far, 1)
    ring(0, 1)
    multiply_other(t_far, 1)
    pack(1)
    for copy in edges:
        copy.start()
    att[...] = jnp.zeros_like(att)
    qz[...] = jnp.zeros_like(qz)
    m_buf[...] = jnp.full_like(m_buf, masked_score)
    for i in range(1, 5):
        turn(i)
    band(1)
    band(2)
    open_ring(1)
    for i in range(2):
        def rest(i=i):
            for u in range(2):
                remote(
                    msg.at[0, u, pl.ds(256, 128)], q_ref.at[i, u], send_a.at[0, u, 1], recv_q.at[i, u], sibling
                ).wait_recv()
            remote(lam_ref.at[0], lamo_ref.at[i], send_lam.at[0], recv_lam.at[i], sibling).wait_recv()
        pl.when(away[i])(rest)
    set_queries()
    ring(0, 2)
    segment(0, 4, (0, 1), True)
    ring(0, 3)
    ring(1, 1)
    segment(4, 12, (0, 1), True)
    ring(1, 2)
    ring(0, 4)
    segment(12, 20, (0,), True)
    ring(1, 3)
    segment(20, 28, (0,), True)
    ring(1, 4)
    band_edges()
    band(0)
    band(3)
    segment(28, 32, (0,), True)
    finish(0)
    segment(12, 18, (1,), False)
    merge_give(0)
    segment(18, 24, (1,), False)
    merge_send(0)
    segment(24, 32, (1,), False)
    finish(1)
    merge_join(0)
    merge_give(1)
    merge_send(1)
    merge_out(0)
    merge_join(1)
    merge_out(1)
    for ref, sem in (
        (xg.at[pl.ds(0, 7)], send_xs),
        (kv_ref.at[pl.ds(0, 14)], send_ring),
        (kv_ref.at[pl.ds(0, 16)], send_sib),
        (give, send_g),
        (joined, send_f),
        (fin, send_n),
    ):
        remote(ref, ref, sem, recv_x.at[0, 0], sibling).wait_send()
    for copy in edges:
        copy.wait_send()
    for i in range(2):
        def sent(i=i):
            for u in range(2):
                for copy in head_copies(i, u):
                    copy.wait_send()
                back(u, i).wait_send()
            lam_copy(i).wait_send()
        pl.when(away[i])(sent)


def layer(length, mix_lambda, sink_logit, inputs, gain, weights):
    bf, f32 = jnp.bfloat16, jnp.float32
    depth = weights[3].shape[0]
    width = weights[6].shape[1]
    dma = pltpu.SemaphoreType.DMA
    vmem = pltpu.VMEM
    return pl.pallas_call(
        layer_kernel,
        out_shape=jax.ShapeDtypeStruct((2 * SHARE, width), bf),
        in_specs=[SMEM_SPEC] * 3 + [VMEM_SPEC] * 2 + [HBM_SPEC] * 8,
        out_specs=VMEM_SPEC,
        scratch_shapes=[
            vmem((GROUPS, 2, GROUPS, SHARE, ROWS), bf),
            vmem((320, depth), bf),
            vmem((depth, 128), bf),
            vmem((depth, 128), bf),
            vmem((depth, 128), bf),
            vmem((GROUP * HEAD, width), bf),
            vmem((128, width), bf),
            vmem((ROWS, ACC_COLS), f32),
            vmem((2, 2, 384, 128), bf),
            vmem((2, 8, 128), f32),
            vmem((2, 8, 128), f32),
            vmem((2, WINDOW, 128), bf),
            vmem((ROWS, 256), bf),
            vmem((ROWS + 2 * WINDOW, 128), bf),
            vmem((HEAD, ROWS + 2 * WINDOW), bf),
            vmem((ROWS, GROUP * HEAD), bf),
            vmem((BLOCKS, 2, HALF, 128), bf),
            vmem((2, 2, 128, 128), bf),
            vmem((2, 128, 2 * TILE), bf),
            vmem((2, 16, ROWS), bf),
            vmem((80, 2 * TILE), f32),
            vmem((2, 256, TILE), f32),
            vmem((2, 8, TILE), f32),
            vmem((8, 2 * TILE), f32),
            vmem((2, 256, 128), f32),
            vmem((2, 256, 128), jnp.int32),
            vmem((2, 2, 8, 128), jnp.int32),
            vmem((2, 2, 128, 128), bf),
            vmem((2, 2, 128, 128), bf),
            vmem((HALF, 128), bf),
            vmem((2, 2, 128, GROUP * HEAD), bf),
            vmem((2, 2, 128, 128), bf),
            vmem((2, CHUNKS, 128, CHUNK), bf),
            vmem((2, CHUNKS, 128, CHUNK), bf),
            vmem((2, NX, CHUNKS, SHARE, CHUNK), bf),
            vmem((2, CHUNKS, SHARE, CHUNK), bf),
            vmem((2, CHUNKS, SHARE, CHUNK), bf),
            vmem((2, 2, CHUNKS, SHARE, CHUNK), bf),
            dma((8,)), dma((GROUPS, 4)), dma,
            dma((BLOCKS, 2)), dma((2, 2)), dma((2,)), dma((2,)),
            dma((2, 2, 2)), dma((2,)), dma, dma, dma((2,)), dma((3,)),
            dma((2, 2)), dma((2, 2)), dma, dma((2, CHUNKS)), dma, dma((2, CHUNKS)),
            dma, dma((2, 2, CHUNKS)),
        ],
        compiler_params=pltpu.CompilerParams(
            collective_id=0, has_side_effects=True, vmem_limit_bytes=62 * 1024 * 1024
        ),
        name="layer",
    )(length, mix_lambda, sink_logit, inputs, gain, *weights)


def body(
    inputs, length, win_query, win_key, win_value, sink_logit,
    diff_query, diff_key, diff_value, mix_lambda, head_gain, win_out, diff_out,
):
    weights = (
        win_query.T, win_key.T, win_value.T, diff_query, diff_key, diff_value, win_out, diff_out,
    )
    rows = inputs.reshape(GROUPS, 2, SHARE, inputs.shape[1])
    return layer(length, mix_lambda, sink_logit, rows, head_gain.reshape(1, HEAD), weights)


def solution(mesh):
    placed = (
        P("sp", "tp"), P(), P(None, "tp"), P(None, "tp"), P(None, "tp"), P("tp"), P(None, "tp"),
        P(None, "tp"), P(None, "tp"), P("tp"), P(), P("tp", None), P("tp", None),
    )
    return jax.shard_map(
        body, mesh=mesh, in_specs=placed, out_specs=P(("sp", "tp"), None), check_vma=False
    )
```
